32 devices in a mesh: sp: 8 (over z, y), tp: 4 (over x, core).
Axes of the slice: x: 2, y: 2, z: 4, core: 2. Of those that a mesh axis runs over, the one named last changes fastest.
Arguments:
- tokens: bfloat16 [2048, 2048], P(('sp', 'tp')), may hold values from -6 to 6
- norm_gain: float32 [2048], replicated, may hold values from 0.1 to 1.9
- query_weight: bfloat16 [1024, 2048], P('tp', 'sp'), may hold values from -0.088609319 to 0.088609319
- key_weight: bfloat16 [256, 2048], P('tp', 'sp'), may hold values from -0.10628699 to 0.10628699
- value_weight: bfloat16 [256, 2048], P('tp', 'sp'), may hold values from -0.125 to 0.125
- gate_weight: bfloat16 [1024, 2048], P('tp', 'sp'), may hold values from -0.125 to 0.125
- left_weight: bfloat16 [1024, 2048], P('tp', 'sp'), may hold values from -0.125 to 0.125
- input_weight: bfloat16 [1024, 2048], P('tp', 'sp'), may hold values from -0.125 to 0.125
- query_gain: float32 [64], replicated, may hold values from 0.3 to 4.5, as said below
- key_gain: float32 [64], replicated, may hold values from 0.3 to 4.5, as said below
- sink_logit: float32 [16], P('tp'), may hold values from 2 to 7
- conv_weight: float32 [3, 1024], P(None, 'tp'), may hold values from -3 to 3
- out_attention: bfloat16 [1024, 2048], P('tp', 'sp'), may hold values from -0.125 to 0.125
- out_conv: bfloat16 [1024, 2048], P('tp', 'sp'), may hold values from -0.125 to 0.125
Outputs:
- mixed: bfloat16 [2048, 2048], P(('sp', 'tp'))
The draws below stay inside these ranges and needn't reach their ends.
Inputs may be any that keep to these rules, and one draw needn't show every extreme that they name: `query_gain`: positive. `key_gain`: positive.
All inputs are finite; a program needn't handle non-finite values.
Results may differ from the reference program's by a relative error of at most 0.024.
Values may be sent and summed in bfloat16 or wider, within the bound.
A program may use at most 64 MiB of HBM per device.

```python
import jax
import jax.numpy as jnp
from jax import lax

D = 2048
HEAD_DIM = 64
Q_HEADS = 16
KV_HEADS = 4
CONV_CH = 1024
WINDOW = 128
BLOCK = 128
TOKENS = 2048
N_TP = 4


def shared_query(key):
    return jnp.clip(jax.random.normal(jax.random.fold_in(key, 101), (Q_HEADS * HEAD_DIM, D), jnp.float32), -4.0, 4.0) * D ** (-0.5)


def draw_query_weight(key, part):
    return shared_query(key).astype(jnp.bfloat16)


def draw_key_weight(key, part):
    noise = jnp.clip(jax.random.normal(jax.random.fold_in(key, 102), (KV_HEADS * HEAD_DIM, D), jnp.float32), -4.0, 4.0) * D ** (-0.5)
    result = noise
    return result.astype(jnp.bfloat16)


def draw_query_gain(key, part):
    result = jax.random.uniform(jax.random.fold_in(key, 103), (HEAD_DIM,), jnp.float32, 0.3, 1.9)
    return result


def draw_key_gain(key, part):
    result = jax.random.uniform(jax.random.fold_in(key, 104), (HEAD_DIM,), jnp.float32, 0.3, 1.9)
    return result


def level_of(rng, shape, cuts, least, top_value):
    def one(axis_at, parts):
        draws = jax.random.uniform(jax.random.fold_in(jax.random.fold_in(rng, 6), axis_at), (parts,), jnp.float32, least / len(cuts), top_value / len(cuts))
        return jnp.repeat(jnp.exp(draws), shape[axis_at] // parts).reshape((-1,) + (1,) * (len(shape) - axis_at - 1))

    loudness = one(*cuts[0])
    for cut in cuts[1:]:
        loudness = loudness * one(*cut)
    return loudness


def centred(own_key, extent, deviation, limit, split=(), held_as=jnp.bfloat16):
    level = level_of(own_key, extent, split, -0.22, 0.18) if split else 1.0
    drawn = jax.random.normal(own_key, extent, jnp.float32) * deviation * level
    return jnp.minimum(jnp.maximum(drawn, -limit), limit).astype(held_as)


def setup_inputs(seed: int = 0) -> dict:
    splits = jax.random.split(jax.random.key(seed), 15)
    return {
        "tokens": centred(splits[0], (TOKENS, D), 1.0, 6.0, ((0, 32),)),
        "norm_gain": jnp.clip(1.0 + 0.18 * jax.random.normal(splits[1], (D,), jnp.float32), 0.1, 1.9),
        "query_weight": draw_query_weight(jax.random.fold_in(splits[14], 71), 0),
        "key_weight": draw_key_weight(jax.random.fold_in(splits[14], 71), 0),
        "value_weight": centred(splits[4], (KV_HEADS * HEAD_DIM, D), D ** -0.5, 0.125, ((0, 4), (1, 8))),
        "gate_weight": centred(splits[5], (CONV_CH, D), D ** -0.5, 0.125, ((0, 4), (1, 8))),
        "left_weight": centred(splits[6], (CONV_CH, D), D ** -0.5, 0.125, ((0, 4), (1, 8))),
        "input_weight": centred(splits[7], (CONV_CH, D), D ** -0.5, 0.125, ((0, 4), (1, 8))),
        "query_gain": draw_query_gain(jax.random.fold_in(splits[14], 71), 0),
        "key_gain": draw_key_gain(jax.random.fold_in(splits[14], 71), 0),
        "sink_logit": jnp.clip(2.0 + 5.0 * jax.random.uniform(splits[10], (Q_HEADS,), jnp.float32) ** level_of(splits[10], (Q_HEADS,), ((0, 4),), -0.2, 0.2), 2.0, 7.0),
        "conv_weight": centred(splits[11], (3, CONV_CH), 0.6, 3.0, ((1, 4),), jnp.float32),
        "out_attention": centred(splits[12], (Q_HEADS * HEAD_DIM, D), (Q_HEADS * HEAD_DIM + CONV_CH) ** -0.5, 0.125, ((0, 4), (1, 8))),
        "out_conv": centred(splits[13], (CONV_CH, D), (Q_HEADS * HEAD_DIM + CONV_CH) ** -0.5, 0.125, ((0, 4), (1, 8))),
    }


EPS = 1e-06
ROPE_BASE = 10000.0
NEG_FILL = -1e+30

def normalize(values, gain):
    return values * lax.rsqrt(lax.optimization_barrier(jnp.mean(values * values, axis=-1, keepdims=True)) + EPS) * gain

def rotate(values, positions):
    half = values.shape[-1] // 2
    freq = ROPE_BASE ** (-jnp.arange(half, dtype=jnp.float32) / half)
    angle = positions[:, None] * freq
    cosine = jnp.cos(angle)[:, None, :]
    sine = jnp.sin(angle)[:, None, :]
    first = values[..., :half]
    second = values[..., half:]
    return jnp.concatenate([first * cosine - second * sine, second * cosine + first * sine], axis=-1)

def project(rows, weight):
    return lax.dot_general(rows, weight, (((1,), (1,)), ((), ())), preferred_element_type=jnp.float32).astype(jnp.bfloat16)

def reference(tokens, norm_gain, query_weight, key_weight, value_weight, gate_weight, left_weight, input_weight, query_gain, key_gain, sink_logit, conv_weight, out_attention, out_conv):
    count = tokens.shape[0]
    normed = normalize(tokens.astype(jnp.float32), norm_gain).astype(jnp.bfloat16)
    query = project(normed, query_weight).reshape(count, Q_HEADS, HEAD_DIM)
    keys = project(normed, key_weight).reshape(count, KV_HEADS, HEAD_DIM)
    values = project(normed, value_weight).reshape(count, KV_HEADS, HEAD_DIM)
    gate = project(normed, gate_weight)
    left = project(normed, left_weight)
    inputs = project(normed, input_weight)
    positions = jnp.arange(count, dtype=jnp.float32)
    query_rot = rotate(normalize(query.astype(jnp.float32), query_gain), positions).astype(jnp.bfloat16)
    key_rot = rotate(normalize(keys.astype(jnp.float32), key_gain), positions).astype(jnp.bfloat16)
    group = Q_HEADS // KV_HEADS
    span = BLOCK + 2 * WINDOW
    padded_keys = jnp.pad(key_rot, ((WINDOW, WINDOW), (0, 0), (0, 0)))
    padded_values = jnp.pad(values, ((WINDOW, WINDOW), (0, 0), (0, 0)))
    nblocks = count // BLOCK
    shaped = query_rot.reshape(nblocks, BLOCK, KV_HEADS, group, HEAD_DIM)
    sinks = sink_logit.reshape(KV_HEADS, group)[:, :, None]

    def one_block(packed):
        block_index, query_block = packed
        begin = block_index * BLOCK
        key_block = lax.dynamic_slice_in_dim(padded_keys, begin, span, 0)
        value_block = lax.dynamic_slice_in_dim(padded_values, begin, span, 0)
        scores = jnp.einsum('qkgd,nkd->kgqn', query_block.astype(jnp.float32), key_block.astype(jnp.float32)) * HEAD_DIM ** (-0.5)
        query_pos = begin + jnp.arange(BLOCK, dtype=jnp.int32)
        key_pos = begin - WINDOW + jnp.arange(span, dtype=jnp.int32)
        allowed = (jnp.abs(query_pos[:, None] - key_pos[None, :]) <= WINDOW) & (key_pos >= 0)[None, :] & (key_pos < count)[None, :]
        scores = jnp.where(allowed, scores, NEG_FILL)
        top = jnp.maximum(lax.optimization_barrier(jnp.max(scores, axis=-1)), sinks)
        expo = jnp.exp(scores - top[..., None])
        total = lax.optimization_barrier(jnp.sum(expo, axis=-1)) + jnp.exp(sinks - top)
        weights = (expo / total[..., None]).astype(jnp.bfloat16)
        return jnp.einsum('kgqn,nkd->qkgd', weights.astype(jnp.float32), value_block.astype(jnp.float32)).astype(jnp.bfloat16)
    attended = lax.map(one_block, (jnp.arange(nblocks, dtype=jnp.int32), shaped)).reshape(count, Q_HEADS * HEAD_DIM)
    product = (left.astype(jnp.float32) * inputs.astype(jnp.float32)).astype(jnp.bfloat16)
    padded = jnp.pad(product.astype(jnp.float32), ((1, 1), (0, 0)))
    convolved = conv_weight[0] * padded[:-2] + conv_weight[1] * padded[1:-1] + conv_weight[2] * padded[2:]
    gated = (gate.astype(jnp.float32) * convolved).astype(jnp.bfloat16)
    attn_width = Q_HEADS * HEAD_DIM // N_TP
    conv_width = CONV_CH // N_TP
    summed = jnp.zeros((count, D), jnp.float32)
    for place in range(N_TP):
        partial_sum = jnp.dot(attended[:, place * attn_width:(place + 1) * attn_width], out_attention[place * attn_width:(place + 1) * attn_width], preferred_element_type=jnp.float32)
        partial_sum = partial_sum + jnp.dot(gated[:, place * conv_width:(place + 1) * conv_width], out_conv[place * conv_width:(place + 1) * conv_width], preferred_element_type=jnp.float32)
        summed = summed + partial_sum.astype(jnp.bfloat16).astype(jnp.float32)
    return summed.astype(jnp.bfloat16)
```

```python
import functools

import jax
import jax.numpy as jnp
import numpy as np
from jax import lax
from jax.experimental import pallas as pl
from jax.experimental.pallas import tpu as pltpu
from jax.sharding import PartitionSpec as P

HEAD_DIM = 64
WINDOW = 128
BLOCK = 128


EPS = 1e-06
ROPE_BASE = 10000.0
NEG_FILL = -1e30


def with_halo(cells, sides, width):
    for axis, dim in sides:
        count = lax.axis_size(axis)
        ends = count - 1
        head = lax.slice_in_dim(cells, 0, width, axis=dim)
        tail = lax.slice_in_dim(cells, cells.shape[dim] - width, cells.shape[dim], axis=dim)
        cells = jnp.concatenate(
            [
                lax.ppermute(tail, axis, [(i, (i + 1) % count) for i in range(ends)]),
                cells,
                lax.ppermute(head, axis, [((i + 1) % count, i) for i in range(ends)]),
            ],
            axis=dim,
        )
    return cells


def normalize(values, gain):
    return values * lax.rsqrt(jnp.mean(values * values, axis=-1, keepdims=True) + EPS) * gain


def rotate(values, positions):
    half = values.shape[-1] // 2
    freq = ROPE_BASE ** (-jnp.arange(half, dtype=jnp.float32) / half)
    angle = positions[:, None] * freq
    cosine = jnp.cos(angle)[:, None, :]
    sine = jnp.sin(angle)[:, None, :]
    first = values[..., :half]
    second = values[..., half:]
    return jnp.concatenate(
        [first * cosine - second * sine, second * cosine + first * sine], axis=-1
    )


def project(rows, weight):
    return lax.dot_general(
        rows, weight, (((1,), (1,)), ((), ())), preferred_element_type=jnp.float32
    ).astype(jnp.bfloat16)


def attend(query_rot, key_rim, value_rim, sinks, offset, total):
    count = query_rot.shape[0]
    local_heads = query_rot.shape[1]
    kv_local = key_rim.shape[1]
    group = local_heads // kv_local
    span = BLOCK + 2 * WINDOW
    nblocks = count // BLOCK
    shaped = query_rot.reshape(nblocks, BLOCK, kv_local, group, HEAD_DIM)
    sink_group = sinks.reshape(kv_local, group)[:, :, None]

    def one_block(packed):
        block_index, query_block = packed
        begin = block_index * BLOCK
        key_block = lax.dynamic_slice_in_dim(key_rim, begin, span, 0)
        value_block = lax.dynamic_slice_in_dim(value_rim, begin, span, 0)
        scores = jnp.einsum(
            "qkgd,nkd->kgqn", query_block, key_block, preferred_element_type=jnp.float32
        ) * HEAD_DIM ** (-0.5)
        query_pos = offset + begin + jnp.arange(BLOCK, dtype=jnp.int32)
        key_pos = offset + begin - WINDOW + jnp.arange(span, dtype=jnp.int32)
        allowed = (
            (jnp.abs(query_pos[:, None] - key_pos[None, :]) <= WINDOW)
            & (key_pos >= 0)[None, :]
            & (key_pos < total)[None, :]
        )
        scores = jnp.where(allowed, scores, NEG_FILL)
        top = jnp.maximum(jnp.max(scores, axis=-1), sink_group)
        expo = jnp.exp(scores - top[..., None])
        denom = jnp.sum(expo, axis=-1) + jnp.exp(sink_group - top)
        weights = (expo / denom[..., None]).astype(jnp.bfloat16)
        return jnp.einsum(
            "kgqn,nkd->qkgd", weights, value_block, preferred_element_type=jnp.float32
        ).astype(jnp.bfloat16)

    result = lax.map(one_block, (jnp.arange(nblocks, dtype=jnp.int32), shaped))
    return result.reshape(count, local_heads * HEAD_DIM)


def per_device(
    tokens,
    norm_gain,
    query_weight,
    key_weight,
    value_weight,
    gate_weight,
    left_weight,
    input_weight,
    query_gain,
    key_gain,
    sink_logit,
    conv_weight,
    out_attention,
    out_conv,
):
    sp_count = lax.axis_size("sp")
    sp_place = lax.axis_index("sp")
    gathered = (
        lax.all_gather(query_weight, "sp", axis=1, tiled=True),
        lax.all_gather(key_weight, "sp", axis=1, tiled=True),
        lax.all_gather(value_weight, "sp", axis=1, tiled=True),
        lax.all_gather(gate_weight, "sp", axis=1, tiled=True),
        lax.all_gather(left_weight, "sp", axis=1, tiled=True),
        lax.all_gather(input_weight, "sp", axis=1, tiled=True),
        lax.all_gather(out_attention, "sp", axis=1, tiled=True),
        lax.all_gather(out_conv, "sp", axis=1, tiled=True),
    )
    (
        query_full,
        key_full,
        value_full,
        gate_full,
        left_full,
        input_full,
        attn_out_full,
        conv_out_full,
    ) = gathered
    normed = normalize(tokens.astype(jnp.float32), norm_gain).astype(jnp.bfloat16)
    widths = [
        query_full.shape[0],
        key_full.shape[0],
        value_full.shape[0],
        gate_full.shape[0],
        left_full.shape[0],
        input_full.shape[0],
    ]
    piece = lax.all_gather(normed, "tp", axis=0, tiled=True)
    joined = jnp.concatenate(
        [
            project(piece, weight)
            for weight in (query_full, key_full, value_full, gate_full, left_full, input_full)
        ],
        axis=1,
    )
    count = joined.shape[0]
    bounds = [0]
    for width in widths:
        bounds.append(bounds[-1] + width)
    query, keys, values, gate, left, inputs = [
        joined[:, bounds[place] : bounds[place + 1]] for place in range(6)
    ]
    offset = sp_place * count
    total = count * sp_count
    positions = (offset + jnp.arange(count, dtype=jnp.int32)).astype(jnp.float32)
    local_heads = widths[0] // HEAD_DIM
    kv_local = widths[1] // HEAD_DIM
    query_rot = rotate(
        normalize(query.reshape(count, local_heads, HEAD_DIM).astype(jnp.float32), query_gain),
        positions,
    ).astype(jnp.bfloat16)
    key_rot = rotate(
        normalize(keys.reshape(count, kv_local, HEAD_DIM).astype(jnp.float32), key_gain), positions
    ).astype(jnp.bfloat16)
    key_flat = key_rot.reshape(count, kv_local * HEAD_DIM)
    product = (left.astype(jnp.float32) * inputs.astype(jnp.float32)).astype(jnp.bfloat16)
    kv_width = widths[1]
    pair_rim = with_halo(jnp.concatenate([key_flat, values], axis=1), (("sp", 0),), WINDOW)
    product_rim = with_halo(product, (("sp", 0),), 1)
    rim_rows = pair_rim.shape[0]
    key_rim = pair_rim[:, :kv_width].reshape(rim_rows, kv_local, HEAD_DIM)
    value_rim = pair_rim[:, kv_width:].reshape(rim_rows, kv_local, HEAD_DIM)
    attended = attend(query_rot, key_rim, value_rim, sink_logit, offset, total)
    padded = product_rim.astype(jnp.float32)
    convolved = (
        conv_weight[0] * padded[:-2] + conv_weight[1] * padded[1:-1] + conv_weight[2] * padded[2:]
    )
    gated = (gate.astype(jnp.float32) * convolved).astype(jnp.bfloat16)
    return lax.psum_scatter(
        (
            jnp.dot(attended, attn_out_full, preferred_element_type=jnp.float32)
            + jnp.dot(gated, conv_out_full, preferred_element_type=jnp.float32)
        ).astype(jnp.bfloat16),
        "tp",
        scatter_dimension=0,
        tiled=True,
    )


MESH = pl.DeviceIdType.MESH


def fused_kernel(
    dims,
    tok_hbm, gain_hbm, q_hbm, k_hbm, v_hbm, g_hbm, l_hbm, i_hbm,
    qgain_hbm, kgain_hbm, sink_hbm, conv_hbm, oa_hbm, oc_hbm, trig_hbm,
    out_ref,
    gain_ref, qgain_ref, kgain_ref, sink_ref, conv_ref, tok, trig, stage, ostage, win, wout, normed, normed2, acc, acc2, rim, prod, prod2, mix_a, mix_c, gated2,
    qrot,
    keep, s1, r1, s2, r2,
    local_sem, y_send, w_recv, m_send, e_send,
    tok_send, tok_recv, tok2_send, tok2_recv, rim_send, rim_recv, prod_send, prod_recv, g_send, g_recv,
    rs_send, rs_recv,
):
    scope = jax.named_scope
    line, rows, depth, qr, kr, cr = (
        dims["line"], dims["rows"], dims["depth"], dims["qr"], dims["kr"], dims["cr"]
    )
    sp = lax.axis_index("sp")
    tp = lax.axis_index("tp")
    z, y = sp // 2, sp % 2
    x, c = tp // 2, tp % 2
    y_peer = (2 * z + 1 - y, tp)
    x_peer = (sp, 2 * (1 - x) + c)
    c_peer = (sp, 2 * x + 1 - c)
    low_side = z < 2
    toward = jnp.where(low_side, 1, -1)
    is_end = (z == 0) | (z == line - 1)
    inner = (z > 0) & (z < line - 1)
    m_plane = z + toward
    e_plane = jnp.where(inner, z - toward, m_plane)
    m_peer = (2 * m_plane + y, tp)
    e_peer = (2 * e_plane + y, tp)
    near = jnp.where(inner, z - toward, z + toward)
    mid = jnp.where(inner, z + toward, z + 2 * toward)
    far = jnp.where(inner, z + 2 * toward, z + 3 * toward)
    sources = (z, near, mid, far)
    s_own = sp
    s_mate = 2 * z + 1 - y
    plane = 8 * rows
    core = qr + 2 * kr

    barrier = pltpu.get_barrier_semaphore()
    for peer in (y_peer, x_peer, c_peer, m_peer):
        pl.semaphore_signal(barrier, inc=1, device_id=peer, device_id_type=MESH)

    @pl.when(inner)
    def _():
        pl.semaphore_signal(barrier, inc=1, device_id=e_peer, device_id_type=MESH)

    counter = [0]

    def local(src, dst):
        copy = pltpu.make_async_copy(src, dst, local_sem.at[counter[0]])
        counter[0] += 1
        copy.start()
        return copy

    def core_pieces(which, dst):
        q0 = pl.multiple_of(which * qr, qr)
        return [
            local(q_hbm.at[pl.ds(q0, qr)], dst.at[0:qr]),
            local(k_hbm, dst.at[qr : qr + kr]),
            local(v_hbm, dst.at[qr + kr : qr + 2 * kr]),
        ]

    def conv_pieces(which, dst):
        c0 = pl.multiple_of(which * cr, cr)
        return [
            local(g_hbm.at[pl.ds(c0, cr)], dst.at[core : core + cr]),
            local(l_hbm.at[pl.ds(c0, cr)], dst.at[core + cr : core + 2 * cr]),
            local(i_hbm.at[pl.ds(c0, cr)], dst.at[core + 2 * cr : core + 3 * cr]),
        ]

    def out_pieces(which, dst):
        q0, c0 = pl.multiple_of(which * qr, qr), pl.multiple_of(which * cr, cr)
        return [
            local(oa_hbm.at[pl.ds(q0, qr)], dst.at[0:qr]),
            local(oc_hbm.at[pl.ds(c0, cr)], dst.at[qr : qr + cr]),
        ]

    loads = core_pieces(y, win.at[s_own]) + core_pieces(1 - y, stage)
    tok_loads = [local(tok_hbm, tok), local(gain_hbm, gain_ref)]
    loads += conv_pieces(y, win.at[s_own]) + conv_pieces(1 - y, stage)
    loads += out_pieces(y, wout.at[s_own]) + out_pieces(1 - y, ostage)
    side_copies = [
        local(trig_hbm.at[pl.ds(pl.multiple_of(z * plane, plane), plane)], trig),
        local(qgain_hbm, qgain_ref),
        local(kgain_hbm, kgain_ref),
        local(sink_hbm, sink_ref),
        local(conv_hbm, conv_ref),
    ]

    with scope("barrier"):
        pl.semaphore_wait(barrier, 4 + inner.astype(jnp.int32))

    def remote(src, dst, send, recv, peer):
        return pltpu.make_async_remote_copy(
            src_ref=src, dst_ref=dst, send_sem=send, recv_sem=recv,
            device_id=peer, device_id_type=MESH,
        )

    def chunk(kind, s):
        if kind == 2:
            return wout.at[s]
        return win.at[s, 0:core] if kind == 0 else win.at[s, core : core + 3 * cr]

    def hop(kind, s, sends, peer):
        return remote(chunk(kind, s), chunk(kind, s), sends.at[kind, s], w_recv.at[kind, s], peer)

    def send_m(kind, s):
        hop(kind, s, m_send, m_peer).start()

    def send_e(kind, s):
        hop(kind, s, e_send, e_peer).start()

    def take(kind, s):
        hop(kind, s, m_send, m_peer).wait_recv()

    def y_hop(kind):
        if kind == 2:
            src = ostage
        else:
            src = stage.at[0:core] if kind == 0 else stage.at[core : core + 3 * cr]
        return remote(src, chunk(kind, s_own), y_send.at[kind], w_recv.at[kind, s_own], y_peer)

    def first_of(source):
        return 2 * source + y

    def second_of(source):
        return 2 * source + 1 - y

    for copy in loads:
        copy.wait()
    send_m(0, s_own)

    @pl.when(inner)
    def _():
        send_e(0, s_own)

    y_hop(0).start()

    @pl.when(inner)
    def _():
        send_m(1, s_own)
        send_e(2, s_own)

    with scope("norm"):
        for copy in tok_loads:
            copy.wait()
        t = tok[...].astype(jnp.float32)
        t = t * lax.rsqrt(jnp.mean(t * t, axis=-1, keepdims=True) + EPS) * gain_ref[...]

        def block_of(yy, xx, cc):
            return 4 * yy + 2 * xx + cc

        own_block = block_of(y, x, c)
        xb = block_of(y, 1 - x, c)
        yb = block_of(1 - y, x, c)
        db = block_of(1 - y, 1 - x, c)
        normed[own_block] = t.astype(jnp.bfloat16)

    def tok_hop(block, slot, peer):
        return remote(
            normed.at[block], normed.at[block], tok_send.at[slot], tok_recv.at[block], peer
        )

    def end_tok(block, slot, half=None):
        part = slice(0, rows) if half is None else slice(half * rows // 2, (half + 1) * rows // 2)
        return remote(
            normed.at[block, part], normed2.at[block, part], tok2_send.at[slot],
            tok2_recv.at[block], m_peer,
        )

    def tok2_hop(block, slot, peer):
        return remote(
            normed2.at[block], normed2.at[block], tok2_send.at[slot], tok2_recv.at[block], peer
        )

    tok_copies = []

    def tok_go(block, peer):
        copy = tok_hop(block, len(tok_copies), peer)
        copy.start()
        tok_copies.append(copy)

    def tok_wait(block):
        tok_hop(block, 0, x_peer).wait_recv()

    def tok2_wait(block):
        tok2_hop(block, 0, x_peer).wait_recv()

    @pl.when(is_end)
    def _():
        end_tok(own_block, 6, 0).start()

    tok_go(own_block, x_peer)
    tok_go(own_block, y_peer)
    tok_go(own_block, c_peer)
    y_hop(1).start()

    with scope("c_mate"):
        take(0, s_mate)
        send_m(0, s_mate)

        @pl.when(inner)
        def _():
            send_e(0, s_mate)
            take(0, first_of(near))
            send_m(0, first_of(near))
            take(0, first_of(mid))
            send_e(0, first_of(mid))

        @pl.when(is_end)
        def _():
            end_tok(own_block, 8, 1).start()
            send_m(1, s_own)

    with scope("tok_xb"):
        tok_wait(xb)
        tok_go(xb, c_peer)

    with scope("tok_yb"):
        tok_wait(yb)
        tok_go(yb, x_peer)
        tok_go(yb, c_peer)

    with scope("c_fwd"):
        @pl.when(inner)
        def _():
            take(0, second_of(mid))
            send_e(0, second_of(mid))
            take(0, second_of(near))
            send_m(0, second_of(near))

    with scope("tok2_own"):
        @pl.when(inner)
        def _():
            tok2_wait(own_block)
            tok2_hop(own_block, 0, x_peer).start()
            tok2_hop(own_block, 1, y_peer).start()
            tok2_hop(own_block, 2, c_peer).start()

    y_hop(2).start()

    with scope("v_mate"):
        take(1, s_mate)
        send_m(1, s_mate)

    with scope("far1"):
        @pl.when(inner)
        def _():
            take(0, first_of(far))
            send_e(0, first_of(far))

    with scope("tok_db"):
        tok_wait(db)
        tok_go(db, c_peer)

        @pl.when(is_end)
        def _():
            end_tok(db, 7).start()
            send_m(2, s_own)

    with scope("far2"):
        @pl.when(inner)
        def _():
            take(1, first_of(near))
            send_m(1, first_of(near))
            take(0, second_of(far))
            send_e(0, second_of(far))

    with scope("tok_rest"):
        for yy in range(2):
            for xx in range(2):
                tok_wait(block_of(yy, xx, 1 - c))

    def columns(s):
        return pl.ds(pl.multiple_of(s * depth, depth), depth)

    def dot_t(a, w):
        return lax.dot_general(a, w, (((1,), (1,)), ((), ())), preferred_element_type=jnp.float32)

    with scope("c_dots"):
        @pl.when(is_end)
        def _():
            for source in (near, mid, far):
                for s in (first_of(source), second_of(source)):
                    take(0, s)

        acc[:, 0:core] = jnp.zeros((plane, core), jnp.float32)

        def c_step(s, carry):
            a = normed[:, :, columns(s)].reshape(plane, depth)
            acc[:, 0:core] += dot_t(a, win[s, 0:core])
            return carry

        lax.fori_loop(0, 2 * line, c_step, 0)

    with scope("rot"):
        for copy in side_copies:
            copy.wait()
        lane = lax.broadcasted_iota(jnp.int32, (plane, qr), 1)
        half_dim = HEAD_DIM // 2
        table = trig[...]
        cos2 = jnp.where(lane < HEAD_DIM, table, pltpu.roll(table, HEAD_DIM, 1))
        sin2 = jnp.where(lane < HEAD_DIM, pltpu.roll(table, HEAD_DIM, 1), table)
        low = lane < HEAD_DIM
        first_half = lane % HEAD_DIM < half_dim

        def rot(v):
            partner = jnp.where(
                first_half, pltpu.roll(v, qr - half_dim, 1), pltpu.roll(v, half_dim, 1)
            )
            return v * cos2 + partner * sin2

        def bf(v):
            return v.astype(jnp.bfloat16).astype(jnp.float32)

        kv = bf(acc[:, qr : 2 * qr])
        ksq = jnp.sum(jnp.where(low, kv * kv, 0.0), axis=-1, keepdims=True) / HEAD_DIM
        kgain = jnp.concatenate([kgain_ref[...], kgain_ref[...]], axis=1)
        kn = kv * lax.rsqrt(ksq + EPS) * kgain
        krot = rot(kn)
        rim[WINDOW : WINDOW + plane, :] = jnp.where(low, krot, kv).astype(jnp.bfloat16)

    bottom = pl.ds(WINDOW, WINDOW)
    top = pl.ds(plane, WINDOW)
    up = (jnp.minimum(2 * (z + 1) + y, 2 * line - 1), tp)
    down = (jnp.maximum(2 * (z - 1) + y, 0), tp)
    has_up = z < line - 1
    has_down = z > 0
    rim_up = remote(rim.at[top], rim.at[pl.ds(0, WINDOW)], rim_send.at[0], rim_recv.at[0], up)
    rim_down = remote(
        rim.at[bottom], rim.at[pl.ds(WINDOW + plane, WINDOW)], rim_send.at[1], rim_recv.at[1], down
    )

    @pl.when(has_up)
    def _():
        rim_up.start()

    @pl.when(has_down)
    def _():
        rim_down.start()

    zero_rim = jnp.zeros((WINDOW, qr), jnp.bfloat16)

    @pl.when(z == 0)
    def _():
        rim[0:WINDOW] = zero_rim

    @pl.when(z == line - 1)
    def _():
        rim[WINDOW + plane :] = zero_rim

    with scope("v_near"):
        @pl.when(inner)
        def _():
            take(1, second_of(near))
            send_m(1, second_of(near))

    with scope("rotq"):
        qv = bf(acc[:, 0:qr])
        qq = qv * qv
        q_lo = jnp.sum(jnp.where(low, qq, 0.0), axis=-1, keepdims=True) / HEAD_DIM
        q_hi = jnp.sum(jnp.where(low, 0.0, qq), axis=-1, keepdims=True) / HEAD_DIM
        qgain = jnp.concatenate([qgain_ref[...], qgain_ref[...]], axis=1)
        qn = qv * lax.rsqrt(jnp.where(low, q_lo, q_hi) + EPS) * qgain
        qro = rot(qn)
        qrot[0] = jnp.where(low, qro, 0.0).astype(jnp.bfloat16)
        qrot[1] = jnp.where(low, pltpu.roll(qro, HEAD_DIM, 1), 0.0).astype(jnp.bfloat16)

    with scope("o_mate"):
        take(2, s_mate)

        @pl.when(is_end)
        def _():
            send_m(2, s_mate)

        @pl.when(inner)
        def _():
            send_m(2, 2 * z)
            send_m(2, 2 * z + 1)
            send_e(2, s_mate)
            for block, slot in ((xb, 3), (yb, 4)):
                tok2_wait(block)
                tok2_hop(block, slot, c_peer).start()

    span = BLOCK + 2 * WINDOW
    total = plane * line

    def att_block(block):
        begin = pl.multiple_of(block * BLOCK, BLOCK)
        kvb = rim[pl.ds(begin, span), :]
        qb = qrot[:, pl.ds(begin, BLOCK), :].reshape(2 * BLOCK, qr)
        scores = lax.dot_general(
            qb, kvb, (((1,), (1,)), ((), ())), preferred_element_type=jnp.float32
        ) * HEAD_DIM ** (-0.5)
        row = lax.broadcasted_iota(jnp.int32, (2 * BLOCK, span), 0)
        col = lax.broadcasted_iota(jnp.int32, (2 * BLOCK, span), 1)
        gap = row % BLOCK + WINDOW - col
        pos = z * plane + begin - WINDOW + col
        allowed = (gap <= WINDOW) & (gap >= -WINDOW) & (pos >= 0) & (pos < total)
        scores = jnp.where(allowed, scores, NEG_FILL)
        head = lax.broadcasted_iota(jnp.int32, (2 * BLOCK, 1), 0)
        sink = jnp.where(head < BLOCK, sink_ref[0, 2 * y], sink_ref[0, 2 * y + 1])
        peak = jnp.maximum(jnp.max(scores, axis=-1, keepdims=True), sink)
        expo = jnp.exp(scores - peak)
        denom = jnp.sum(expo, axis=-1, keepdims=True) + jnp.exp(sink - peak)
        weights = (expo / denom).astype(jnp.bfloat16)
        o = jnp.dot(weights, kvb, preferred_element_type=jnp.float32)
        low_b = lax.broadcasted_iota(jnp.int32, (BLOCK, qr), 1) < HEAD_DIM
        both = jnp.where(low_b, pltpu.roll(o[:BLOCK], HEAD_DIM, 1), o[BLOCK:])
        mix_a[pl.ds(begin, BLOCK), :] = both.astype(jnp.bfloat16)

    nblocks = plane // BLOCK

    def att_inner(block, carry):
        att_block(block)
        return carry

    with scope("att_in"):
        lax.fori_loop(1, nblocks - 1, att_inner, 0)

    def v_dot(s):
        a = normed[:, :, columns(s)].reshape(plane, depth)
        acc[:, core:] += dot_t(a, win[s, core:])

    def help_dot(s):
        a = normed2[:, :, columns(s)].reshape(plane, depth)
        acc2[...] += dot_t(a, win[s, core:])

    def early(k):
        source = jnp.where(k < 2, z, jnp.where(k < 4, near, mid))
        return 2 * source + k % 2

    with scope("tok2_side"):
        @pl.when(inner)
        def _():
            acc[:, core:] = jnp.zeros((plane, 3 * cr), jnp.float32)
            acc2[...] = jnp.zeros_like(acc2)
            for s in (first_of(mid), second_of(mid)):
                take(1, s)

    with scope("v_dots"):
        @pl.when(inner)
        def _():
            def v_step(k, carry):
                v_dot(early(k))
                return carry

            lax.fori_loop(0, 6, v_step, 0)

    with scope("rim_wait"):
        @pl.when(has_down)
        def _():
            rim_up.wait_recv()

        @pl.when(has_up)
        def _():
            rim_down.wait_recv()

    with scope("att_out"):
        def att_outer(k, carry):
            att_block(k * (nblocks - 1))
            return carry

        lax.fori_loop(0, 2, att_outer, 0)

    pad = 16
    zero_pad = jnp.zeros((pad, cr), jnp.bfloat16)
    taps = conv_ref[y]
    base = core

    def convolve(ref, gate):
        p = ref[...].astype(jnp.float32)
        before = pltpu.roll(p, 1, 0)[pad : pad + plane]
        after = pltpu.roll(p, plane + 2 * pad - 1, 0)[pad : pad + plane]
        mixed = taps[0:1] * before + taps[1:2] * p[pad : pad + plane] + taps[2:3] * after
        return (gate * mixed).astype(jnp.bfloat16)

    prod_up = remote(
        prod.at[pl.ds(plane, pad)], prod.at[pl.ds(0, pad)], prod_send.at[0], prod_recv.at[0], up
    )
    prod_down = remote(
        prod.at[pl.ds(pad, pad)], prod.at[pl.ds(pad + plane, pad)],
        prod_send.at[1], prod_recv.at[1], down,
    )
    low_inner = inner & low_side
    high_inner = inner & (z >= 2)
    g_copy = remote(gated2, mix_c, g_send.at[0], g_recv.at[0], e_peer)

    @pl.when(inner)
    def _():
        with scope("tok2_rest"):
            tok2_wait(db)
            tok2_hop(db, 5, c_peer).start()
            for yy in range(2):
                for xx in range(2):
                    tok2_wait(block_of(yy, xx, 1 - c))

        with scope("help_dots"):
            def help_step(k, carry):
                help_dot(early(k))
                return carry

            lax.fori_loop(0, 6, help_step, 0)

        with scope("far_dots"):
            for s in (first_of(far), second_of(far)):
                take(1, s)

            def far_step(k, carry):
                v_dot(2 * far + k)
                help_dot(2 * far + k)
                return carry

            lax.fori_loop(0, 2, far_step, 0)

        with scope("prod"):
            left = bf(acc[:, base + cr : base + 2 * cr])
            inputs = bf(acc[:, base + 2 * cr : base + 3 * cr])
            prod[pad : pad + plane] = (left * inputs).astype(jnp.bfloat16)

            @pl.when(low_inner)
            def _():
                prod_up.start()

            @pl.when(high_inner)
            def _():
                prod_down.start()

            take(2, first_of(near))
            send_m(2, first_of(near))

            prod2[pad : pad + plane] = (
                bf(acc2[:, cr : 2 * cr]) * bf(acc2[:, 2 * cr : 3 * cr])
            ).astype(jnp.bfloat16)

            @pl.when(z == 1)
            def _():
                prod2[0:pad] = zero_pad
                prod2[pad + plane :] = prod[pad : 2 * pad]
                prod[0:pad] = prod2[plane : plane + pad]

            @pl.when(z != 1)
            def _():
                prod2[0:pad] = prod[plane : plane + pad]
                prod2[pad + plane :] = zero_pad
                prod[pad + plane :] = prod2[pad : 2 * pad]

            gated2[...] = convolve(prod2, bf(acc2[:, 0:cr]))
            g_copy.start()

        with scope("o_fwd"):
            take(2, second_of(near))
            send_m(2, second_of(near))
            take(2, 2 * mid)
            send_e(2, 2 * mid)

        with scope("prod_wait"):
            @pl.when(low_inner)
            def _():
                prod_down.wait_recv()

            @pl.when(high_inner)
            def _():
                prod_up.wait_recv()

            mix_c[...] = convolve(prod, bf(acc[:, base : base + cr]))

    with scope("g_wait"):
        @pl.when(is_end)
        def _():
            g_copy.wait_recv()

    def group(cc):
        spans = [pl.ds(pl.multiple_of((2 * q + cc) * rows, rows), rows) for q in range(4)]
        return [jnp.concatenate([mix_a[w, :], mix_c[w, :]], axis=1) for w in spans]

    mine_rows = jnp.concatenate(group(c), axis=0)
    other_rows = jnp.concatenate(group(1 - c), axis=0)
    rs_copies = []

    def send_rs(src, dst, stage_id, s, peer):
        copy = remote(src, dst, rs_send.at[stage_id, s], rs_recv.at[stage_id, s], peer)
        copy.start()
        rs_copies.append(copy)

    def out_take(i):
        s = 2 * sources[i // 2] + i % 2
        take(2, s)

    def out_forward(i):
        s = 2 * sources[i // 2] + i % 2
        take(2, s)
        send_e(2, s)

    def stage_a(i):
        s = 2 * sources[i // 2] + i % 2
        weight = wout[s]
        s1[s] = jnp.dot(
            other_rows, weight, preferred_element_type=jnp.float32
        ).astype(jnp.bfloat16).reshape(2, 2, rows, depth)
        send_rs(s1.at[s], r1.at[s], 0, s, c_peer)
        keep[s] = jnp.dot(
            mine_rows, weight, preferred_element_type=jnp.float32
        ).reshape(2, 2, rows, depth)

    d_peer = (2 * z + 1 - y, 2 * (1 - x) + c)
    corners = ((1 - y, 1 - x, d_peer), (1 - y, x, y_peer), (y, 1 - x, x_peer))

    def stage_b(i):
        s = 2 * sources[i // 2] + i % 2
        remote(s1.at[s], r1.at[s], rs_send.at[0, s], rs_recv.at[0, s], c_peer).wait_recv()
        for j, (yy, xx, peer) in enumerate(corners):
            s2[s, j] = (keep[s, yy, xx] + r1[s, yy, xx].astype(jnp.float32)).astype(jnp.bfloat16)
            send_rs(s2.at[s, j], r2.at[s, j], 1 + j, s, peer)

    def stage_d(i):
        s = 2 * sources[i // 2] + i % 2
        part = keep[s, y, x] + r1[s, y, x].astype(jnp.float32)
        for j in (1, 2, 0):
            peer = corners[j][2]
            remote(
                s2.at[s, j], r2.at[s, j], rs_send.at[1 + j, s], rs_recv.at[1 + j, s], peer
            ).wait_recv()
        for j in range(3):
            part = part + r2[s, j].astype(jnp.float32)
        out_ref[:, columns(s)] = part.astype(jnp.bfloat16)

    order = (
        ("a", (0, 1, 2)), ("b", (0,)), ("a", (3,)), ("b", (1, 2, 3)), ("f", (5,)),
        ("w", (4,)), ("a", (4,)), ("b", (4,)), ("w", (5,)), ("a", (5,)), ("b", (5,)),
        ("f", (6,)), ("d", (0,)), ("f", (7,)), ("d", (1,)),
        ("w", (6,)), ("a", (6,)), ("b", (6,)), ("d", (2, 3)),
        ("w", (7,)), ("a", (7,)), ("b", (7,)), ("d", (4, 5, 6, 7)),
    )

    for step, places in order:
        for i in places:
            with scope(f"{step}{i}"):
                if step == "w":
                    pl.when(is_end)(functools.partial(out_take, i))
                elif step == "f":
                    pl.when(inner)(functools.partial(out_forward, i))
                elif step == "a":
                    if i in (2, 3):
                        pl.when(is_end)(functools.partial(out_take, i))
                    stage_a(i)
                elif step == "b":
                    stage_b(i)
                else:
                    stage_d(i)

    with scope("sends"):
        for kind in range(3):
            y_hop(kind).wait_send()
        for copy in tok_copies + rs_copies:
            copy.wait_send()

        @pl.when(has_up)
        def _():
            rim_up.wait_send()

        @pl.when(has_down)
        def _():
            rim_down.wait_send()

        for kind in range(3):
            for half in range(2):
                hop(kind, 2 * z + half, m_send, m_peer).wait_send()

        @pl.when(is_end)
        def _():
            end_tok(own_block, 6, 0).wait_send()
            end_tok(own_block, 8, 1).wait_send()
            end_tok(db, 7).wait_send()

        @pl.when(inner)
        def _():
            for slot in range(6):
                tok2_hop(own_block, slot, x_peer).wait_send()
            g_copy.wait_send()
            for half in range(2):
                for kind in range(3):
                    hop(kind, 2 * near + half, m_send, m_peer).wait_send()
                for source in (z, mid, far):
                    for kind in (0, 2):
                        hop(kind, 2 * source + half, e_send, e_peer).wait_send()

        @pl.when(low_inner)
        def _():
            prod_up.wait_send()

        @pl.when(high_inner)
        def _():
            prod_down.wait_send()


def trig_table(total):
    half = HEAD_DIM // 2
    freq = np.float64(ROPE_BASE) ** (-np.arange(half) / half)
    angle = np.arange(total)[:, None] * freq
    cosine, sine = np.cos(angle), np.sin(angle)
    return np.concatenate([cosine, cosine, -sine, sine], axis=1).astype(np.float32)


def fused_device(
    tokens, norm_gain, query_weight, key_weight, value_weight, gate_weight, left_weight,
    input_weight, query_gain, key_gain, sink_logit, conv_weight, out_attention, out_conv,
):
    sp_count = lax.axis_size("sp")
    line = sp_count // 2
    rows, width = tokens.shape
    depth = query_weight.shape[1]
    qr = query_weight.shape[0] // 2
    kr = key_weight.shape[0]
    cr = gate_weight.shape[0] // 2
    fan = qr + 2 * kr + 3 * cr
    plane = 8 * rows
    dims = dict(line=line, rows=rows, depth=depth, qr=qr, kr=kr, cr=cr)
    vm = pl.BlockSpec(memory_space=pltpu.VMEM)
    hb = pl.BlockSpec(memory_space=pl.ANY)
    bf16, f32 = jnp.bfloat16, jnp.float32
    dma = pltpu.SemaphoreType.DMA
    n = sp_count
    scratch = [
        pltpu.VMEM((1, width), f32),
        pltpu.VMEM((1, HEAD_DIM), f32),
        pltpu.VMEM((1, HEAD_DIM), f32),
        pltpu.SMEM((1, 4), f32),
        pltpu.VMEM((2, 3, cr), f32),
        pltpu.VMEM((rows, width), bf16),
        pltpu.VMEM((plane, 2 * HEAD_DIM), f32),
        pltpu.VMEM((fan, depth), bf16),
        pltpu.VMEM((qr + cr, depth), bf16),
        pltpu.VMEM((n, fan, depth), bf16),
        pltpu.VMEM((n, qr + cr, depth), bf16),
        pltpu.VMEM((8, rows, width), bf16),
        pltpu.VMEM((8, rows, width), bf16),
        pltpu.VMEM((plane, fan), f32),
        pltpu.VMEM((plane, 3 * cr), f32),
        pltpu.VMEM((plane + 2 * WINDOW, qr), bf16),
        pltpu.VMEM((plane + 32, cr), bf16),
        pltpu.VMEM((plane + 32, cr), bf16),
        pltpu.VMEM((plane, qr), bf16),
        pltpu.VMEM((plane, cr), bf16),
        pltpu.VMEM((plane, cr), bf16),
        pltpu.VMEM((2, plane, qr), bf16),
        pltpu.VMEM((n, 2, 2, rows, depth), f32),
        pltpu.VMEM((n, 2, 2, rows, depth), bf16),
        pltpu.VMEM((n, 2, 2, rows, depth), bf16),
        pltpu.VMEM((n, 3, rows, depth), bf16),
        pltpu.VMEM((n, 3, rows, depth), bf16),
        dma((23,)), dma((3,)), dma((3, n)), dma((3, n)), dma((3, n)),
        dma((7,)), dma((8,)), dma((9,)), dma((8,)), dma((2,)), dma((2,)), dma((2,)), dma((2,)),
        dma((1,)), dma((1,)), dma((4, n)), dma((4, n)),
    ]
    taps = conv_weight.reshape(3, 2, cr).transpose(1, 0, 2)
    return pl.pallas_call(
        functools.partial(fused_kernel, dims),
        out_shape=jax.ShapeDtypeStruct((rows, width), bf16),
        in_specs=[hb] * 15,
        out_specs=vm,
        scratch_shapes=scratch,
        compiler_params=pltpu.CompilerParams(
            collective_id=0, has_side_effects=True, vmem_limit_bytes=56 * 1024 * 1024
        ),
    )(
        tokens, norm_gain[None, :], query_weight, key_weight, value_weight, gate_weight,
        left_weight, input_weight, query_gain[None, :],
        key_gain[None, :], sink_logit[None, :], taps, out_attention, out_conv,
        jnp.asarray(trig_table(plane * line)),
    )


def local_device(*args):
    tokens, query_weight, key_weight, gate_weight = args[0], args[2], args[3], args[5]
    fits = (
        lax.axis_size("sp") == 8
        and lax.axis_size("tp") == 4
        and query_weight.shape[1] % 128 == 0
        and query_weight.shape[0] == 4 * HEAD_DIM
        and key_weight.shape[0] == HEAD_DIM
        and gate_weight.shape[0] == 256
        and tokens.shape[0] % 16 == 0
        and 8 * tokens.shape[0] % BLOCK == 0
        and 8 * tokens.shape[0] >= 2 * BLOCK
    )
    return fused_device(*args) if fits else per_device(*args)


def solution(mesh):
    in_specs = (
        P(("sp", "tp"), None),
        P(),
        P("tp", "sp"),
        P("tp", "sp"),
        P("tp", "sp"),
        P("tp", "sp"),
        P("tp", "sp"),
        P("tp", "sp"),
        P(),
        P(),
        P("tp"),
        P(None, "tp"),
        P("tp", "sp"),
        P("tp", "sp"),
    )
    out_specs = P(("sp", "tp"), None)
    return jax.shard_map(
        local_device, mesh=mesh, in_specs=in_specs, out_specs=out_specs, check_vma=False
    )
```

```python
import functools

import jax
import jax.numpy as jnp
import numpy as np
from jax import lax
from jax.experimental import pallas as pl
from jax.experimental.pallas import tpu as pltpu
from jax.sharding import PartitionSpec as P

HEAD_DIM = 64
WINDOW = 128
BLOCK = 128


EPS = 1e-06
ROPE_BASE = 10000.0
NEG_FILL = -1e30


def with_halo(cells, sides, width):
    for axis, dim in sides:
        count = lax.axis_size(axis)
        ends = count - 1
        head = lax.slice_in_dim(cells, 0, width, axis=dim)
        tail = lax.slice_in_dim(cells, cells.shape[dim] - width, cells.shape[dim], axis=dim)
        cells = jnp.concatenate(
            [
                lax.ppermute(tail, axis, [(i, (i + 1) % count) for i in range(ends)]),
                cells,
                lax.ppermute(head, axis, [((i + 1) % count, i) for i in range(ends)]),
            ],
            axis=dim,
        )
    return cells


def normalize(values, gain):
    return values * lax.rsqrt(jnp.mean(values * values, axis=-1, keepdims=True) + EPS) * gain


def rotate(values, positions):
    half = values.shape[-1] // 2
    freq = ROPE_BASE ** (-jnp.arange(half, dtype=jnp.float32) / half)
    angle = positions[:, None] * freq
    cosine = jnp.cos(angle)[:, None, :]
    sine = jnp.sin(angle)[:, None, :]
    first = values[..., :half]
    second = values[..., half:]
    return jnp.concatenate(
        [first * cosine - second * sine, second * cosine + first * sine], axis=-1
    )


def project(rows, weight):
    return lax.dot_general(
        rows, weight, (((1,), (1,)), ((), ())), preferred_element_type=jnp.float32
    ).astype(jnp.bfloat16)


def attend(query_rot, key_rim, value_rim, sinks, offset, total):
    count = query_rot.shape[0]
    local_heads = query_rot.shape[1]
    kv_local = key_rim.shape[1]
    group = local_heads // kv_local
    span = BLOCK + 2 * WINDOW
    nblocks = count // BLOCK
    shaped = query_rot.reshape(nblocks, BLOCK, kv_local, group, HEAD_DIM)
    sink_group = sinks.reshape(kv_local, group)[:, :, None]

    def one_block(packed):
        block_index, query_block = packed
        begin = block_index * BLOCK
        key_block = lax.dynamic_slice_in_dim(key_rim, begin, span, 0)
        value_block = lax.dynamic_slice_in_dim(value_rim, begin, span, 0)
        scores = jnp.einsum(
            "qkgd,nkd->kgqn", query_block, key_block, preferred_element_type=jnp.float32
        ) * HEAD_DIM ** (-0.5)
        query_pos = offset + begin + jnp.arange(BLOCK, dtype=jnp.int32)
        key_pos = offset + begin - WINDOW + jnp.arange(span, dtype=jnp.int32)
        allowed = (
            (jnp.abs(query_pos[:, None] - key_pos[None, :]) <= WINDOW)
            & (key_pos >= 0)[None, :]
            & (key_pos < total)[None, :]
        )
        scores = jnp.where(allowed, scores, NEG_FILL)
        top = jnp.maximum(jnp.max(scores, axis=-1), sink_group)
        expo = jnp.exp(scores - top[..., None])
        denom = jnp.sum(expo, axis=-1) + jnp.exp(sink_group - top)
        weights = (expo / denom[..., None]).astype(jnp.bfloat16)
        return jnp.einsum(
            "kgqn,nkd->qkgd", weights, value_block, preferred_element_type=jnp.float32
        ).astype(jnp.bfloat16)

    result = lax.map(one_block, (jnp.arange(nblocks, dtype=jnp.int32), shaped))
    return result.reshape(count, local_heads * HEAD_DIM)


def per_device(
    tokens,
    norm_gain,
    query_weight,
    key_weight,
    value_weight,
    gate_weight,
    left_weight,
    input_weight,
    query_gain,
    key_gain,
    sink_logit,
    conv_weight,
    out_attention,
    out_conv,
):
    sp_count = lax.axis_size("sp")
    sp_place = lax.axis_index("sp")
    gathered = (
        lax.all_gather(query_weight, "sp", axis=1, tiled=True),
        lax.all_gather(key_weight, "sp", axis=1, tiled=True),
        lax.all_gather(value_weight, "sp", axis=1, tiled=True),
        lax.all_gather(gate_weight, "sp", axis=1, tiled=True),
        lax.all_gather(left_weight, "sp", axis=1, tiled=True),
        lax.all_gather(input_weight, "sp", axis=1, tiled=True),
        lax.all_gather(out_attention, "sp", axis=1, tiled=True),
        lax.all_gather(out_conv, "sp", axis=1, tiled=True),
    )
    (
        query_full,
        key_full,
        value_full,
        gate_full,
        left_full,
        input_full,
        attn_out_full,
        conv_out_full,
    ) = gathered
    normed = normalize(tokens.astype(jnp.float32), norm_gain).astype(jnp.bfloat16)
    widths = [
        query_full.shape[0],
        key_full.shape[0],
        value_full.shape[0],
        gate_full.shape[0],
        left_full.shape[0],
        input_full.shape[0],
    ]
    piece = lax.all_gather(normed, "tp", axis=0, tiled=True)
    joined = jnp.concatenate(
        [
            project(piece, weight)
            for weight in (query_full, key_full, value_full, gate_full, left_full, input_full)
        ],
        axis=1,
    )
    count = joined.shape[0]
    bounds = [0]
    for width in widths:
        bounds.append(bounds[-1] + width)
    query, keys, values, gate, left, inputs = [
        joined[:, bounds[place] : bounds[place + 1]] for place in range(6)
    ]
    offset = sp_place * count
    total = count * sp_count
    positions = (offset + jnp.arange(count, dtype=jnp.int32)).astype(jnp.float32)
    local_heads = widths[0] // HEAD_DIM
    kv_local = widths[1] // HEAD_DIM
    query_rot = rotate(
        normalize(query.reshape(count, local_heads, HEAD_DIM).astype(jnp.float32), query_gain),
        positions,
    ).astype(jnp.bfloat16)
    key_rot = rotate(
        normalize(keys.reshape(count, kv_local, HEAD_DIM).astype(jnp.float32), key_gain), positions
    ).astype(jnp.bfloat16)
    key_flat = key_rot.reshape(count, kv_local * HEAD_DIM)
    product = (left.astype(jnp.float32) * inputs.astype(jnp.float32)).astype(jnp.bfloat16)
    kv_width = widths[1]
    pair_rim = with_halo(jnp.concatenate([key_flat, values], axis=1), (("sp", 0),), WINDOW)
    product_rim = with_halo(product, (("sp", 0),), 1)
    rim_rows = pair_rim.shape[0]
    key_rim = pair_rim[:, :kv_width].reshape(rim_rows, kv_local, HEAD_DIM)
    value_rim = pair_rim[:, kv_width:].reshape(rim_rows, kv_local, HEAD_DIM)
    attended = attend(query_rot, key_rim, value_rim, sink_logit, offset, total)
    padded = product_rim.astype(jnp.float32)
    convolved = (
        conv_weight[0] * padded[:-2] + conv_weight[1] * padded[1:-1] + conv_weight[2] * padded[2:]
    )
    gated = (gate.astype(jnp.float32) * convolved).astype(jnp.bfloat16)
    return lax.psum_scatter(
        (
            jnp.dot(attended, attn_out_full, preferred_element_type=jnp.float32)
            + jnp.dot(gated, conv_out_full, preferred_element_type=jnp.float32)
        ).astype(jnp.bfloat16),
        "tp",
        scatter_dimension=0,
        tiled=True,
    )


MESH = pl.DeviceIdType.MESH


def fused_kernel(
    dims,
    tok_hbm, gain_hbm, q_hbm, k_hbm, v_hbm, g_hbm, l_hbm, i_hbm,
    qgain_hbm, kgain_hbm, sink_hbm, conv_hbm, oa_hbm, oc_hbm, trig_hbm,
    out_ref,
    gain_ref, qgain_ref, kgain_ref, sink_ref, conv_ref, tok, trig, stage, ostage, win, wout, normed, normed2, acc, acc2, rim, prod, prod2, mix_a, mix_c, gated2,
    qrot,
    keep, s1, r1, s2, r2,
    local_sem, y_send, w_recv, m_send, e_send,
    tok_send, tok_recv, tok2_send, tok2_recv, rim_send, rim_recv, prod_send, prod_recv, g_send, g_recv,
    rs_send, rs_recv,
):
    scope = jax.named_scope
    line, rows, depth, qr, kr, cr = (
        dims["line"], dims["rows"], dims["depth"], dims["qr"], dims["kr"], dims["cr"]
    )
    sp = lax.axis_index("sp")
    tp = lax.axis_index("tp")
    z, y = sp // 2, sp % 2
    x, c = tp // 2, tp % 2
    y_peer = (2 * z + 1 - y, tp)
    x_peer = (sp, 2 * (1 - x) + c)
    c_peer = (sp, 2 * x + 1 - c)
    low_side = z < 2
    toward = jnp.where(low_side, 1, -1)
    is_end = (z == 0) | (z == line - 1)
    inner = (z > 0) & (z < line - 1)
    m_plane = z + toward
    e_plane = jnp.where(inner, z - toward, m_plane)
    m_peer = (2 * m_plane + y, tp)
    e_peer = (2 * e_plane + y, tp)
    near = jnp.where(inner, z - toward, z + toward)
    mid = jnp.where(inner, z + toward, z + 2 * toward)
    far = jnp.where(inner, z + 2 * toward, z + 3 * toward)
    sources = (z, near, mid, far)
    s_own = sp
    s_mate = 2 * z + 1 - y
    plane = 8 * rows
    core = qr + 2 * kr

    barrier = pltpu.get_barrier_semaphore()
    for peer in (y_peer, x_peer, c_peer, m_peer):
        pl.semaphore_signal(barrier, inc=1, device_id=peer, device_id_type=MESH)

    @pl.when(inner)
    def _():
        pl.semaphore_signal(barrier, inc=1, device_id=e_peer, device_id_type=MESH)

    counter = [0]

    def local(src, dst):
        copy = pltpu.make_async_copy(src, dst, local_sem.at[counter[0]])
        counter[0] += 1
        copy.start()
        return copy

    def core_pieces(which, dst):
        q0 = pl.multiple_of(which * qr, qr)
        return [
            local(q_hbm.at[pl.ds(q0, qr)], dst.at[0:qr]),
            local(k_hbm, dst.at[qr : qr + kr]),
            local(v_hbm, dst.at[qr + kr : qr + 2 * kr]),
        ]

    def conv_pieces(which, dst):
        c0 = pl.multiple_of(which * cr, cr)
        return [
            local(g_hbm.at[pl.ds(c0, cr)], dst.at[core : core + cr]),
            local(l_hbm.at[pl.ds(c0, cr)], dst.at[core + cr : core + 2 * cr]),
            local(i_hbm.at[pl.ds(c0, cr)], dst.at[core + 2 * cr : core + 3 * cr]),
        ]

    def out_pieces(which, dst):
        q0, c0 = pl.multiple_of(which * qr, qr), pl.multiple_of(which * cr, cr)
        return [
            local(oa_hbm.at[pl.ds(q0, qr)], dst.at[0:qr]),
            local(oc_hbm.at[pl.ds(c0, cr)], dst.at[qr : qr + cr]),
        ]

    loads = core_pieces(y, win.at[s_own]) + core_pieces(1 - y, stage)
    tok_loads = [local(tok_hbm, tok), local(gain_hbm, gain_ref)]
    loads += conv_pieces(y, win.at[s_own]) + conv_pieces(1 - y, stage)
    loads += out_pieces(y, wout.at[s_own]) + out_pieces(1 - y, ostage)
    side_copies = [
        local(trig_hbm.at[pl.ds(pl.multiple_of(z * plane, plane), plane)], trig),
        local(qgain_hbm, qgain_ref),
        local(kgain_hbm, kgain_ref),
        local(sink_hbm, sink_ref),
        local(conv_hbm, conv_ref),
    ]

    with scope("barrier"):
        pl.semaphore_wait(barrier, 4 + inner.astype(jnp.int32))

    def remote(src, dst, send, recv, peer):
        return pltpu.make_async_remote_copy(
            src_ref=src, dst_ref=dst, send_sem=send, recv_sem=recv,
            device_id=peer, device_id_type=MESH,
        )

    def chunk(kind, s):
        if kind > 1:
            return wout.at[s, 0:qr] if kind == 2 else wout.at[s, qr : qr + cr]
        return win.at[s, 0:core] if kind == 0 else win.at[s, core : core + 3 * cr]

    def hop(kind, s, sends, peer):
        return remote(chunk(kind, s), chunk(kind, s), sends.at[kind, s], w_recv.at[kind, s], peer)

    def send_m(kind, s):
        hop(kind, s, m_send, m_peer).start()

    def send_e(kind, s):
        hop(kind, s, e_send, e_peer).start()

    def take(kind, s):
        hop(kind, s, m_send, m_peer).wait_recv()

    def y_hop(kind):
        if kind > 1:
            src = ostage.at[0:qr] if kind == 2 else ostage.at[qr : qr + cr]
        else:
            src = stage.at[0:core] if kind == 0 else stage.at[core : core + 3 * cr]
        return remote(src, chunk(kind, s_own), y_send.at[kind], w_recv.at[kind, s_own], y_peer)

    def out_hop(s, *sends):
        for kind in (2, 3):
            take(kind, s)
            for send in sends:
                send(kind, s)

    def out_send(s, send):
        send(2, s)
        send(3, s)

    def first_of(source):
        return 2 * source + y

    def second_of(source):
        return 2 * source + 1 - y

    for copy in loads:
        copy.wait()
    send_m(0, s_own)

    @pl.when(inner)
    def _():
        send_e(0, s_own)

    y_hop(0).start()

    @pl.when(inner)
    def _():
        send_m(1, s_own)
        out_send(s_own, send_e)

    with scope("norm"):
        for copy in tok_loads:
            copy.wait()
        t = tok[...].astype(jnp.float32)
        t = t * lax.rsqrt(jnp.mean(t * t, axis=-1, keepdims=True) + EPS) * gain_ref[...]

        def block_of(yy, xx, cc):
            return 4 * yy + 2 * xx + cc

        own_block = block_of(y, x, c)
        xb = block_of(y, 1 - x, c)
        yb = block_of(1 - y, x, c)
        db = block_of(1 - y, 1 - x, c)
        normed[own_block] = t.astype(jnp.bfloat16)

    def part(ref, block, half):
        if half == 2:
            return ref.at[block]
        return ref.at[block, half * rows // 2 : (half + 1) * rows // 2]

    def tok_hop(block, half, slot, peer):
        here = part(normed, block, half)
        return remote(here, here, tok_send.at[slot], tok_recv.at[half, block], peer)

    def end_tok(block, half, slot):
        return remote(
            part(normed, block, half), part(normed2, block, half), tok2_send.at[slot],
            tok2_recv.at[half, block], m_peer,
        )

    def tok2_hop(block, half, slot, peer):
        here = part(normed2, block, half)
        return remote(here, here, tok2_send.at[slot], tok2_recv.at[half, block], peer)

    tok_copies = []

    def tok_go(block, half, peer):
        copy = tok_hop(block, half, len(tok_copies), peer)
        copy.start()
        tok_copies.append(copy)

    def tok_wait(block, half):
        tok_hop(block, half, 0, x_peer).wait_recv()

    def tok2_wait(block, half):
        tok2_hop(block, half, 0, x_peer).wait_recv()

    @pl.when(is_end)
    def _():
        end_tok(own_block, 0, 6).start()

    tok_go(own_block, 1, x_peer)
    tok_go(own_block, 0, y_peer)
    tok_go(own_block, 0, x_peer)
    tok_go(own_block, 1, y_peer)
    y_hop(1).start()
    tok_go(own_block, 2, c_peer)

    with scope("c_mate"):
        take(0, s_mate)
        send_m(0, s_mate)

        @pl.when(inner)
        def _():
            send_e(0, s_mate)
            take(0, first_of(near))
            send_m(0, first_of(near))
            take(0, first_of(mid))
            send_e(0, first_of(mid))

        @pl.when(is_end)
        def _():
            end_tok(own_block, 1, 7).start()
            send_m(1, s_own)

    with scope("tok_xy"):
        tok_wait(xb, 1)
        tok_go(xb, 1, y_peer)
        tok_wait(yb, 0)
        tok_go(yb, 0, x_peer)
        tok_wait(xb, 0)
        tok_go(xb, 2, c_peer)
        tok_wait(yb, 1)
        tok_go(yb, 2, c_peer)

    with scope("c_fwd"):
        @pl.when(inner)
        def _():
            take(0, second_of(mid))
            send_e(0, second_of(mid))
            take(0, second_of(near))
            send_m(0, second_of(near))

    with scope("tok2_own"):
        @pl.when(inner)
        def _():
            tok2_wait(own_block, 0)
            tok2_wait(own_block, 1)
            tok2_hop(own_block, 2, 0, x_peer).start()
            tok2_hop(own_block, 2, 1, y_peer).start()
            tok2_hop(own_block, 2, 2, c_peer).start()

    y_hop(2).start()
    y_hop(3).start()

    with scope("far1"):
        @pl.when(inner)
        def _():
            take(0, first_of(far))
            send_e(0, first_of(far))

    with scope("v_mate"):
        take(1, s_mate)
        send_m(1, s_mate)

    with scope("far2"):
        @pl.when(inner)
        def _():
            take(0, second_of(far))
            send_e(0, second_of(far))

    with scope("tok_db"):
        tok_wait(db, 0)
        tok_wait(db, 1)
        tok_go(db, 2, c_peer)

        @pl.when(is_end)
        def _():
            end_tok(db, 0, 8).start()
            end_tok(db, 1, 9).start()

    with scope("v_near1"):
        @pl.when(inner)
        def _():
            take(1, first_of(near))
            send_m(1, first_of(near))

    with scope("tok_rest"):
        for yy in range(2):
            for xx in range(2):
                tok_wait(block_of(yy, xx, 1 - c), 2)

    def columns(s):
        return pl.ds(pl.multiple_of(s * depth, depth), depth)

    def dot_t(a, w):
        return lax.dot_general(a, w, (((1,), (1,)), ((), ())), preferred_element_type=jnp.float32)

    def plane_dots(tokens, into, cols, weight_rows, source, add):
        total = into[:, cols] if add else None
        for half in range(2):
            s = 2 * source + half
            a = tokens[:, :, columns(s)].reshape(plane, depth)
            product = dot_t(a, win[s, weight_rows])
            total = product if total is None else total + product
        into[:, cols] = total

    conv_rows = slice(core, core + 3 * cr)

    def early_dots(tokens, into, cols, weight_rows, count):
        plane_dots(tokens, into, cols, weight_rows, z, False)

        def step(k, carry):
            source = jnp.where(k == 1, near, jnp.where(k == 2, mid, far))
            plane_dots(tokens, into, cols, weight_rows, source, True)
            return carry

        lax.fori_loop(1, count, step, 0)

    with scope("c_dots"):
        @pl.when(is_end)
        def _():
            for source in (near, mid, far):
                for s in (first_of(source), second_of(source)):
                    take(0, s)

        early_dots(normed, acc, slice(0, core), slice(0, core), line)

    with scope("rot"):
        for copy in side_copies:
            copy.wait()
        lane = lax.broadcasted_iota(jnp.int32, (plane, qr), 1)
        half_dim = HEAD_DIM // 2
        table = trig[...]
        cos2 = jnp.where(lane < HEAD_DIM, table, pltpu.roll(table, HEAD_DIM, 1))
        sin2 = jnp.where(lane < HEAD_DIM, pltpu.roll(table, HEAD_DIM, 1), table)
        low = lane < HEAD_DIM
        first_half = lane % HEAD_DIM < half_dim

        def rot(v):
            partner = jnp.where(
                first_half, pltpu.roll(v, qr - half_dim, 1), pltpu.roll(v, half_dim, 1)
            )
            return v * cos2 + partner * sin2

        def bf(v):
            return v.astype(jnp.bfloat16).astype(jnp.float32)

        kv = bf(acc[:, qr : 2 * qr])
        ksq = jnp.sum(jnp.where(low, kv * kv, 0.0), axis=-1, keepdims=True) / HEAD_DIM
        kgain = jnp.concatenate([kgain_ref[...], kgain_ref[...]], axis=1)
        kn = kv * lax.rsqrt(ksq + EPS) * kgain
        krot = rot(kn)
        rim[WINDOW : WINDOW + plane, :] = jnp.where(low, krot, kv).astype(jnp.bfloat16)

    bottom = pl.ds(WINDOW, WINDOW)
    top = pl.ds(plane, WINDOW)
    up = (jnp.minimum(2 * (z + 1) + y, 2 * line - 1), tp)
    down = (jnp.maximum(2 * (z - 1) + y, 0), tp)
    has_up = z < line - 1
    has_down = z > 0
    rim_up = remote(rim.at[top], rim.at[pl.ds(0, WINDOW)], rim_send.at[0], rim_recv.at[0], up)
    rim_down = remote(
        rim.at[bottom], rim.at[pl.ds(WINDOW + plane, WINDOW)], rim_send.at[1], rim_recv.at[1], down
    )

    @pl.when(has_up)
    def _():
        rim_up.start()

    @pl.when(has_down)
    def _():
        rim_down.start()

    zero_rim = jnp.zeros((WINDOW, qr), jnp.bfloat16)

    @pl.when(z == 0)
    def _():
        rim[0:WINDOW] = zero_rim

    @pl.when(z == line - 1)
    def _():
        rim[WINDOW + plane :] = zero_rim

    with scope("rotq"):
        qv = bf(acc[:, 0:qr])
        qq = qv * qv
        q_lo = jnp.sum(jnp.where(low, qq, 0.0), axis=-1, keepdims=True) / HEAD_DIM
        q_hi = jnp.sum(jnp.where(low, 0.0, qq), axis=-1, keepdims=True) / HEAD_DIM
        qgain = jnp.concatenate([qgain_ref[...], qgain_ref[...]], axis=1)
        qn = qv * lax.rsqrt(jnp.where(low, q_lo, q_hi) + EPS) * qgain
        qro = rot(qn)
        qrot[0] = jnp.where(low, qro, 0.0).astype(jnp.bfloat16)
        qrot[1] = jnp.where(low, pltpu.roll(qro, HEAD_DIM, 1), 0.0).astype(jnp.bfloat16)

    with scope("tok2_xb"):
        @pl.when(inner)
        def _():
            tok2_wait(xb, 2)
            tok2_hop(xb, 2, 3, c_peer).start()

    span = BLOCK + 2 * WINDOW
    total = plane * line

    def att_block(block):
        begin = pl.multiple_of(block * BLOCK, BLOCK)
        kvb = rim[pl.ds(begin, span), :]
        qb = qrot[:, pl.ds(begin, BLOCK), :].reshape(2 * BLOCK, qr)
        scores = lax.dot_general(
            qb, kvb, (((1,), (1,)), ((), ())), preferred_element_type=jnp.float32
        ) * HEAD_DIM ** (-0.5)
        row = lax.broadcasted_iota(jnp.int32, (2 * BLOCK, span), 0)
        col = lax.broadcasted_iota(jnp.int32, (2 * BLOCK, span), 1)
        gap = row % BLOCK + WINDOW - col
        pos = z * plane + begin - WINDOW + col
        allowed = (gap <= WINDOW) & (gap >= -WINDOW) & (pos >= 0) & (pos < total)
        scores = jnp.where(allowed, scores, NEG_FILL)
        head = lax.broadcasted_iota(jnp.int32, (2 * BLOCK, 1), 0)
        sink = jnp.where(head < BLOCK, sink_ref[0, 2 * y], sink_ref[0, 2 * y + 1])
        peak = jnp.maximum(jnp.max(scores, axis=-1, keepdims=True), sink)
        expo = jnp.exp(scores - peak)
        denom = jnp.sum(expo, axis=-1, keepdims=True) + jnp.exp(sink - peak)
        weights = (expo / denom).astype(jnp.bfloat16)
        o = jnp.dot(weights, kvb, preferred_element_type=jnp.float32)
        low_b = lax.broadcasted_iota(jnp.int32, (BLOCK, qr), 1) < HEAD_DIM
        both = jnp.where(low_b, pltpu.roll(o[:BLOCK], HEAD_DIM, 1), o[BLOCK:])
        mix_a[pl.ds(begin, BLOCK), :] = both.astype(jnp.bfloat16)

    nblocks = plane // BLOCK

    def att_inner(block, carry):
        att_block(block)
        return carry

    with scope("att_in"):
        lax.fori_loop(1, nblocks - 1, att_inner, 0)

    with scope("tok2_yb"):
        @pl.when(inner)
        def _():
            tok2_wait(yb, 2)
            tok2_hop(yb, 2, 4, c_peer).start()

    with scope("v_near2"):
        @pl.when(inner)
        def _():
            take(1, second_of(near))
            send_m(1, second_of(near))

    with scope("o_mate"):
        @pl.when(is_end)
        def _():
            out_send(s_own, send_m)
            out_hop(s_mate, send_m)

        @pl.when(inner)
        def _():
            out_send(s_own, send_m)
            out_hop(s_mate, send_e)

    with scope("v_mid"):
        @pl.when(inner)
        def _():
            for s in (first_of(mid), second_of(mid)):
                take(1, s)

    with scope("v_dots"):
        @pl.when(inner)
        def _():
            early_dots(normed, acc, conv_rows, conv_rows, 3)

    with scope("tok2_db"):
        @pl.when(inner)
        def _():
            tok2_wait(db, 0)
            tok2_wait(db, 1)
            tok2_hop(db, 2, 5, c_peer).start()

    def attend_edges():
        with scope("rim_wait"):
            @pl.when(has_down)
            def _():
                rim_up.wait_recv()

            @pl.when(has_up)
            def _():
                rim_down.wait_recv()

        with scope("att_out"):
            def att_outer(k, carry):
                att_block(k * (nblocks - 1))
                return carry

            lax.fori_loop(0, 2, att_outer, 0)

    pad = 16
    zero_pad = jnp.zeros((pad, cr), jnp.bfloat16)
    taps = conv_ref[y]
    base = core

    def convolve(ref, gate):
        p = ref[...].astype(jnp.float32)
        before = pltpu.roll(p, 1, 0)[pad : pad + plane]
        after = pltpu.roll(p, plane + 2 * pad - 1, 0)[pad : pad + plane]
        mixed = taps[0:1] * before + taps[1:2] * p[pad : pad + plane] + taps[2:3] * after
        return (gate * mixed).astype(jnp.bfloat16)

    prod_up = remote(
        prod.at[pl.ds(plane, pad)], prod.at[pl.ds(0, pad)], prod_send.at[0], prod_recv.at[0], up
    )
    prod_down = remote(
        prod.at[pl.ds(pad, pad)], prod.at[pl.ds(pad + plane, pad)],
        prod_send.at[1], prod_recv.at[1], down,
    )
    low_inner = inner & low_side
    high_inner = inner & (z >= 2)
    g_copy = remote(gated2, mix_c, g_send.at[0], g_recv.at[0], e_peer)

    @pl.when(inner)
    def _():
        with scope("tok2_rest"):
            for yy in range(2):
                for xx in range(2):
                    tok2_wait(block_of(yy, xx, 1 - c), 2)

        with scope("help_dots"):
            early_dots(normed2, acc2, slice(0, 3 * cr), conv_rows, 3)

        with scope("far_dots"):
            for s in (first_of(far), second_of(far)):
                take(1, s)
            plane_dots(normed2, acc2, slice(0, 3 * cr), conv_rows, far, True)
            plane_dots(normed, acc, conv_rows, conv_rows, far, True)

        with scope("prod"):
            left = bf(acc[:, base + cr : base + 2 * cr])
            inputs = bf(acc[:, base + 2 * cr : base + 3 * cr])
            prod[pad : pad + plane] = (left * inputs).astype(jnp.bfloat16)

            @pl.when(low_inner)
            def _():
                prod_up.start()

            @pl.when(high_inner)
            def _():
                prod_down.start()

            out_send(s_mate, send_m)
            out_hop(first_of(near), send_m)

            prod2[pad : pad + plane] = (
                bf(acc2[:, cr : 2 * cr]) * bf(acc2[:, 2 * cr : 3 * cr])
            ).astype(jnp.bfloat16)

            @pl.when(z == 1)
            def _():
                prod2[0:pad] = zero_pad
                prod2[pad + plane :] = prod[pad : 2 * pad]
                prod[0:pad] = prod2[plane : plane + pad]

            @pl.when(z != 1)
            def _():
                prod2[0:pad] = prod[plane : plane + pad]
                prod2[pad + plane :] = zero_pad
                prod[pad + plane :] = prod2[pad : 2 * pad]

            gated2[...] = convolve(prod2, bf(acc2[:, 0:cr]))
            g_copy.start()

        attend_edges()

        with scope("o_fwd"):
            out_hop(second_of(near), send_m)
            out_hop(first_of(mid), send_e)

        with scope("prod_wait"):
            @pl.when(low_inner)
            def _():
                prod_down.wait_recv()

            @pl.when(high_inner)
            def _():
                prod_up.wait_recv()

            mix_c[...] = convolve(prod, bf(acc[:, base : base + cr]))

    @pl.when(is_end)
    def _():
        attend_edges()
        with scope("g_wait"):
            g_copy.wait_recv()

    def group(cc):
        spans = [pl.ds(pl.multiple_of((2 * q + cc) * rows, rows), rows) for q in range(4)]
        return [jnp.concatenate([mix_a[w, :], mix_c[w, :]], axis=1) for w in spans]

    mine_rows = jnp.concatenate(group(c), axis=0)
    other_rows = jnp.concatenate(group(1 - c), axis=0)
    rs_copies = []

    def send_rs(src, dst, stage_id, s, peer):
        copy = remote(src, dst, rs_send.at[stage_id, s], rs_recv.at[stage_id, s], peer)
        copy.start()
        rs_copies.append(copy)

    def out_take(i):
        s = 2 * sources[i // 2] + i % 2
        out_hop(s)

    def out_forward(i):
        source = sources[i // 2]
        out_hop(first_of(source) if i % 2 == 0 else second_of(source), send_e)

    def stage_a(i):
        s = 2 * sources[i // 2] + i % 2
        weight = wout[s]
        s1[s] = jnp.dot(
            other_rows, weight, preferred_element_type=jnp.float32
        ).astype(jnp.bfloat16).reshape(2, 2, rows, depth)
        send_rs(s1.at[s], r1.at[s], 0, s, c_peer)
        keep[s] = jnp.dot(
            mine_rows, weight, preferred_element_type=jnp.float32
        ).reshape(2, 2, rows, depth)

    d_peer = (2 * z + 1 - y, 2 * (1 - x) + c)
    corners = ((1 - y, 1 - x, d_peer), (1 - y, x, y_peer), (y, 1 - x, x_peer))

    def stage_b(i):
        s = 2 * sources[i // 2] + i % 2
        remote(s1.at[s], r1.at[s], rs_send.at[0, s], rs_recv.at[0, s], c_peer).wait_recv()
        for j, (yy, xx, peer) in enumerate(corners):
            s2[s, j] = (keep[s, yy, xx] + r1[s, yy, xx].astype(jnp.float32)).astype(jnp.bfloat16)
            send_rs(s2.at[s, j], r2.at[s, j], 1 + j, s, peer)

    def stage_d(i):
        s = 2 * sources[i // 2] + i % 2
        piece = keep[s, y, x] + r1[s, y, x].astype(jnp.float32)
        for j in (1, 2, 0):
            peer = corners[j][2]
            remote(
                s2.at[s, j], r2.at[s, j], rs_send.at[1 + j, s], rs_recv.at[1 + j, s], peer
            ).wait_recv()
        for j in range(3):
            piece = piece + r2[s, j].astype(jnp.float32)
        out_ref[:, columns(s)] = piece.astype(jnp.bfloat16)

    order = (
        ("a", (0, 1)), ("f", (5,)), ("b", (0,)), ("a", (2,)), ("b", (1,)), ("a", (3,)),
        ("b", (2, 3)), ("w", (4,)), ("a", (4,)), ("f", (6,)), ("b", (4,)),
        ("w", (5,)), ("a", (5,)), ("b", (5,)), ("f", (7,)), ("w", (6,)), ("a", (6,)), ("b", (6,)),
        ("d", (0, 1)), ("w", (7,)), ("a", (7,)), ("b", (7,)),
        ("d", (2, 3, 4, 5, 6, 7)),
    )

    for step, places in order:
        for i in places:
            with scope(f"{step}{i}"):
                if step == "w":
                    pl.when(is_end)(functools.partial(out_take, i))
                elif step == "f":
                    pl.when(inner)(functools.partial(out_forward, i))
                elif step == "a":
                    if i in (2, 3):
                        pl.when(is_end)(functools.partial(out_take, i))
                    stage_a(i)
                elif step == "b":
                    stage_b(i)
                else:
                    stage_d(i)

    with scope("sends"):
        for kind in range(4):
            y_hop(kind).wait_send()
        for copy in tok_copies + rs_copies:
            copy.wait_send()

        @pl.when(has_up)
        def _():
            rim_up.wait_send()

        @pl.when(has_down)
        def _():
            rim_down.wait_send()

        for kind in range(4):
            for half in range(2):
                hop(kind, 2 * z + half, m_send, m_peer).wait_send()

        @pl.when(is_end)
        def _():
            for half in range(2):
                end_tok(own_block, half, 6 + half).wait_send()
                end_tok(db, half, 8 + half).wait_send()

        @pl.when(inner)
        def _():
            for slot in range(6):
                tok2_hop(own_block, 2, slot, x_peer).wait_send()
            g_copy.wait_send()
            for half in range(2):
                for kind in range(4):
                    hop(kind, 2 * near + half, m_send, m_peer).wait_send()
                for source in (z, mid, far):
                    for kind in (0, 2, 3):
                        hop(kind, 2 * source + half, e_send, e_peer).wait_send()

        @pl.when(low_inner)
        def _():
            prod_up.wait_send()

        @pl.when(high_inner)
        def _():
            prod_down.wait_send()


def trig_table(total):
    half = HEAD_DIM // 2
    freq = np.float64(ROPE_BASE) ** (-np.arange(half) / half)
    angle = np.arange(total)[:, None] * freq
    cosine, sine = np.cos(angle), np.sin(angle)
    return np.concatenate([cosine, cosine, -sine, sine], axis=1).astype(np.float32)


def fused_device(
    tokens, norm_gain, query_weight, key_weight, value_weight, gate_weight, left_weight,
    input_weight, query_gain, key_gain, sink_logit, conv_weight, out_attention, out_conv,
):
    sp_count = lax.axis_size("sp")
    line = sp_count // 2
    rows, width = tokens.shape
    depth = query_weight.shape[1]
    qr = query_weight.shape[0] // 2
    kr = key_weight.shape[0]
    cr = gate_weight.shape[0] // 2
    fan = qr + 2 * kr + 3 * cr
    plane = 8 * rows
    dims = dict(line=line, rows=rows, depth=depth, qr=qr, kr=kr, cr=cr)
    vm = pl.BlockSpec(memory_space=pltpu.VMEM)
    hb = pl.BlockSpec(memory_space=pl.ANY)
    bf16, f32 = jnp.bfloat16, jnp.float32
    dma = pltpu.SemaphoreType.DMA
    n = sp_count
    scratch = [
        pltpu.VMEM((1, width), f32),
        pltpu.VMEM((1, HEAD_DIM), f32),
        pltpu.VMEM((1, HEAD_DIM), f32),
        pltpu.SMEM((1, 4), f32),
        pltpu.VMEM((2, 3, cr), f32),
        pltpu.VMEM((rows, width), bf16),
        pltpu.VMEM((plane, 2 * HEAD_DIM), f32),
        pltpu.VMEM((fan, depth), bf16),
        pltpu.VMEM((qr + cr, depth), bf16),
        pltpu.VMEM((n, fan, depth), bf16),
        pltpu.VMEM((n, qr + cr, depth), bf16),
        pltpu.VMEM((8, rows, width), bf16),
        pltpu.VMEM((8, rows, width), bf16),
        pltpu.VMEM((plane, fan), f32),
        pltpu.VMEM((plane, 3 * cr), f32),
        pltpu.VMEM((plane + 2 * WINDOW, qr), bf16),
        pltpu.VMEM((plane + 32, cr), bf16),
        pltpu.VMEM((plane + 32, cr), bf16),
        pltpu.VMEM((plane, qr), bf16),
        pltpu.VMEM((plane, cr), bf16),
        pltpu.VMEM((plane, cr), bf16),
        pltpu.VMEM((2, plane, qr), bf16),
        pltpu.VMEM((n, 2, 2, rows, depth), f32),
        pltpu.VMEM((n, 2, 2, rows, depth), bf16),
        pltpu.VMEM((n, 2, 2, rows, depth), bf16),
        pltpu.VMEM((n, 3, rows, depth), bf16),
        pltpu.VMEM((n, 3, rows, depth), bf16),
        dma((23,)), dma((4,)), dma((4, n)), dma((4, n)), dma((4, n)),
        dma((10,)), dma((3, 8)), dma((10,)), dma((3, 8)), dma((2,)), dma((2,)), dma((2,)), dma((2,)),
        dma((1,)), dma((1,)), dma((4, n)), dma((4, n)),
    ]
    taps = conv_weight.reshape(3, 2, cr).transpose(1, 0, 2)
    return pl.pallas_call(
        functools.partial(fused_kernel, dims),
        out_shape=jax.ShapeDtypeStruct((rows, width), bf16),
        in_specs=[hb] * 15,
        out_specs=vm,
        scratch_shapes=scratch,
        compiler_params=pltpu.CompilerParams(
            collective_id=0, has_side_effects=True, vmem_limit_bytes=56 * 1024 * 1024
        ),
    )(
        tokens, norm_gain[None, :], query_weight, key_weight, value_weight, gate_weight,
        left_weight, input_weight, query_gain[None, :],
        key_gain[None, :], sink_logit[None, :], taps, out_attention, out_conv,
        jnp.asarray(trig_table(plane * line)),
    )


def local_device(*args):
    tokens, query_weight, key_weight, gate_weight = args[0], args[2], args[3], args[5]
    fits = (
        lax.axis_size("sp") == 8
        and lax.axis_size("tp") == 4
        and query_weight.shape[1] % 128 == 0
        and query_weight.shape[0] == 4 * HEAD_DIM
        and key_weight.shape[0] == HEAD_DIM
        and gate_weight.shape[0] == 256
        and tokens.shape[0] % 32 == 0
        and 8 * tokens.shape[0] % BLOCK == 0
        and 8 * tokens.shape[0] >= 2 * BLOCK
    )
    return fused_device(*args) if fits else per_device(*args)


def solution(mesh):
    in_specs = (
        P(("sp", "tp"), None),
        P(),
        P("tp", "sp"),
        P("tp", "sp"),
        P("tp", "sp"),
        P("tp", "sp"),
        P("tp", "sp"),
        P("tp", "sp"),
        P(),
        P(),
        P("tp"),
        P(None, "tp"),
        P("tp", "sp"),
        P("tp", "sp"),
    )
    out_specs = P(("sp", "tp"), None)
    return jax.shard_map(
        local_device, mesh=mesh, in_specs=in_specs, out_specs=out_specs, check_vma=False
    )
```

```python
import functools

import jax
import jax.numpy as jnp
import numpy as np
from jax import lax
from jax.experimental import pallas as pl
from jax.experimental.pallas import tpu as pltpu
from jax.sharding import PartitionSpec as P

HEAD_DIM = 64
WINDOW = 128
BLOCK = 128


EPS = 1e-06
ROPE_BASE = 10000.0
NEG_FILL = -1e30


def with_halo(cells, sides, width):
    for axis, dim in sides:
        count = lax.axis_size(axis)
        ends = count - 1
        head = lax.slice_in_dim(cells, 0, width, axis=dim)
        tail = lax.slice_in_dim(cells, cells.shape[dim] - width, cells.shape[dim], axis=dim)
        cells = jnp.concatenate(
            [
                lax.ppermute(tail, axis, [(i, (i + 1) % count) for i in range(ends)]),
                cells,
                lax.ppermute(head, axis, [((i + 1) % count, i) for i in range(ends)]),
            ],
            axis=dim,
        )
    return cells


def normalize(values, gain):
    return values * lax.rsqrt(jnp.mean(values * values, axis=-1, keepdims=True) + EPS) * gain


def rotate(values, positions):
    half = values.shape[-1] // 2
    freq = ROPE_BASE ** (-jnp.arange(half, dtype=jnp.float32) / half)
    angle = positions[:, None] * freq
    cosine = jnp.cos(angle)[:, None, :]
    sine = jnp.sin(angle)[:, None, :]
    first = values[..., :half]
    second = values[..., half:]
    return jnp.concatenate(
        [first * cosine - second * sine, second * cosine + first * sine], axis=-1
    )


def project(rows, weight):
    return lax.dot_general(
        rows, weight, (((1,), (1,)), ((), ())), preferred_element_type=jnp.float32
    ).astype(jnp.bfloat16)


def attend(query_rot, key_rim, value_rim, sinks, offset, total):
    count = query_rot.shape[0]
    local_heads = query_rot.shape[1]
    kv_local = key_rim.shape[1]
    group = local_heads // kv_local
    span = BLOCK + 2 * WINDOW
    nblocks = count // BLOCK
    shaped = query_rot.reshape(nblocks, BLOCK, kv_local, group, HEAD_DIM)
    sink_group = sinks.reshape(kv_local, group)[:, :, None]

    def one_block(packed):
        block_index, query_block = packed
        begin = block_index * BLOCK
        key_block = lax.dynamic_slice_in_dim(key_rim, begin, span, 0)
        value_block = lax.dynamic_slice_in_dim(value_rim, begin, span, 0)
        scores = jnp.einsum(
            "qkgd,nkd->kgqn", query_block, key_block, preferred_element_type=jnp.float32
        ) * HEAD_DIM ** (-0.5)
        query_pos = offset + begin + jnp.arange(BLOCK, dtype=jnp.int32)
        key_pos = offset + begin - WINDOW + jnp.arange(span, dtype=jnp.int32)
        allowed = (
            (jnp.abs(query_pos[:, None] - key_pos[None, :]) <= WINDOW)
            & (key_pos >= 0)[None, :]
            & (key_pos < total)[None, :]
        )
        scores = jnp.where(allowed, scores, NEG_FILL)
        top = jnp.maximum(jnp.max(scores, axis=-1), sink_group)
        expo = jnp.exp(scores - top[..., None])
        denom = jnp.sum(expo, axis=-1) + jnp.exp(sink_group - top)
        weights = (expo / denom[..., None]).astype(jnp.bfloat16)
        return jnp.einsum(
            "kgqn,nkd->qkgd", weights, value_block, preferred_element_type=jnp.float32
        ).astype(jnp.bfloat16)

    result = lax.map(one_block, (jnp.arange(nblocks, dtype=jnp.int32), shaped))
    return result.reshape(count, local_heads * HEAD_DIM)


def per_device(
    tokens,
    norm_gain,
    query_weight,
    key_weight,
    value_weight,
    gate_weight,
    left_weight,
    input_weight,
    query_gain,
    key_gain,
    sink_logit,
    conv_weight,
    out_attention,
    out_conv,
):
    sp_count = lax.axis_size("sp")
    sp_place = lax.axis_index("sp")
    gathered = (
        lax.all_gather(query_weight, "sp", axis=1, tiled=True),
        lax.all_gather(key_weight, "sp", axis=1, tiled=True),
        lax.all_gather(value_weight, "sp", axis=1, tiled=True),
        lax.all_gather(gate_weight, "sp", axis=1, tiled=True),
        lax.all_gather(left_weight, "sp", axis=1, tiled=True),
        lax.all_gather(input_weight, "sp", axis=1, tiled=True),
        lax.all_gather(out_attention, "sp", axis=1, tiled=True),
        lax.all_gather(out_conv, "sp", axis=1, tiled=True),
    )
    (
        query_full,
        key_full,
        value_full,
        gate_full,
        left_full,
        input_full,
        attn_out_full,
        conv_out_full,
    ) = gathered
    normed = normalize(tokens.astype(jnp.float32), norm_gain).astype(jnp.bfloat16)
    widths = [
        query_full.shape[0],
        key_full.shape[0],
        value_full.shape[0],
        gate_full.shape[0],
        left_full.shape[0],
        input_full.shape[0],
    ]
    piece = lax.all_gather(normed, "tp", axis=0, tiled=True)
    joined = jnp.concatenate(
        [
            project(piece, weight)
            for weight in (query_full, key_full, value_full, gate_full, left_full, input_full)
        ],
        axis=1,
    )
    count = joined.shape[0]
    bounds = [0]
    for width in widths:
        bounds.append(bounds[-1] + width)
    query, keys, values, gate, left, inputs = [
        joined[:, bounds[place] : bounds[place + 1]] for place in range(6)
    ]
    offset = sp_place * count
    total = count * sp_count
    positions = (offset + jnp.arange(count, dtype=jnp.int32)).astype(jnp.float32)
    local_heads = widths[0] // HEAD_DIM
    kv_local = widths[1] // HEAD_DIM
    query_rot = rotate(
        normalize(query.reshape(count, local_heads, HEAD_DIM).astype(jnp.float32), query_gain),
        positions,
    ).astype(jnp.bfloat16)
    key_rot = rotate(
        normalize(keys.reshape(count, kv_local, HEAD_DIM).astype(jnp.float32), key_gain), positions
    ).astype(jnp.bfloat16)
    key_flat = key_rot.reshape(count, kv_local * HEAD_DIM)
    product = (left.astype(jnp.float32) * inputs.astype(jnp.float32)).astype(jnp.bfloat16)
    kv_width = widths[1]
    pair_rim = with_halo(jnp.concatenate([key_flat, values], axis=1), (("sp", 0),), WINDOW)
    product_rim = with_halo(product, (("sp", 0),), 1)
    rim_rows = pair_rim.shape[0]
    key_rim = pair_rim[:, :kv_width].reshape(rim_rows, kv_local, HEAD_DIM)
    value_rim = pair_rim[:, kv_width:].reshape(rim_rows, kv_local, HEAD_DIM)
    attended = attend(query_rot, key_rim, value_rim, sink_logit, offset, total)
    padded = product_rim.astype(jnp.float32)
    convolved = (
        conv_weight[0] * padded[:-2] + conv_weight[1] * padded[1:-1] + conv_weight[2] * padded[2:]
    )
    gated = (gate.astype(jnp.float32) * convolved).astype(jnp.bfloat16)
    return lax.psum_scatter(
        (
            jnp.dot(attended, attn_out_full, preferred_element_type=jnp.float32)
            + jnp.dot(gated, conv_out_full, preferred_element_type=jnp.float32)
        ).astype(jnp.bfloat16),
        "tp",
        scatter_dimension=0,
        tiled=True,
    )


MESH = pl.DeviceIdType.MESH


def fused_kernel(
    dims,
    tok_hbm, gain_hbm, q_hbm, k_hbm, v_hbm, g_hbm, l_hbm, i_hbm,
    qgain_hbm, kgain_hbm, sink_hbm, conv_hbm, oa_hbm, oc_hbm, trig_hbm,
    out_ref,
    gain_ref, qgain_ref, kgain_ref, sink_ref, conv_ref, tok, trig, stage, ostage, win, wout, normed, normed2, acc, acc2, rim, prod, prod2, mix_a, mix_c, gated2,
    qrot,
    keep, s1, r1, s2, r2,
    local_sem, y_send, w_recv, m_send, e_send,
    tok_send, tok_recv, tok2_send, tok2_recv, rim_send, rim_recv, prod_send, prod_recv, g_send, g_recv,
    rs_send, rs_recv,
):
    scope = jax.named_scope
    line, rows, depth, qr, kr, cr = (
        dims["line"], dims["rows"], dims["depth"], dims["qr"], dims["kr"], dims["cr"]
    )
    sp = lax.axis_index("sp")
    tp = lax.axis_index("tp")
    z, y = sp // 2, sp % 2
    x, c = tp // 2, tp % 2
    y_peer = (2 * z + 1 - y, tp)
    x_peer = (sp, 2 * (1 - x) + c)
    c_peer = (sp, 2 * x + 1 - c)
    low_side = z < 2
    toward = jnp.where(low_side, 1, -1)
    is_end = (z == 0) | (z == line - 1)
    inner = (z > 0) & (z < line - 1)
    m_plane = z + toward
    e_plane = jnp.where(inner, z - toward, m_plane)
    m_peer = (2 * m_plane + y, tp)
    e_peer = (2 * e_plane + y, tp)
    near = jnp.where(inner, z - toward, z + toward)
    mid = jnp.where(inner, z + toward, z + 2 * toward)
    far = jnp.where(inner, z + 2 * toward, z + 3 * toward)
    sources = (z, near, mid, far)
    s_own = sp
    s_mate = 2 * z + 1 - y
    plane = 8 * rows
    core = qr + 2 * kr

    barrier = pltpu.get_barrier_semaphore()
    for peer in (y_peer, x_peer, c_peer, m_peer):
        pl.semaphore_signal(barrier, inc=1, device_id=peer, device_id_type=MESH)

    @pl.when(inner)
    def _():
        pl.semaphore_signal(barrier, inc=1, device_id=e_peer, device_id_type=MESH)

    def local(src, dst, place):
        copy = pltpu.make_async_copy(src, dst, local_sem.at[place])
        copy.start()
        return copy

    def in_pieces(which, dst, place):
        q0, c0 = pl.multiple_of(which * qr, qr), pl.multiple_of(which * cr, cr)
        local(q_hbm.at[pl.ds(q0, qr)], dst.at[0:qr], place)
        local(k_hbm, dst.at[qr : qr + kr], place)
        local(v_hbm, dst.at[qr + kr : core], place)
        for turn, ref in enumerate((g_hbm, l_hbm, i_hbm)):
            lo = core + turn * cr
            local(ref.at[pl.ds(c0, cr)], dst.at[lo : lo + cr], place)
        return pltpu.make_async_copy(dst, dst, local_sem.at[place])

    def out_pieces(which, dst, place):
        q0, c0 = pl.multiple_of(which * qr, qr), pl.multiple_of(which * cr, cr)
        local(oa_hbm.at[pl.ds(q0, qr)], dst.at[0:qr], place)
        local(oc_hbm.at[pl.ds(c0, cr)], dst.at[qr : qr + cr], place)
        return pltpu.make_async_copy(dst, dst, local_sem.at[place])

    loads = [in_pieces(y, win.at[s_own], 0), in_pieces(1 - y, stage, 1)]
    tok_loads = [local(tok_hbm, tok, 2), local(gain_hbm, gain_ref, 3)]
    loads += [out_pieces(y, wout.at[s_own], 4), out_pieces(1 - y, ostage, 5)]
    side_copies = [
        local(trig_hbm.at[pl.ds(pl.multiple_of(z * plane, plane), plane)], trig, 6),
        local(qgain_hbm, qgain_ref, 7),
        local(kgain_hbm, kgain_ref, 8),
        local(sink_hbm, sink_ref, 9),
        local(conv_hbm, conv_ref, 10),
    ]

    with scope("barrier"):
        pl.semaphore_wait(barrier, 4 + inner.astype(jnp.int32))

    def remote(src, dst, send, recv, peer):
        return pltpu.make_async_remote_copy(
            src_ref=src, dst_ref=dst, send_sem=send, recv_sem=recv,
            device_id=peer, device_id_type=MESH,
        )

    def chunk(kind, s):
        if kind > 1:
            return wout.at[s, 0:qr] if kind == 2 else wout.at[s, qr : qr + cr]
        return win.at[s, 0:core] if kind == 0 else win.at[s, core : core + 3 * cr]

    def hop(kind, s, sends, peer):
        return remote(chunk(kind, s), chunk(kind, s), sends.at[kind], w_recv.at[kind, s], peer)

    def send_m(kind, s):
        hop(kind, s, m_send, m_peer).start()

    def send_e(kind, s):
        hop(kind, s, e_send, e_peer).start()

    def take(kind, s):
        hop(kind, s, m_send, m_peer).wait_recv()

    def y_hop(kind):
        if kind > 1:
            src = ostage.at[0:qr] if kind == 2 else ostage.at[qr : qr + cr]
        else:
            src = stage.at[0:core] if kind == 0 else stage.at[core : core + 3 * cr]
        return remote(src, chunk(kind, s_own), y_send.at[kind], w_recv.at[kind, s_own], y_peer)

    def out_hop(s, *sends):
        for kind in (2, 3):
            take(kind, s)
            for send in sends:
                send(kind, s)

    def out_send(s, send):
        send(2, s)
        send(3, s)

    def first_of(source):
        return 2 * source + y

    def second_of(source):
        return 2 * source + 1 - y

    for copy in loads:
        copy.wait()
    send_m(0, s_own)

    @pl.when(inner)
    def _():
        send_e(0, s_own)

    y_hop(0).start()

    @pl.when(inner)
    def _():
        send_m(1, s_own)
        out_send(s_own, send_e)

    with scope("norm"):
        for copy in tok_loads:
            copy.wait()
        t = tok[...].astype(jnp.float32)
        t = t * lax.rsqrt(jnp.mean(t * t, axis=-1, keepdims=True) + EPS) * gain_ref[...]

        def block_of(yy, xx, cc):
            return 4 * yy + 2 * xx + cc

        own_block = block_of(y, x, c)
        xb = block_of(y, 1 - x, c)
        yb = block_of(1 - y, x, c)
        db = block_of(1 - y, 1 - x, c)
        normed[own_block] = t.astype(jnp.bfloat16)

    def part(ref, block, half):
        if half == 2:
            return ref.at[block]
        return ref.at[block, half * rows // 2 : (half + 1) * rows // 2]

    def tok_hop(block, half, place, peer):
        here = part(normed, block, half)
        return remote(here, here, tok_send.at[0], tok_recv.at[place], peer)

    def end_tok(block, half, place):
        return remote(
            part(normed, block, half), part(normed2, block, half), tok2_send.at[0],
            tok2_recv.at[place], m_peer,
        )

    def tok2_hop(block, place, peer):
        return remote(
            normed2.at[block], normed2.at[block], tok2_send.at[0], tok2_recv.at[place], peer
        )

    def quad(yy, xx):
        return 2 * yy + xx

    def tok_go(block, half, place, peer):
        tok_hop(block, half, place, peer).start()

    def tok_wait(block, half, place):
        tok_hop(block, half, place, x_peer).wait_recv()

    def tok2_wait(block, place):
        tok2_hop(block, place, x_peer).wait_recv()

    def tok_share(block, yy, xx):
        tok_go(block, 2, 6 + quad(yy, xx), c_peer)

    def tok2_share(block, yy, xx):
        tok2_hop(block, 4 + quad(yy, xx), c_peer).start()

    @pl.when(is_end)
    def _():
        end_tok(own_block, 0, 0).start()

    tok_go(own_block, 1, 1, x_peer)
    tok_go(own_block, 0, 2, y_peer)
    tok_go(own_block, 0, 0, x_peer)
    tok_go(own_block, 1, 3, y_peer)
    y_hop(1).start()
    tok_share(own_block, y, x)

    with scope("c_mate"):
        take(0, s_mate)
        send_m(0, s_mate)

        @pl.when(inner)
        def _():
            send_e(0, s_mate)
            take(0, first_of(near))
            send_m(0, first_of(near))
            take(0, first_of(mid))
            send_e(0, first_of(mid))

        @pl.when(is_end)
        def _():
            end_tok(own_block, 1, 0).start()
            send_m(1, s_own)

    with scope("tok_xy"):
        tok_wait(xb, 1, 1)
        tok_go(xb, 1, 5, y_peer)
        tok_wait(yb, 0, 2)
        tok_go(yb, 0, 4, x_peer)
        tok_wait(xb, 0, 0)
        tok_share(xb, y, 1 - x)
        tok_wait(yb, 1, 3)
        tok_share(yb, 1 - y, x)

    with scope("c_fwd"):
        @pl.when(inner)
        def _():
            take(0, second_of(mid))
            send_e(0, second_of(mid))
            take(0, second_of(near))
            send_m(0, second_of(near))

    with scope("tok2_own"):
        @pl.when(inner)
        def _():
            tok2_wait(own_block, 0)
            tok2_hop(own_block, 2, x_peer).start()
            tok2_hop(own_block, 3, y_peer).start()
            tok2_share(own_block, y, x)

    y_hop(2).start()
    y_hop(3).start()

    with scope("far1"):
        @pl.when(inner)
        def _():
            take(0, first_of(far))
            send_e(0, first_of(far))

    with scope("v_mate"):
        take(1, s_mate)
        send_m(1, s_mate)

    with scope("far2"):
        @pl.when(inner)
        def _():
            take(0, second_of(far))
            send_e(0, second_of(far))

    with scope("tok_db"):
        tok_wait(db, 0, 4)
        tok_wait(db, 1, 5)
        tok_share(db, 1 - y, 1 - x)

        @pl.when(is_end)
        def _():
            end_tok(db, 2, 1).start()

    with scope("v_near1"):
        @pl.when(inner)
        def _():
            take(1, first_of(near))
            send_m(1, first_of(near))

    with scope("tok_rest"):
        for yy in range(2):
            for xx in range(2):
                tok_wait(block_of(yy, xx, 1 - c), 2, 6 + quad(yy, xx))

    def columns(s):
        return pl.ds(pl.multiple_of(s * depth, depth), depth)

    def dot_t(a, w):
        return lax.dot_general(a, w, (((1,), (1,)), ((), ())), preferred_element_type=jnp.float32)

    def plane_dots(tokens, into, cols, weight_rows, source, add):
        total = into[:, cols] if add else None
        for half in range(2):
            s = 2 * source + half
            a = tokens[:, :, columns(s)].reshape(plane, depth)
            product = dot_t(a, win[s, weight_rows])
            total = product if total is None else total + product
        into[:, cols] = total

    conv_rows = slice(core, core + 3 * cr)

    def early_dots(tokens, into, cols, weight_rows, count):
        plane_dots(tokens, into, cols, weight_rows, z, False)

        def step(k, carry):
            source = jnp.where(k == 1, near, jnp.where(k == 2, mid, far))
            plane_dots(tokens, into, cols, weight_rows, source, True)
            return carry

        lax.fori_loop(1, count, step, 0)

    with scope("c_dots"):
        @pl.when(is_end)
        def _():
            for source in (near, mid, far):
                for s in (first_of(source), second_of(source)):
                    take(0, s)

        early_dots(normed, acc, slice(0, core), slice(0, core), line)

    with scope("rot"):
        for copy in side_copies:
            copy.wait()
        lane = lax.broadcasted_iota(jnp.int32, (plane, qr), 1)
        half_dim = HEAD_DIM // 2
        table = trig[...]
        cos2 = jnp.where(lane < HEAD_DIM, table, pltpu.roll(table, HEAD_DIM, 1))
        sin2 = jnp.where(lane < HEAD_DIM, pltpu.roll(table, HEAD_DIM, 1), table)
        low = lane < HEAD_DIM
        first_half = lane % HEAD_DIM < half_dim

        def rot(v):
            partner = jnp.where(
                first_half, pltpu.roll(v, qr - half_dim, 1), pltpu.roll(v, half_dim, 1)
            )
            return v * cos2 + partner * sin2

        def bf(v):
            return v.astype(jnp.bfloat16).astype(jnp.float32)

        kv = bf(acc[:, qr : 2 * qr])
        ksq = jnp.sum(jnp.where(low, kv * kv, 0.0), axis=-1, keepdims=True) / HEAD_DIM
        kgain = jnp.concatenate([kgain_ref[...], kgain_ref[...]], axis=1)
        kn = kv * lax.rsqrt(ksq + EPS) * kgain
        krot = rot(kn)
        rim[WINDOW : WINDOW + plane, :] = jnp.where(low, krot, kv).astype(jnp.bfloat16)

    bottom = pl.ds(WINDOW, WINDOW)
    top = pl.ds(plane, WINDOW)
    up = (jnp.minimum(2 * (z + 1) + y, 2 * line - 1), tp)
    down = (jnp.maximum(2 * (z - 1) + y, 0), tp)
    has_up = z < line - 1
    has_down = z > 0
    rim_up = remote(rim.at[top], rim.at[pl.ds(0, WINDOW)], rim_send.at[0], rim_recv.at[0], up)
    rim_down = remote(
        rim.at[bottom], rim.at[pl.ds(WINDOW + plane, WINDOW)], rim_send.at[1], rim_recv.at[1], down
    )

    @pl.when(has_up)
    def _():
        rim_up.start()

    @pl.when(has_down)
    def _():
        rim_down.start()

    zero_rim = jnp.zeros((WINDOW, qr), jnp.bfloat16)

    @pl.when(z == 0)
    def _():
        rim[0:WINDOW] = zero_rim

    @pl.when(z == line - 1)
    def _():
        rim[WINDOW + plane :] = zero_rim

    with scope("rotq"):
        qv = bf(acc[:, 0:qr])
        qq = qv * qv
        q_lo = jnp.sum(jnp.where(low, qq, 0.0), axis=-1, keepdims=True) / HEAD_DIM
        q_hi = jnp.sum(jnp.where(low, 0.0, qq), axis=-1, keepdims=True) / HEAD_DIM
        qgain = jnp.concatenate([qgain_ref[...], qgain_ref[...]], axis=1)
        qn = qv * lax.rsqrt(jnp.where(low, q_lo, q_hi) + EPS) * qgain
        qro = rot(qn)
        qrot[0] = jnp.where(low, qro, 0.0).astype(jnp.bfloat16)
        qrot[1] = jnp.where(low, pltpu.roll(qro, HEAD_DIM, 1), 0.0).astype(jnp.bfloat16)

    with scope("tok2_xb"):
        @pl.when(inner)
        def _():
            tok2_wait(xb, 2)
            tok2_share(xb, y, 1 - x)

    span = BLOCK + 2 * WINDOW
    total = plane * line

    def att_block(block):
        begin = pl.multiple_of(block * BLOCK, BLOCK)
        kvb = rim[pl.ds(begin, span), :]
        qb = qrot[:, pl.ds(begin, BLOCK), :].reshape(2 * BLOCK, qr)
        scores = lax.dot_general(
            qb, kvb, (((1,), (1,)), ((), ())), preferred_element_type=jnp.float32
        ) * HEAD_DIM ** (-0.5)
        row = lax.broadcasted_iota(jnp.int32, (2 * BLOCK, span), 0)
        col = lax.broadcasted_iota(jnp.int32, (2 * BLOCK, span), 1)
        gap = row % BLOCK + WINDOW - col
        pos = z * plane + begin - WINDOW + col
        allowed = (gap <= WINDOW) & (gap >= -WINDOW) & (pos >= 0) & (pos < total)
        scores = jnp.where(allowed, scores, NEG_FILL)
        head = lax.broadcasted_iota(jnp.int32, (2 * BLOCK, 1), 0)
        sink = jnp.where(head < BLOCK, sink_ref[0, 2 * y], sink_ref[0, 2 * y + 1])
        peak = jnp.maximum(jnp.max(scores, axis=-1, keepdims=True), sink)
        expo = jnp.exp(scores - peak)
        denom = jnp.sum(expo, axis=-1, keepdims=True) + jnp.exp(sink - peak)
        weights = (expo / denom).astype(jnp.bfloat16)
        o = jnp.dot(weights, kvb, preferred_element_type=jnp.float32)
        low_b = lax.broadcasted_iota(jnp.int32, (BLOCK, qr), 1) < HEAD_DIM
        both = jnp.where(low_b, pltpu.roll(o[:BLOCK], HEAD_DIM, 1), o[BLOCK:])
        mix_a[pl.ds(begin, BLOCK), :] = both.astype(jnp.bfloat16)

    nblocks = plane // BLOCK

    def att_inner(block, carry):
        att_block(block)
        return carry

    with scope("att_in"):
        lax.fori_loop(1, nblocks - 1, att_inner, 0)

    with scope("tok2_yb"):
        @pl.when(inner)
        def _():
            tok2_wait(yb, 3)
            tok2_share(yb, 1 - y, x)

    with scope("v_near2"):
        @pl.when(inner)
        def _():
            take(1, second_of(near))
            send_m(1, second_of(near))

    with scope("o_mate"):
        @pl.when(is_end)
        def _():
            out_send(s_own, send_m)
            out_hop(s_mate, send_m)

        @pl.when(inner)
        def _():
            out_send(s_own, send_m)
            out_hop(s_mate, send_e)

    with scope("v_mid"):
        @pl.when(inner)
        def _():
            for s in (first_of(mid), second_of(mid)):
                take(1, s)

    with scope("v_dots"):
        @pl.when(inner)
        def _():
            early_dots(normed, acc, conv_rows, conv_rows, 3)

    with scope("tok2_db"):
        @pl.when(inner)
        def _():
            tok2_wait(db, 1)
            tok2_share(db, 1 - y, 1 - x)

    def attend_edges():
        with scope("rim_wait"):
            @pl.when(has_down)
            def _():
                rim_up.wait_recv()

            @pl.when(has_up)
            def _():
                rim_down.wait_recv()

        with scope("att_out"):
            def att_outer(k, carry):
                att_block(k * (nblocks - 1))
                return carry

            lax.fori_loop(0, 2, att_outer, 0)

    pad = 16
    zero_pad = jnp.zeros((pad, cr), jnp.bfloat16)
    taps = conv_ref[y]
    base = core

    def convolve(ref, gate):
        p = ref[...].astype(jnp.float32)
        before = pltpu.roll(p, 1, 0)[pad : pad + plane]
        after = pltpu.roll(p, plane + 2 * pad - 1, 0)[pad : pad + plane]
        mixed = taps[0:1] * before + taps[1:2] * p[pad : pad + plane] + taps[2:3] * after
        return (gate * mixed).astype(jnp.bfloat16)

    prod_up = remote(
        prod.at[pl.ds(plane, pad)], prod.at[pl.ds(0, pad)], prod_send.at[0], prod_recv.at[0], up
    )
    prod_down = remote(
        prod.at[pl.ds(pad, pad)], prod.at[pl.ds(pad + plane, pad)],
        prod_send.at[1], prod_recv.at[1], down,
    )
    low_inner = inner & low_side
    high_inner = inner & (z >= 2)
    g_copy = remote(gated2, mix_c, g_send.at[0], g_recv.at[0], e_peer)

    @pl.when(inner)
    def _():
        with scope("tok2_rest"):
            for yy in range(2):
                for xx in range(2):
                    tok2_wait(block_of(yy, xx, 1 - c), 4 + quad(yy, xx))

        with scope("help_dots"):
            early_dots(normed2, acc2, slice(0, 3 * cr), conv_rows, 3)

        with scope("far_dots"):
            for s in (first_of(far), second_of(far)):
                take(1, s)
            plane_dots(normed2, acc2, slice(0, 3 * cr), conv_rows, far, True)
            plane_dots(normed, acc, conv_rows, conv_rows, far, True)

        with scope("prod"):
            left = bf(acc[:, base + cr : base + 2 * cr])
            inputs = bf(acc[:, base + 2 * cr : base + 3 * cr])
            prod[pad : pad + plane] = (left * inputs).astype(jnp.bfloat16)

            @pl.when(low_inner)
            def _():
                prod_up.start()

            @pl.when(high_inner)
            def _():
                prod_down.start()

            out_send(s_mate, send_m)
            out_hop(first_of(near), send_m)

            prod2[pad : pad + plane] = (
                bf(acc2[:, cr : 2 * cr]) * bf(acc2[:, 2 * cr : 3 * cr])
            ).astype(jnp.bfloat16)

            @pl.when(z == 1)
            def _():
                prod2[0:pad] = zero_pad
                prod2[pad + plane :] = prod[pad : 2 * pad]
                prod[0:pad] = prod2[plane : plane + pad]

            @pl.when(z != 1)
            def _():
                prod2[0:pad] = prod[plane : plane + pad]
                prod2[pad + plane :] = zero_pad
                prod[pad + plane :] = prod2[pad : 2 * pad]

            gated2[...] = convolve(prod2, bf(acc2[:, 0:cr]))
            g_copy.start()

        attend_edges()

        with scope("o_fwd"):
            out_hop(second_of(near), send_m)
            out_hop(first_of(mid), send_e)

        with scope("prod_wait"):
            @pl.when(low_inner)
            def _():
                prod_down.wait_recv()

            @pl.when(high_inner)
            def _():
                prod_up.wait_recv()

            mix_c[...] = convolve(prod, bf(acc[:, base : base + cr]))

    @pl.when(is_end)
    def _():
        attend_edges()
        with scope("g_wait"):
            g_copy.wait_recv()

    def group(cc):
        spans = [pl.ds(pl.multiple_of((2 * q + cc) * rows, rows), rows) for q in range(4)]
        return [jnp.concatenate([mix_a[w, :], mix_c[w, :]], axis=1) for w in spans]

    mine_rows = jnp.concatenate(group(c), axis=0)
    other_rows = jnp.concatenate(group(1 - c), axis=0)

    def rs_hop(src, dst, stage_id, s, peer):
        return remote(src, dst, rs_send.at[stage_id], rs_recv.at[stage_id, s], peer)

    def out_take(i):
        s = 2 * sources[i // 2] + i % 2
        out_hop(s)

    def out_forward(i):
        source = sources[i // 2]
        out_hop(first_of(source) if i % 2 == 0 else second_of(source), send_e)

    def stage_a(i):
        s = 2 * sources[i // 2] + i % 2
        weight = wout[s]
        s1[s] = jnp.dot(
            other_rows, weight, preferred_element_type=jnp.float32
        ).astype(jnp.bfloat16).reshape(2, 2, rows, depth)
        rs_hop(s1.at[s], r1.at[s], 0, s, c_peer).start()
        keep[s] = jnp.dot(
            mine_rows, weight, preferred_element_type=jnp.float32
        ).reshape(2, 2, rows, depth)

    d_peer = (2 * z + 1 - y, 2 * (1 - x) + c)
    corners = ((1 - y, 1 - x, d_peer), (1 - y, x, y_peer), (y, 1 - x, x_peer))

    def stage_b(i):
        s = 2 * sources[i // 2] + i % 2
        rs_hop(s1.at[s], r1.at[s], 0, s, c_peer).wait_recv()
        for j, (yy, xx, peer) in enumerate(corners):
            s2[s, j] = (keep[s, yy, xx] + r1[s, yy, xx].astype(jnp.float32)).astype(jnp.bfloat16)
            rs_hop(s2.at[s, j], r2.at[s, j], 1, s, peer).start()

    def stage_d(i):
        s = 2 * sources[i // 2] + i % 2
        piece = keep[s, y, x] + r1[s, y, x].astype(jnp.float32)
        rs_hop(s2.at[s], r2.at[s], 1, s, d_peer).wait_recv()
        for j in range(3):
            piece = piece + r2[s, j].astype(jnp.float32)
        out_ref[:, columns(s)] = piece.astype(jnp.bfloat16)

    order = (
        ("a", (0, 1)), ("f", (5,)), ("b", (0,)), ("a", (2,)), ("b", (1,)), ("a", (3,)),
        ("b", (2, 3)), ("w", (4,)), ("a", (4,)), ("f", (6,)), ("b", (4,)),
        ("w", (5,)), ("a", (5,)), ("b", (5,)), ("f", (7,)), ("w", (6,)), ("a", (6,)), ("b", (6,)),
        ("d", (0, 1)), ("w", (7,)), ("a", (7,)), ("b", (7,)),
        ("d", (2, 3, 4, 5, 6, 7)),
    )

    for step, places in order:
        for i in places:
            with scope(f"{step}{i}"):
                if step == "w":
                    pl.when(is_end)(functools.partial(out_take, i))
                elif step == "f":
                    pl.when(inner)(functools.partial(out_forward, i))
                elif step == "a":
                    if i in (2, 3):
                        pl.when(is_end)(functools.partial(out_take, i))
                    stage_a(i)
                elif step == "b":
                    stage_b(i)
                else:
                    stage_d(i)

    def sent(ref, send):
        remote(ref, ref, send, w_recv.at[0, 0], m_peer).wait_send()

    def chunks_sent(kind, count, sends):
        if kind > 1:
            ref = wout.at[0:count, 0:qr] if kind == 2 else wout.at[0:count, qr : qr + cr]
        else:
            ref = win.at[0:count, 0:core] if kind == 0 else win.at[0:count, core : core + 3 * cr]
        sent(ref, sends.at[kind])

    with scope("sends"):
        for kind in range(4):
            y_hop(kind).wait_send()
        sent(normed.at[0:7], tok_send.at[0])
        sent(s1, rs_send.at[0])
        sent(s2, rs_send.at[1])

        @pl.when(has_up)
        def _():
            rim_up.wait_send()

        @pl.when(has_down)
        def _():
            rim_down.wait_send()

        @pl.when(is_end)
        def _():
            sent(normed.at[0:2], tok2_send.at[0])
            for kind in range(4):
                chunks_sent(kind, 2, m_send)

        @pl.when(inner)
        def _():
            sent(normed2.at[0:6], tok2_send.at[0])
            g_copy.wait_send()
            for kind in range(4):
                chunks_sent(kind, 4, m_send)
            for kind in (0, 2, 3):
                chunks_sent(kind, 6, e_send)

        @pl.when(low_inner)
        def _():
            prod_up.wait_send()

        @pl.when(high_inner)
        def _():
            prod_down.wait_send()


def trig_table(total):
    half = HEAD_DIM // 2
    freq = np.float64(ROPE_BASE) ** (-np.arange(half) / half)
    angle = np.arange(total)[:, None] * freq
    cosine, sine = np.cos(angle), np.sin(angle)
    return np.concatenate([cosine, cosine, -sine, sine], axis=1).astype(np.float32)


def fused_device(
    tokens, norm_gain, query_weight, key_weight, value_weight, gate_weight, left_weight,
    input_weight, query_gain, key_gain, sink_logit, conv_weight, out_attention, out_conv,
):
    sp_count = lax.axis_size("sp")
    line = sp_count // 2
    rows, width = tokens.shape
    depth = query_weight.shape[1]
    qr = query_weight.shape[0] // 2
    kr = key_weight.shape[0]
    cr = gate_weight.shape[0] // 2
    fan = qr + 2 * kr + 3 * cr
    plane = 8 * rows
    dims = dict(line=line, rows=rows, depth=depth, qr=qr, kr=kr, cr=cr)
    hb = pl.BlockSpec(memory_space=pltpu.HBM)
    bf16, f32 = jnp.bfloat16, jnp.float32
    dma = pltpu.SemaphoreType.DMA
    n = sp_count
    scratch = [
        pltpu.VMEM((1, width), f32),
        pltpu.VMEM((1, HEAD_DIM), f32),
        pltpu.VMEM((1, HEAD_DIM), f32),
        pltpu.SMEM((1, 4), f32),
        pltpu.VMEM((2, 3, cr), f32),
        pltpu.VMEM((rows, width), bf16),
        pltpu.VMEM((plane, 2 * HEAD_DIM), f32),
        pltpu.VMEM((fan, depth), bf16),
        pltpu.VMEM((qr + cr, depth), bf16),
        pltpu.VMEM((n, fan, depth), bf16),
        pltpu.VMEM((n, qr + cr, depth), bf16),
        pltpu.VMEM((8, rows, width), bf16),
        pltpu.VMEM((8, rows, width), bf16),
        pltpu.VMEM((plane, fan), f32),
        pltpu.VMEM((plane, 3 * cr), f32),
        pltpu.VMEM((plane + 2 * WINDOW, qr), bf16),
        pltpu.VMEM((plane + 32, cr), bf16),
        pltpu.VMEM((plane + 32, cr), bf16),
        pltpu.VMEM((plane, qr), bf16),
        pltpu.VMEM((plane, cr), bf16),
        pltpu.VMEM((plane, cr), bf16),
        pltpu.VMEM((2, plane, qr), bf16),
        pltpu.VMEM((n, 2, 2, rows, depth), f32),
        pltpu.VMEM((n, 2, 2, rows, depth), bf16),
        pltpu.VMEM((n, 2, 2, rows, depth), bf16),
        pltpu.VMEM((n, 3, rows, depth), bf16),
        pltpu.VMEM((n, 3, rows, depth), bf16),
        dma((11,)), dma((4,)), dma((4, n)), dma((4,)), dma((4,)),
        dma((1,)), dma((10,)), dma((1,)), dma((8,)), dma((2,)), dma((2,)), dma((2,)), dma((2,)),
        dma((1,)), dma((1,)), dma((2,)), dma((2, n)),
    ]
    taps = conv_weight.reshape(3, 2, cr).transpose(1, 0, 2)
    return pl.pallas_call(
        functools.partial(fused_kernel, dims),
        out_shape=jax.ShapeDtypeStruct((rows, width), bf16),
        in_specs=[hb] * 15,
        out_specs=pl.BlockSpec(memory_space=pltpu.VMEM),
        scratch_shapes=scratch,
        compiler_params=pltpu.CompilerParams(
            collective_id=0, has_side_effects=True, vmem_limit_bytes=32 * 1024 * 1024
        ),
    )(*(pltpu.with_memory_space_constraint(array, pltpu.HBM) for array in (
        tokens, norm_gain[None, :], query_weight, key_weight, value_weight, gate_weight,
        left_weight, input_weight, query_gain[None, :],
        key_gain[None, :], sink_logit[None, :], taps, out_attention, out_conv,
        jnp.asarray(trig_table(plane * line)),
    )))


def local_device(*args):
    tokens, query_weight, key_weight, gate_weight = args[0], args[2], args[3], args[5]
    fits = (
        lax.axis_size("sp") == 8
        and lax.axis_size("tp") == 4
        and query_weight.shape[1] % 128 == 0
        and query_weight.shape[0] == 4 * HEAD_DIM
        and key_weight.shape[0] == HEAD_DIM
        and gate_weight.shape[0] == 256
        and tokens.shape[0] % 32 == 0
        and 8 * tokens.shape[0] % BLOCK == 0
        and 8 * tokens.shape[0] >= 2 * BLOCK
    )
    return fused_device(*args) if fits else per_device(*args)


def solution(mesh):
    in_specs = (
        P(("sp", "tp"), None),
        P(),
        P("tp", "sp"),
        P("tp", "sp"),
        P("tp", "sp"),
        P("tp", "sp"),
        P("tp", "sp"),
        P("tp", "sp"),
        P(),
        P(),
        P("tp"),
        P(None, "tp"),
        P("tp", "sp"),
        P("tp", "sp"),
    )
    out_specs = P(("sp", "tp"), None)
    return jax.shard_map(
        local_device, mesh=mesh, in_specs=in_specs, out_specs=out_specs, check_vma=False
    )
```

```python
import functools

import jax
import jax.numpy as jnp
import numpy as np
from jax import lax
from jax.experimental import pallas as pl
from jax.experimental.pallas import tpu as pltpu
from jax.sharding import PartitionSpec as P

HEAD_DIM = 64
WINDOW = 128
BLOCK = 128


EPS = 1e-06
ROPE_BASE = 10000.0
NEG_FILL = -1e30


def with_halo(cells, sides, width):
    for axis, dim in sides:
        count = lax.axis_size(axis)
        ends = count - 1
        head = lax.slice_in_dim(cells, 0, width, axis=dim)
        tail = lax.slice_in_dim(cells, cells.shape[dim] - width, cells.shape[dim], axis=dim)
        cells = jnp.concatenate(
            [
                lax.ppermute(tail, axis, [(i, (i + 1) % count) for i in range(ends)]),
                cells,
                lax.ppermute(head, axis, [((i + 1) % count, i) for i in range(ends)]),
            ],
            axis=dim,
        )
    return cells


def normalize(values, gain):
    return values * lax.rsqrt(jnp.mean(values * values, axis=-1, keepdims=True) + EPS) * gain


def rotate(values, positions):
    half = values.shape[-1] // 2
    freq = ROPE_BASE ** (-jnp.arange(half, dtype=jnp.float32) / half)
    angle = positions[:, None] * freq
    cosine = jnp.cos(angle)[:, None, :]
    sine = jnp.sin(angle)[:, None, :]
    first = values[..., :half]
    second = values[..., half:]
    return jnp.concatenate(
        [first * cosine - second * sine, second * cosine + first * sine], axis=-1
    )


def project(rows, weight):
    return lax.dot_general(
        rows, weight, (((1,), (1,)), ((), ())), preferred_element_type=jnp.float32
    ).astype(jnp.bfloat16)


def attend(query_rot, key_rim, value_rim, sinks, offset, total):
    count = query_rot.shape[0]
    local_heads = query_rot.shape[1]
    kv_local = key_rim.shape[1]
    group = local_heads // kv_local
    span = BLOCK + 2 * WINDOW
    nblocks = count // BLOCK
    shaped = query_rot.reshape(nblocks, BLOCK, kv_local, group, HEAD_DIM)
    sink_group = sinks.reshape(kv_local, group)[:, :, None]

    def one_block(packed):
        block_index, query_block = packed
        begin = block_index * BLOCK
        key_block = lax.dynamic_slice_in_dim(key_rim, begin, span, 0)
        value_block = lax.dynamic_slice_in_dim(value_rim, begin, span, 0)
        scores = jnp.einsum(
            "qkgd,nkd->kgqn", query_block, key_block, preferred_element_type=jnp.float32
        ) * HEAD_DIM ** (-0.5)
        query_pos = offset + begin + jnp.arange(BLOCK, dtype=jnp.int32)
        key_pos = offset + begin - WINDOW + jnp.arange(span, dtype=jnp.int32)
        allowed = (
            (jnp.abs(query_pos[:, None] - key_pos[None, :]) <= WINDOW)
            & (key_pos >= 0)[None, :]
            & (key_pos < total)[None, :]
        )
        scores = jnp.where(allowed, scores, NEG_FILL)
        top = jnp.maximum(jnp.max(scores, axis=-1), sink_group)
        expo = jnp.exp(scores - top[..., None])
        denom = jnp.sum(expo, axis=-1) + jnp.exp(sink_group - top)
        weights = (expo / denom[..., None]).astype(jnp.bfloat16)
        return jnp.einsum(
            "kgqn,nkd->qkgd", weights, value_block, preferred_element_type=jnp.float32
        ).astype(jnp.bfloat16)

    result = lax.map(one_block, (jnp.arange(nblocks, dtype=jnp.int32), shaped))
    return result.reshape(count, local_heads * HEAD_DIM)


def per_device(
    tokens,
    norm_gain,
    query_weight,
    key_weight,
    value_weight,
    gate_weight,
    left_weight,
    input_weight,
    query_gain,
    key_gain,
    sink_logit,
    conv_weight,
    out_attention,
    out_conv,
):
    sp_count = lax.axis_size("sp")
    sp_place = lax.axis_index("sp")
    gathered = (
        lax.all_gather(query_weight, "sp", axis=1, tiled=True),
        lax.all_gather(key_weight, "sp", axis=1, tiled=True),
        lax.all_gather(value_weight, "sp", axis=1, tiled=True),
        lax.all_gather(gate_weight, "sp", axis=1, tiled=True),
        lax.all_gather(left_weight, "sp", axis=1, tiled=True),
        lax.all_gather(input_weight, "sp", axis=1, tiled=True),
        lax.all_gather(out_attention, "sp", axis=1, tiled=True),
        lax.all_gather(out_conv, "sp", axis=1, tiled=True),
    )
    (
        query_full,
        key_full,
        value_full,
        gate_full,
        left_full,
        input_full,
        attn_out_full,
        conv_out_full,
    ) = gathered
    normed = normalize(tokens.astype(jnp.float32), norm_gain).astype(jnp.bfloat16)
    widths = [
        query_full.shape[0],
        key_full.shape[0],
        value_full.shape[0],
        gate_full.shape[0],
        left_full.shape[0],
        input_full.shape[0],
    ]
    piece = lax.all_gather(normed, "tp", axis=0, tiled=True)
    joined = jnp.concatenate(
        [
            project(piece, weight)
            for weight in (query_full, key_full, value_full, gate_full, left_full, input_full)
        ],
        axis=1,
    )
    count = joined.shape[0]
    bounds = [0]
    for width in widths:
        bounds.append(bounds[-1] + width)
    query, keys, values, gate, left, inputs = [
        joined[:, bounds[place] : bounds[place + 1]] for place in range(6)
    ]
    offset = sp_place * count
    total = count * sp_count
    positions = (offset + jnp.arange(count, dtype=jnp.int32)).astype(jnp.float32)
    local_heads = widths[0] // HEAD_DIM
    kv_local = widths[1] // HEAD_DIM
    query_rot = rotate(
        normalize(query.reshape(count, local_heads, HEAD_DIM).astype(jnp.float32), query_gain),
        positions,
    ).astype(jnp.bfloat16)
    key_rot = rotate(
        normalize(keys.reshape(count, kv_local, HEAD_DIM).astype(jnp.float32), key_gain), positions
    ).astype(jnp.bfloat16)
    key_flat = key_rot.reshape(count, kv_local * HEAD_DIM)
    product = (left.astype(jnp.float32) * inputs.astype(jnp.float32)).astype(jnp.bfloat16)
    kv_width = widths[1]
    pair_rim = with_halo(jnp.concatenate([key_flat, values], axis=1), (("sp", 0),), WINDOW)
    product_rim = with_halo(product, (("sp", 0),), 1)
    rim_rows = pair_rim.shape[0]
    key_rim = pair_rim[:, :kv_width].reshape(rim_rows, kv_local, HEAD_DIM)
    value_rim = pair_rim[:, kv_width:].reshape(rim_rows, kv_local, HEAD_DIM)
    attended = attend(query_rot, key_rim, value_rim, sink_logit, offset, total)
    padded = product_rim.astype(jnp.float32)
    convolved = (
        conv_weight[0] * padded[:-2] + conv_weight[1] * padded[1:-1] + conv_weight[2] * padded[2:]
    )
    gated = (gate.astype(jnp.float32) * convolved).astype(jnp.bfloat16)
    return lax.psum_scatter(
        (
            jnp.dot(attended, attn_out_full, preferred_element_type=jnp.float32)
            + jnp.dot(gated, conv_out_full, preferred_element_type=jnp.float32)
        ).astype(jnp.bfloat16),
        "tp",
        scatter_dimension=0,
        tiled=True,
    )


MESH = pl.DeviceIdType.MESH


def fused_kernel(
    dims,
    tok_hbm, gain_hbm, q_hbm, k_hbm, v_hbm, g_hbm, l_hbm, i_hbm,
    qgain_hbm, kgain_hbm, sink_hbm, conv_hbm, oa_hbm, oc_hbm, trig_hbm,
    out_ref,
    gain_ref, qgain_ref, kgain_ref, sink_ref, conv_ref, tok, trig, stage, ostage, win, wout, normed, normed2, acc, acc2, keys, prod, prod2, mix_a, mix_c, gated2,
    qrot,
    keep, s1, r1, s2, r2,
    local_sem, y_send, w_recv, m_send, e_send,
    tok_send, tok_recv, tok2_send, tok2_recv, rim_send, rim_recv, kv_send, kv_recv, prod_send, prod_recv, g_send, g_recv,
    rs_send, rs_recv,
):
    scope = jax.named_scope
    line, rows, depth, qr, kr, cr = (
        dims["line"], dims["rows"], dims["depth"], dims["qr"], dims["kr"], dims["cr"]
    )
    sp = lax.axis_index("sp")
    tp = lax.axis_index("tp")
    z, y = sp // 2, sp % 2
    x, c = tp // 2, tp % 2
    y_peer = (2 * z + 1 - y, tp)
    x_peer = (sp, 2 * (1 - x) + c)
    c_peer = (sp, 2 * x + 1 - c)
    low_side = z < 2
    toward = jnp.where(low_side, 1, -1)
    is_end = (z == 0) | (z == line - 1)
    inner = (z > 0) & (z < line - 1)
    m_plane = z + toward
    e_plane = jnp.where(inner, z - toward, m_plane)
    m_peer = (2 * m_plane + y, tp)
    e_peer = (2 * e_plane + y, tp)
    near = jnp.where(inner, z - toward, z + toward)
    mid = jnp.where(inner, z + toward, z + 2 * toward)
    far = jnp.where(inner, z + 2 * toward, z + 3 * toward)
    sources = (z, near, mid, far)
    s_own = sp
    s_mate = 2 * z + 1 - y
    plane = 8 * rows
    core = qr + kr

    barrier = pltpu.get_barrier_semaphore()
    for peer in (y_peer, x_peer, c_peer, m_peer):
        pl.semaphore_signal(barrier, inc=1, device_id=peer, device_id_type=MESH)

    @pl.when(inner)
    def _():
        pl.semaphore_signal(barrier, inc=1, device_id=e_peer, device_id_type=MESH)

    def local(src, dst, place):
        copy = pltpu.make_async_copy(src, dst, local_sem.at[place])
        copy.start()
        return copy

    def in_pieces(which, dst, place):
        q0, c0 = pl.multiple_of(which * qr, qr), pl.multiple_of(which * cr, cr)
        local(q_hbm.at[pl.ds(q0, qr)], dst.at[0:qr], place)

        @pl.when(which == 0)
        def _():
            local(k_hbm, dst.at[qr:core], place)

        @pl.when(which == 1)
        def _():
            local(v_hbm, dst.at[qr:core], place)

        for turn, ref in enumerate((g_hbm, l_hbm, i_hbm)):
            lo = core + turn * cr
            local(ref.at[pl.ds(c0, cr)], dst.at[lo : lo + cr], place)
        return pltpu.make_async_copy(dst, dst, local_sem.at[place])

    def out_pieces(which, dst, place):
        q0, c0 = pl.multiple_of(which * qr, qr), pl.multiple_of(which * cr, cr)
        local(oa_hbm.at[pl.ds(q0, qr)], dst.at[0:qr], place)
        local(oc_hbm.at[pl.ds(c0, cr)], dst.at[qr : qr + cr], place)
        return pltpu.make_async_copy(dst, dst, local_sem.at[place])

    loads = [in_pieces(y, win.at[s_own], 0), in_pieces(1 - y, stage, 1)]
    tok_loads = [local(tok_hbm, tok, 2), local(gain_hbm, gain_ref, 3)]
    loads += [out_pieces(y, wout.at[s_own], 4), out_pieces(1 - y, ostage, 5)]
    side_copies = [
        local(trig_hbm.at[pl.ds(pl.multiple_of(z * plane, plane), plane)], trig, 6),
        local(qgain_hbm, qgain_ref, 7),
        local(kgain_hbm, kgain_ref, 8),
        local(sink_hbm, sink_ref, 9),
        local(conv_hbm, conv_ref, 10),
    ]

    with scope("barrier"):
        pl.semaphore_wait(barrier, 4 + inner.astype(jnp.int32))

    def remote(src, dst, send, recv, peer):
        return pltpu.make_async_remote_copy(
            src_ref=src, dst_ref=dst, send_sem=send, recv_sem=recv,
            device_id=peer, device_id_type=MESH,
        )

    def chunk(kind, s):
        if kind > 1:
            return wout.at[s, 0:qr] if kind == 2 else wout.at[s, qr : qr + cr]
        return win.at[s, 0:core] if kind == 0 else win.at[s, core : core + 3 * cr]

    def hop(kind, s, sends, peer):
        return remote(chunk(kind, s), chunk(kind, s), sends.at[kind], w_recv.at[kind, s], peer)

    def send_m(kind, s):
        hop(kind, s, m_send, m_peer).start()

    def send_e(kind, s):
        hop(kind, s, e_send, e_peer).start()

    def take(kind, s):
        hop(kind, s, m_send, m_peer).wait_recv()

    def y_hop(kind):
        if kind > 1:
            src = ostage.at[0:qr] if kind == 2 else ostage.at[qr : qr + cr]
        else:
            src = stage.at[0:core] if kind == 0 else stage.at[core : core + 3 * cr]
        return remote(src, chunk(kind, s_own), y_send.at[kind], w_recv.at[kind, s_own], y_peer)

    def out_hop(s, *sends):
        for kind in (2, 3):
            take(kind, s)
            for send in sends:
                send(kind, s)

    def out_send(s, send):
        send(2, s)
        send(3, s)

    def first_of(source):
        return 2 * source + y

    def second_of(source):
        return 2 * source + 1 - y

    for copy in loads:
        copy.wait()
    send_m(0, s_own)

    @pl.when(inner)
    def _():
        send_e(0, s_own)

    y_hop(0).start()

    @pl.when(inner)
    def _():
        send_m(1, s_own)
        out_send(s_own, send_e)

    with scope("norm"):
        for copy in tok_loads:
            copy.wait()
        t = tok[...].astype(jnp.float32)
        t = t * lax.rsqrt(jnp.mean(t * t, axis=-1, keepdims=True) + EPS) * gain_ref[...]

        def block_of(yy, xx, cc):
            return 4 * yy + 2 * xx + cc

        own_block = block_of(y, x, c)
        xb = block_of(y, 1 - x, c)
        yb = block_of(1 - y, x, c)
        db = block_of(1 - y, 1 - x, c)
        normed[own_block] = t.astype(jnp.bfloat16)

    def part(ref, block, half):
        if half == 2:
            return ref.at[block]
        return ref.at[block, half * rows // 2 : (half + 1) * rows // 2]

    def tok_hop(block, half, place, peer):
        here = part(normed, block, half)
        return remote(here, here, tok_send.at[0], tok_recv.at[place], peer)

    def end_tok(block, half, place):
        return remote(
            part(normed, block, half), part(normed2, block, half), tok2_send.at[0],
            tok2_recv.at[place], m_peer,
        )

    def tok2_hop(block, place, peer):
        return remote(
            normed2.at[block], normed2.at[block], tok2_send.at[0], tok2_recv.at[place], peer
        )

    def quad(yy, xx):
        return 2 * yy + xx

    def tok_go(block, half, place, peer):
        tok_hop(block, half, place, peer).start()

    def tok_wait(block, half, place):
        tok_hop(block, half, place, x_peer).wait_recv()

    def tok2_wait(block, place):
        tok2_hop(block, place, x_peer).wait_recv()

    def tok_share(block, yy, xx):
        tok_go(block, 2, 6 + quad(yy, xx), c_peer)

    def tok2_share(block, yy, xx):
        tok2_hop(block, 4 + quad(yy, xx), c_peer).start()

    @pl.when(is_end)
    def _():
        end_tok(own_block, 0, 0).start()

    tok_go(own_block, 1, 1, x_peer)
    tok_go(own_block, 0, 2, y_peer)
    tok_go(own_block, 0, 0, x_peer)
    tok_go(own_block, 1, 3, y_peer)
    y_hop(1).start()
    tok_share(own_block, y, x)

    with scope("c_mate"):
        take(0, s_mate)
        send_m(0, s_mate)

        @pl.when(inner)
        def _():
            send_e(0, s_mate)
            take(0, first_of(near))
            send_m(0, first_of(near))
            take(0, first_of(mid))
            send_e(0, first_of(mid))

        @pl.when(is_end)
        def _():
            end_tok(own_block, 1, 0).start()
            send_m(1, s_own)

    with scope("tok_xy"):
        tok_wait(xb, 1, 1)
        tok_go(xb, 1, 5, y_peer)
        tok_wait(yb, 0, 2)
        tok_go(yb, 0, 4, x_peer)
        tok_wait(xb, 0, 0)
        tok_share(xb, y, 1 - x)
        tok_wait(yb, 1, 3)
        tok_share(yb, 1 - y, x)

    with scope("c_fwd"):
        @pl.when(inner)
        def _():
            take(0, second_of(mid))
            send_e(0, second_of(mid))
            take(0, second_of(near))
            send_m(0, second_of(near))

        @pl.when(inner & (c == 1))
        def _():
            out_send(s_own, send_m)

    with scope("tok2_own"):
        @pl.when(inner)
        def _():
            tok2_wait(own_block, 0)
            tok2_hop(own_block, 2, x_peer).start()
            tok2_hop(own_block, 3, y_peer).start()
            tok2_share(own_block, y, x)

    y_hop(2).start()
    y_hop(3).start()

    with scope("far1"):
        @pl.when(inner)
        def _():
            take(0, first_of(far))
            send_e(0, first_of(far))

    with scope("v_mate"):
        take(1, s_mate)
        send_m(1, s_mate)

    with scope("far2"):
        @pl.when(inner)
        def _():
            take(0, second_of(far))
            send_e(0, second_of(far))

    with scope("tok_db"):
        tok_wait(db, 0, 4)
        tok_wait(db, 1, 5)
        tok_share(db, 1 - y, 1 - x)

        @pl.when(is_end)
        def _():
            end_tok(db, 2, 1).start()

    with scope("v_near1"):
        @pl.when(inner)
        def _():
            take(1, first_of(near))
            send_m(1, first_of(near))

        @pl.when(inner & (c == 1))
        def _():
            out_hop(first_of(mid), send_e)

    with scope("tok_rest"):
        for yy in range(2):
            for xx in range(2):
                tok_wait(block_of(yy, xx, 1 - c), 2, 6 + quad(yy, xx))

    def columns(s):
        return pl.ds(pl.multiple_of(s * depth, depth), depth)

    def dot_t(a, w):
        return lax.dot_general(a, w, (((1,), (1,)), ((), ())), preferred_element_type=jnp.float32)

    def plane_dots(tokens, into, cols, weight_rows, source, add):
        total = into[:, cols] if add else None
        for half in range(2):
            s = 2 * source + half
            a = tokens[:, :, columns(s)].reshape(plane, depth)
            product = dot_t(a, win[s, weight_rows])
            total = product if total is None else total + product
        into[:, cols] = total

    conv_rows = slice(core, core + 3 * cr)
    conv_cols = slice(2 * qr, 2 * qr + 3 * cr)

    def early_dots(tokens, into, cols, weight_rows, count):
        plane_dots(tokens, into, cols, weight_rows, z, False)

        def step(k, carry):
            source = jnp.where(k == 1, near, jnp.where(k == 2, mid, far))
            plane_dots(tokens, into, cols, weight_rows, source, True)
            return carry

        lax.fori_loop(1, count, step, 0)

    with scope("c_dots"):
        @pl.when(is_end)
        def _():
            for source in (near, mid, far):
                for s in (first_of(source), second_of(source)):
                    take(0, s)

        early_dots(normed, acc, slice(0, core), slice(0, core), line)

    with scope("rot"):
        for copy in side_copies:
            copy.wait()
        lane = lax.broadcasted_iota(jnp.int32, (plane, qr), 1)
        half_dim = HEAD_DIM // 2
        table = trig[...]
        cos2 = jnp.where(lane < HEAD_DIM, table, pltpu.roll(table, HEAD_DIM, 1))
        sin2 = jnp.where(lane < HEAD_DIM, pltpu.roll(table, HEAD_DIM, 1), table)
        low = lane < HEAD_DIM
        first_half = lane % HEAD_DIM < half_dim

        def rot(v):
            partner = jnp.where(
                first_half, pltpu.roll(v, qr - half_dim, 1), pltpu.roll(v, half_dim, 1)
            )
            return v * cos2 + partner * sin2

        def bf(v):
            return v.astype(jnp.bfloat16).astype(jnp.float32)

        kv = jnp.where(low, bf(acc[:, qr : 2 * qr]), 0.0)
        ksq = jnp.sum(kv * kv, axis=-1, keepdims=True) / HEAD_DIM
        kgain = jnp.concatenate([kgain_ref[...], kgain_ref[...]], axis=1)
        kn = kv * lax.rsqrt(ksq + EPS) * kgain
        krot = rot(kn)
        keyed = jnp.where(y == 0, jnp.where(low, krot, 0.0), kv)
        keys[y, WINDOW : WINDOW + plane, :] = keyed.astype(jnp.bfloat16)

    bottom = pl.ds(WINDOW, WINDOW)
    top = pl.ds(plane, WINDOW)
    up = (jnp.minimum(2 * (z + 1) + y, 2 * line - 1), tp)
    down = (jnp.maximum(2 * (z - 1) + y, 0), tp)
    has_up = z < line - 1
    has_down = z > 0
    rim_up = remote(
        keys.at[y, top], keys.at[y, pl.ds(0, WINDOW)], rim_send.at[0], rim_recv.at[0], up
    )
    rim_down = remote(
        keys.at[y, bottom], keys.at[y, pl.ds(WINDOW + plane, WINDOW)], rim_send.at[1],
        rim_recv.at[1], down,
    )

    @pl.when(has_up)
    def _():
        rim_up.start()

    @pl.when(has_down)
    def _():
        rim_down.start()

    def kv_hop(place):
        begin, size = ((WINDOW, plane), (0, WINDOW), (WINDOW + plane, WINDOW))[place]
        here = keys.at[y, pl.ds(begin, size)]
        return remote(here, here, kv_send.at[place], kv_recv.at[place], y_peer)

    kv_hop(0).start()
    zero_rim = jnp.zeros((2, WINDOW, qr), jnp.bfloat16)

    @pl.when(z == 0)
    def _():
        keys[:, 0:WINDOW] = zero_rim

    @pl.when(z == line - 1)
    def _():
        keys[:, WINDOW + plane :] = zero_rim

    with scope("rotq"):
        qv = bf(acc[:, 0:qr])
        qq = qv * qv
        q_lo = jnp.sum(jnp.where(low, qq, 0.0), axis=-1, keepdims=True) / HEAD_DIM
        q_hi = jnp.sum(jnp.where(low, 0.0, qq), axis=-1, keepdims=True) / HEAD_DIM
        qgain = jnp.concatenate([qgain_ref[...], qgain_ref[...]], axis=1)
        qn = qv * lax.rsqrt(jnp.where(low, q_lo, q_hi) + EPS) * qgain
        qro = rot(qn)
        qrot[0] = jnp.where(low, qro, 0.0).astype(jnp.bfloat16)
        qrot[1] = jnp.where(low, pltpu.roll(qro, HEAD_DIM, 1), 0.0).astype(jnp.bfloat16)

    with scope("tok2_xb"):
        @pl.when(inner)
        def _():
            tok2_wait(xb, 2)
            tok2_share(xb, y, 1 - x)

    span = BLOCK + 2 * WINDOW
    total = plane * line

    def att_block(block):
        begin = pl.multiple_of(block * BLOCK, BLOCK)
        keyed = keys[0, pl.ds(begin, span), :]
        valued = keys[1, pl.ds(begin, span), :]
        qb = qrot[:, pl.ds(begin, BLOCK), :].reshape(2 * BLOCK, qr)
        scores = lax.dot_general(
            qb, keyed, (((1,), (1,)), ((), ())), preferred_element_type=jnp.float32
        ) * HEAD_DIM ** (-0.5)
        row = lax.broadcasted_iota(jnp.int32, (2 * BLOCK, span), 0)
        col = lax.broadcasted_iota(jnp.int32, (2 * BLOCK, span), 1)
        gap = row % BLOCK + WINDOW - col
        pos = z * plane + begin - WINDOW + col
        allowed = (gap <= WINDOW) & (gap >= -WINDOW) & (pos >= 0) & (pos < total)
        scores = jnp.where(allowed, scores, NEG_FILL)
        head = lax.broadcasted_iota(jnp.int32, (2 * BLOCK, 1), 0)
        sink = jnp.where(head < BLOCK, sink_ref[0, 2 * y], sink_ref[0, 2 * y + 1])
        peak = jnp.maximum(jnp.max(scores, axis=-1, keepdims=True), sink)
        expo = jnp.exp(scores - peak)
        denom = jnp.sum(expo, axis=-1, keepdims=True) + jnp.exp(sink - peak)
        weights = (expo / denom).astype(jnp.bfloat16)
        o = jnp.dot(weights, valued, preferred_element_type=jnp.float32)
        low_b = lax.broadcasted_iota(jnp.int32, (BLOCK, qr), 1) < HEAD_DIM
        both = jnp.where(low_b, o[:BLOCK], pltpu.roll(o[BLOCK:], HEAD_DIM, 1))
        mix_a[pl.ds(begin, BLOCK), :] = both.astype(jnp.bfloat16)

    nblocks = plane // BLOCK

    def att_inner(block, carry):
        att_block(block)
        return carry

    with scope("v_near2"):
        @pl.when(inner)
        def _():
            take(1, second_of(near))
            send_m(1, second_of(near))

        @pl.when(inner & (c == 0))
        def _():
            out_send(s_own, send_m)

    with scope("tok2_yb"):
        @pl.when(inner)
        def _():
            tok2_wait(yb, 3)
            tok2_share(yb, 1 - y, x)

    with scope("v_mid"):
        @pl.when(inner)
        def _():
            for s in (first_of(mid), second_of(mid)):
                take(1, s)

    with scope("v_dots"):
        @pl.when(inner)
        def _():
            early_dots(normed, acc, conv_cols, conv_rows, 3)

    def share_rims():
        with scope("rim_wait"):
            @pl.when(has_down)
            def _():
                rim_up.wait_recv()
                kv_hop(1).start()

            @pl.when(has_up)
            def _():
                rim_down.wait_recv()
                kv_hop(2).start()

    with scope("tok2_db"):
        @pl.when(inner)
        def _():
            tok2_wait(db, 1)
            tok2_share(db, 1 - y, 1 - x)

    with scope("o_mate"):
        @pl.when(is_end)
        def _():
            out_send(s_own, send_m)
            out_hop(s_mate, send_m)

    share_rims()

    with scope("o_mate"):
        @pl.when(inner)
        def _():
            out_hop(s_mate, send_m, send_e)

    def attend():
        with scope("kv_wait"):
            kv_hop(0).wait_recv()

        with scope("att_in"):
            lax.fori_loop(1, nblocks - 1, att_inner, 0)

        with scope("o_fwd"):
            @pl.when(inner)
            def _():
                out_hop(second_of(mid), send_e)

        with scope("kv_rims"):
            @pl.when(has_down)
            def _():
                kv_hop(1).wait_recv()

            @pl.when(has_up)
            def _():
                kv_hop(2).wait_recv()

        with scope("att_out"):
            def att_outer(k, carry):
                att_block(k * (nblocks - 1))
                return carry

            lax.fori_loop(0, 2, att_outer, 0)

    pad = 16
    zero_pad = jnp.zeros((pad, cr), jnp.bfloat16)
    taps = conv_ref[y]
    base = 2 * qr

    def convolve(ref, gate):
        p = ref[...].astype(jnp.float32)
        before = pltpu.roll(p, 1, 0)[pad : pad + plane]
        after = pltpu.roll(p, plane + 2 * pad - 1, 0)[pad : pad + plane]
        mixed = taps[0:1] * before + taps[1:2] * p[pad : pad + plane] + taps[2:3] * after
        return (gate * mixed).astype(jnp.bfloat16)

    prod_up = remote(
        prod.at[pl.ds(plane, pad)], prod.at[pl.ds(0, pad)], prod_send.at[0], prod_recv.at[0], up
    )
    prod_down = remote(
        prod.at[pl.ds(pad, pad)], prod.at[pl.ds(pad + plane, pad)],
        prod_send.at[1], prod_recv.at[1], down,
    )
    low_inner = inner & low_side
    high_inner = inner & (z >= 2)
    g_copy = remote(gated2, mix_c, g_send.at[0], g_recv.at[0], e_peer)

    @pl.when(inner)
    def _():
        with scope("tok2_rest"):
            for yy in range(2):
                for xx in range(2):
                    tok2_wait(block_of(yy, xx, 1 - c), 4 + quad(yy, xx))

        with scope("help_dots"):
            early_dots(normed2, acc2, slice(0, 3 * cr), conv_rows, 3)

        with scope("far_dots"):
            for s in (first_of(far), second_of(far)):
                take(1, s)
            plane_dots(normed2, acc2, slice(0, 3 * cr), conv_rows, far, True)
            plane_dots(normed, acc, conv_cols, conv_rows, far, True)

        with scope("prod"):
            left = bf(acc[:, base + cr : base + 2 * cr])
            inputs = bf(acc[:, base + 2 * cr : base + 3 * cr])
            prod[pad : pad + plane] = (left * inputs).astype(jnp.bfloat16)

            @pl.when(low_inner)
            def _():
                prod_up.start()

            @pl.when(high_inner)
            def _():
                prod_down.start()

            out_hop(first_of(near), send_m)

            prod2[pad : pad + plane] = (
                bf(acc2[:, cr : 2 * cr]) * bf(acc2[:, 2 * cr : 3 * cr])
            ).astype(jnp.bfloat16)

            @pl.when(z == 1)
            def _():
                prod2[0:pad] = zero_pad
                prod2[pad + plane :] = prod[pad : 2 * pad]
                prod[0:pad] = prod2[plane : plane + pad]

            @pl.when(z != 1)
            def _():
                prod2[0:pad] = prod[plane : plane + pad]
                prod2[pad + plane :] = zero_pad
                prod[pad + plane :] = prod2[pad : 2 * pad]

            gated2[...] = convolve(prod2, bf(acc2[:, 0:cr]))
            g_copy.start()

            @pl.when(c == 0)
            def _():
                out_hop(first_of(mid), send_e)

            out_hop(second_of(near), send_m)

        attend()

        with scope("prod_wait"):
            @pl.when(low_inner)
            def _():
                prod_down.wait_recv()

            @pl.when(high_inner)
            def _():
                prod_up.wait_recv()

            mix_c[...] = convolve(prod, bf(acc[:, base : base + cr]))

    @pl.when(is_end)
    def _():
        attend()
        with scope("g_wait"):
            g_copy.wait_recv()

    def group(cc):
        spans = [pl.ds(pl.multiple_of((2 * q + cc) * rows, rows), rows) for q in range(4)]
        return [jnp.concatenate([mix_a[w, :], mix_c[w, :]], axis=1) for w in spans]

    mine_rows = jnp.concatenate(group(c), axis=0)
    other_rows = jnp.concatenate(group(1 - c), axis=0)

    def rs_hop(src, dst, stage_id, s, peer):
        return remote(src, dst, rs_send.at[min(stage_id, 1)], rs_recv.at[stage_id, s], peer)

    def out_take(i):
        s = 2 * sources[i // 2] + i % 2
        out_hop(s)

    def out_forward(i):
        source = sources[i // 2]
        out_hop(first_of(source) if i % 2 == 0 else second_of(source), send_e)

    def stage_a(i):
        s = 2 * sources[i // 2] + i % 2
        weight = wout[s]
        s1[s] = jnp.dot(
            other_rows, weight, preferred_element_type=jnp.float32
        ).astype(jnp.bfloat16).reshape(2, 2, rows, depth)
        rs_hop(s1.at[s], r1.at[s], 0, s, c_peer).start()
        keep[s] = jnp.dot(
            mine_rows, weight, preferred_element_type=jnp.float32
        ).reshape(2, 2, rows, depth)

    d_peer = (2 * z + 1 - y, 2 * (1 - x) + c)
    corners = ((1 - y, 1 - x, d_peer), (1 - y, x, y_peer), (y, 1 - x, x_peer))

    staged = 4

    def stage_b(i):
        half = i % 2
        s = 2 * sources[i // 2] + half
        rs_hop(s1.at[s], r1.at[s], 0, s, c_peer).wait_recv()

        def put(j, yy, xx):
            s2[s, j] = (keep[s, yy, xx] + r1[s, yy, xx].astype(jnp.float32)).astype(jnp.bfloat16)

        if i < staged:
            for j in range(2):
                put(j, *((1 - y, j) if half == 0 else (j, 1 - x)))
            pair_hop(s, half).start()
        else:
            for j, (yy, xx, peer) in enumerate(corners):
                put(j, yy, xx)
                rs_hop(s2.at[s, j], r2.at[s, j], 1, s, peer).start()

    def pair_hop(s, half):
        peer = y_peer if half == 0 else x_peer
        return rs_hop(s2.at[s, 0:2], r2.at[s, 0:2], 1, s, peer)

    def last_hop(s, half):
        peer = x_peer if half == 0 else y_peer
        return rs_hop(s2.at[s, 2], r2.at[s, 2], 2, s, peer)

    def stage_c(i):
        half = i % 2
        s = 2 * sources[i // 2] + half
        pair_hop(s, half).wait_recv()
        yy, xx, j = (y, 1 - x, 1 - x) if half == 0 else (1 - y, x, 1 - y)
        piece = keep[s, yy, xx] + r1[s, yy, xx].astype(jnp.float32)
        s2[s, 2] = (piece + r2[s, j].astype(jnp.float32)).astype(jnp.bfloat16)
        last_hop(s, half).start()

    def stage_d(i):
        half = i % 2
        s = 2 * sources[i // 2] + half
        piece = keep[s, y, x] + r1[s, y, x].astype(jnp.float32)
        if i < staged:
            last_hop(s, half).wait_recv()
            piece = piece + r2[s, x if half == 0 else y].astype(jnp.float32)
            piece = piece + r2[s, 2].astype(jnp.float32)
        else:
            rs_hop(s2.at[s], r2.at[s], 1, s, d_peer).wait_recv()
            for j in range(3):
                piece = piece + r2[s, j].astype(jnp.float32)
        out_ref[:, columns(s)] = piece.astype(jnp.bfloat16)

    order = (
        ("a", (0, 1,)), ("f", (6,)), ("b", (0,)), ("a", (2,)), ("b", (1,)), ("a", (3,)),
        ("b", (2,)), ("w", (4,)), ("a", (4,)), ("b", (3,)), ("f", (7,)), ("w", (5,)), ("a", (5,)),
        ("b", (4,)), ("c", (0, 1,)), ("w", (6,)), ("a", (6,)), ("b", (5,)), ("c", (2, 3,)),
        ("w", (7,)), ("a", (7,)), ("b", (6, 7,)), ("d", (0, 1, 2, 3, 4, 6, 5, 7,)),
    )

    for step, places in order:
        for i in places:
            with scope(f"{step}{i}"):
                if step == "w":
                    pl.when(is_end)(functools.partial(out_take, i))
                elif step == "f":
                    pl.when(inner)(functools.partial(out_forward, i))
                elif step == "a":
                    if i in (2, 3):
                        pl.when(is_end)(functools.partial(out_take, i))
                    stage_a(i)
                elif step == "b":
                    stage_b(i)
                elif step == "c":
                    stage_c(i)
                else:
                    stage_d(i)

    def sent(ref, send):
        remote(ref, ref, send, w_recv.at[0, 0], m_peer).wait_send()

    def chunks_sent(kind, count, sends):
        if kind > 1:
            ref = wout.at[0:count, 0:qr] if kind == 2 else wout.at[0:count, qr : qr + cr]
        else:
            ref = win.at[0:count, 0:core] if kind == 0 else win.at[0:count, core : core + 3 * cr]
        sent(ref, sends.at[kind])

    with scope("sends"):
        for kind in range(4):
            y_hop(kind).wait_send()
        sent(normed.at[0:7], tok_send.at[0])
        sent(s1, rs_send.at[0])
        sent(s2, rs_send.at[1])

        kv_hop(0).wait_send()

        @pl.when(has_up)
        def _():
            rim_up.wait_send()
            kv_hop(2).wait_send()

        @pl.when(has_down)
        def _():
            rim_down.wait_send()
            kv_hop(1).wait_send()

        @pl.when(is_end)
        def _():
            sent(normed.at[0:2], tok2_send.at[0])
            for kind in range(4):
                chunks_sent(kind, 2, m_send)

        @pl.when(inner)
        def _():
            sent(normed2.at[0:6], tok2_send.at[0])
            g_copy.wait_send()
            for kind in range(4):
                chunks_sent(kind, 4, m_send)
            for kind in (0, 2, 3):
                chunks_sent(kind, 6, e_send)

        @pl.when(low_inner)
        def _():
            prod_up.wait_send()

        @pl.when(high_inner)
        def _():
            prod_down.wait_send()


def trig_table(total):
    half = HEAD_DIM // 2
    freq = np.float64(ROPE_BASE) ** (-np.arange(half) / half)
    angle = np.arange(total)[:, None] * freq
    cosine, sine = np.cos(angle), np.sin(angle)
    return np.concatenate([cosine, cosine, -sine, sine], axis=1).astype(np.float32)


def fused_device(
    tokens, norm_gain, query_weight, key_weight, value_weight, gate_weight, left_weight,
    input_weight, query_gain, key_gain, sink_logit, conv_weight, out_attention, out_conv,
):
    sp_count = lax.axis_size("sp")
    line = sp_count // 2
    rows, width = tokens.shape
    depth = query_weight.shape[1]
    qr = query_weight.shape[0] // 2
    kr = key_weight.shape[0]
    cr = gate_weight.shape[0] // 2
    fan = qr + kr + 3 * cr
    plane = 8 * rows
    dims = dict(line=line, rows=rows, depth=depth, qr=qr, kr=kr, cr=cr)
    hb = pl.BlockSpec(memory_space=pltpu.HBM)
    bf16, f32 = jnp.bfloat16, jnp.float32
    dma = pltpu.SemaphoreType.DMA
    n = sp_count
    scratch = [
        pltpu.VMEM((1, width), f32),
        pltpu.VMEM((1, HEAD_DIM), f32),
        pltpu.VMEM((1, HEAD_DIM), f32),
        pltpu.SMEM((1, 4), f32),
        pltpu.VMEM((2, 3, cr), f32),
        pltpu.VMEM((rows, width), bf16),
        pltpu.VMEM((plane, 2 * HEAD_DIM), f32),
        pltpu.VMEM((fan, depth), bf16),
        pltpu.VMEM((qr + cr, depth), bf16),
        pltpu.VMEM((n, fan, depth), bf16),
        pltpu.VMEM((n, qr + cr, depth), bf16),
        pltpu.VMEM((8, rows, width), bf16),
        pltpu.VMEM((8, rows, width), bf16),
        pltpu.VMEM((plane, 2 * qr + 3 * cr), f32),
        pltpu.VMEM((plane, 3 * cr), f32),
        pltpu.VMEM((2, plane + 2 * WINDOW, qr), bf16),
        pltpu.VMEM((plane + 32, cr), bf16),
        pltpu.VMEM((plane + 32, cr), bf16),
        pltpu.VMEM((plane, qr), bf16),
        pltpu.VMEM((plane, cr), bf16),
        pltpu.VMEM((plane, cr), bf16),
        pltpu.VMEM((2, plane, qr), bf16),
        pltpu.VMEM((n, 2, 2, rows, depth), f32),
        pltpu.VMEM((n, 2, 2, rows, depth), bf16),
        pltpu.VMEM((n, 2, 2, rows, depth), bf16),
        pltpu.VMEM((n, 3, rows, depth), bf16),
        pltpu.VMEM((n, 3, rows, depth), bf16),
        dma((11,)), dma((4,)), dma((4, n)), dma((4,)), dma((4,)),
        dma((1,)), dma((10,)), dma((1,)), dma((8,)), dma((2,)), dma((2,)), dma((3,)), dma((3,)),
        dma((2,)), dma((2,)),
        dma((1,)), dma((1,)), dma((2,)), dma((3, n)),
    ]
    taps = conv_weight.reshape(3, 2, cr).transpose(1, 0, 2)
    return pl.pallas_call(
        functools.partial(fused_kernel, dims),
        out_shape=jax.ShapeDtypeStruct((rows, width), bf16),
        in_specs=[hb] * 15,
        out_specs=pl.BlockSpec(memory_space=pltpu.VMEM),
        scratch_shapes=scratch,
        compiler_params=pltpu.CompilerParams(
            collective_id=0, has_side_effects=True, vmem_limit_bytes=32 * 1024 * 1024
        ),
    )(*(pltpu.with_memory_space_constraint(array, pltpu.HBM) for array in (
        tokens, norm_gain[None, :], query_weight, key_weight, value_weight, gate_weight,
        left_weight, input_weight, query_gain[None, :],
        key_gain[None, :], sink_logit[None, :], taps, out_attention, out_conv,
        jnp.asarray(trig_table(plane * line)),
    )))


def local_device(*args):
    tokens, query_weight, key_weight, gate_weight = args[0], args[2], args[3], args[5]
    fits = (
        lax.axis_size("sp") == 8
        and lax.axis_size("tp") == 4
        and query_weight.shape[1] % 128 == 0
        and query_weight.shape[0] == 4 * HEAD_DIM
        and key_weight.shape[0] == HEAD_DIM
        and gate_weight.shape[0] == 256
        and tokens.shape[0] % 32 == 0
        and 8 * tokens.shape[0] % BLOCK == 0
        and 8 * tokens.shape[0] >= 2 * BLOCK
    )
    return fused_device(*args) if fits else per_device(*args)


def solution(mesh):
    in_specs = (
        P(("sp", "tp"), None),
        P(),
        P("tp", "sp"),
        P("tp", "sp"),
        P("tp", "sp"),
        P("tp", "sp"),
        P("tp", "sp"),
        P("tp", "sp"),
        P(),
        P(),
        P("tp"),
        P(None, "tp"),
        P("tp", "sp"),
        P("tp", "sp"),
    )
    out_specs = P(("sp", "tp"), None)
    return jax.shard_map(
        local_device, mesh=mesh, in_specs=in_specs, out_specs=out_specs, check_vma=False
    )
```

```python
import functools

import jax
import jax.numpy as jnp
import numpy as np
from jax import lax
from jax.experimental import pallas as pl
from jax.experimental.pallas import tpu as pltpu
from jax.sharding import PartitionSpec as P

HEAD_DIM = 64
WINDOW = 128
BLOCK = 128


EPS = 1e-06
ROPE_BASE = 10000.0
NEG_FILL = -1e30


def with_halo(cells, sides, width):
    for axis, dim in sides:
        count = lax.axis_size(axis)
        ends = count - 1
        head = lax.slice_in_dim(cells, 0, width, axis=dim)
        tail = lax.slice_in_dim(cells, cells.shape[dim] - width, cells.shape[dim], axis=dim)
        cells = jnp.concatenate(
            [
                lax.ppermute(tail, axis, [(i, (i + 1) % count) for i in range(ends)]),
                cells,
                lax.ppermute(head, axis, [((i + 1) % count, i) for i in range(ends)]),
            ],
            axis=dim,
        )
    return cells


def normalize(values, gain):
    return values * lax.rsqrt(jnp.mean(values * values, axis=-1, keepdims=True) + EPS) * gain


def rotate(values, positions):
    half = values.shape[-1] // 2
    freq = ROPE_BASE ** (-jnp.arange(half, dtype=jnp.float32) / half)
    angle = positions[:, None] * freq
    cosine = jnp.cos(angle)[:, None, :]
    sine = jnp.sin(angle)[:, None, :]
    first = values[..., :half]
    second = values[..., half:]
    return jnp.concatenate(
        [first * cosine - second * sine, second * cosine + first * sine], axis=-1
    )


def project(rows, weight):
    return lax.dot_general(
        rows, weight, (((1,), (1,)), ((), ())), preferred_element_type=jnp.float32
    ).astype(jnp.bfloat16)


def attend(query_rot, key_rim, value_rim, sinks, offset, total):
    count = query_rot.shape[0]
    local_heads = query_rot.shape[1]
    kv_local = key_rim.shape[1]
    group = local_heads // kv_local
    span = BLOCK + 2 * WINDOW
    nblocks = count // BLOCK
    shaped = query_rot.reshape(nblocks, BLOCK, kv_local, group, HEAD_DIM)
    sink_group = sinks.reshape(kv_local, group)[:, :, None]

    def one_block(packed):
        block_index, query_block = packed
        begin = block_index * BLOCK
        key_block = lax.dynamic_slice_in_dim(key_rim, begin, span, 0)
        value_block = lax.dynamic_slice_in_dim(value_rim, begin, span, 0)
        scores = jnp.einsum(
            "qkgd,nkd->kgqn", query_block, key_block, preferred_element_type=jnp.float32
        ) * HEAD_DIM ** (-0.5)
        query_pos = offset + begin + jnp.arange(BLOCK, dtype=jnp.int32)
        key_pos = offset + begin - WINDOW + jnp.arange(span, dtype=jnp.int32)
        allowed = (
            (jnp.abs(query_pos[:, None] - key_pos[None, :]) <= WINDOW)
            & (key_pos >= 0)[None, :]
            & (key_pos < total)[None, :]
        )
        scores = jnp.where(allowed, scores, NEG_FILL)
        top = jnp.maximum(jnp.max(scores, axis=-1), sink_group)
        expo = jnp.exp(scores - top[..., None])
        denom = jnp.sum(expo, axis=-1) + jnp.exp(sink_group - top)
        weights = (expo / denom[..., None]).astype(jnp.bfloat16)
        return jnp.einsum(
            "kgqn,nkd->qkgd", weights, value_block, preferred_element_type=jnp.float32
        ).astype(jnp.bfloat16)

    result = lax.map(one_block, (jnp.arange(nblocks, dtype=jnp.int32), shaped))
    return result.reshape(count, local_heads * HEAD_DIM)


def per_device(
    tokens,
    norm_gain,
    query_weight,
    key_weight,
    value_weight,
    gate_weight,
    left_weight,
    input_weight,
    query_gain,
    key_gain,
    sink_logit,
    conv_weight,
    out_attention,
    out_conv,
):
    sp_count = lax.axis_size("sp")
    sp_place = lax.axis_index("sp")
    gathered = (
        lax.all_gather(query_weight, "sp", axis=1, tiled=True),
        lax.all_gather(key_weight, "sp", axis=1, tiled=True),
        lax.all_gather(value_weight, "sp", axis=1, tiled=True),
        lax.all_gather(gate_weight, "sp", axis=1, tiled=True),
        lax.all_gather(left_weight, "sp", axis=1, tiled=True),
        lax.all_gather(input_weight, "sp", axis=1, tiled=True),
        lax.all_gather(out_attention, "sp", axis=1, tiled=True),
        lax.all_gather(out_conv, "sp", axis=1, tiled=True),
    )
    (
        query_full,
        key_full,
        value_full,
        gate_full,
        left_full,
        input_full,
        attn_out_full,
        conv_out_full,
    ) = gathered
    normed = normalize(tokens.astype(jnp.float32), norm_gain).astype(jnp.bfloat16)
    widths = [
        query_full.shape[0],
        key_full.shape[0],
        value_full.shape[0],
        gate_full.shape[0],
        left_full.shape[0],
        input_full.shape[0],
    ]
    piece = lax.all_gather(normed, "tp", axis=0, tiled=True)
    joined = jnp.concatenate(
        [
            project(piece, weight)
            for weight in (query_full, key_full, value_full, gate_full, left_full, input_full)
        ],
        axis=1,
    )
    count = joined.shape[0]
    bounds = [0]
    for width in widths:
        bounds.append(bounds[-1] + width)
    query, keys, values, gate, left, inputs = [
        joined[:, bounds[place] : bounds[place + 1]] for place in range(6)
    ]
    offset = sp_place * count
    total = count * sp_count
    positions = (offset + jnp.arange(count, dtype=jnp.int32)).astype(jnp.float32)
    local_heads = widths[0] // HEAD_DIM
    kv_local = widths[1] // HEAD_DIM
    query_rot = rotate(
        normalize(query.reshape(count, local_heads, HEAD_DIM).astype(jnp.float32), query_gain),
        positions,
    ).astype(jnp.bfloat16)
    key_rot = rotate(
        normalize(keys.reshape(count, kv_local, HEAD_DIM).astype(jnp.float32), key_gain), positions
    ).astype(jnp.bfloat16)
    key_flat = key_rot.reshape(count, kv_local * HEAD_DIM)
    product = (left.astype(jnp.float32) * inputs.astype(jnp.float32)).astype(jnp.bfloat16)
    kv_width = widths[1]
    pair_rim = with_halo(jnp.concatenate([key_flat, values], axis=1), (("sp", 0),), WINDOW)
    product_rim = with_halo(product, (("sp", 0),), 1)
    rim_rows = pair_rim.shape[0]
    key_rim = pair_rim[:, :kv_width].reshape(rim_rows, kv_local, HEAD_DIM)
    value_rim = pair_rim[:, kv_width:].reshape(rim_rows, kv_local, HEAD_DIM)
    attended = attend(query_rot, key_rim, value_rim, sink_logit, offset, total)
    padded = product_rim.astype(jnp.float32)
    convolved = (
        conv_weight[0] * padded[:-2] + conv_weight[1] * padded[1:-1] + conv_weight[2] * padded[2:]
    )
    gated = (gate.astype(jnp.float32) * convolved).astype(jnp.bfloat16)
    return lax.psum_scatter(
        (
            jnp.dot(attended, attn_out_full, preferred_element_type=jnp.float32)
            + jnp.dot(gated, conv_out_full, preferred_element_type=jnp.float32)
        ).astype(jnp.bfloat16),
        "tp",
        scatter_dimension=0,
        tiled=True,
    )


MESH = pl.DeviceIdType.MESH


def fused_kernel(
    dims,
    tok_hbm, gain_hbm, q_hbm, k_hbm, v_hbm, g_hbm, l_hbm, i_hbm,
    qgain_hbm, kgain_hbm, sink_hbm, conv_hbm, oa_hbm, oc_hbm, trig_hbm,
    out_ref,
    gain_ref, qgain_ref, kgain_ref, sink_ref, conv_ref, tok, trig, stage, ostage, win, wout, normed, normed2, acc, acc2, keys, prod, prod2, mix_a, mix_c, gated2,
    qrot,
    keep, s1, r1, s2, r2,
    local_sem, y_send, w_recv, m_send, e_send,
    tok_send, tok_recv, tok2_send, tok2_recv, rim_send, rim_recv, kv_send, kv_recv, prod_send, prod_recv, g_send, g_recv,
    rs_send, rs_recv,
):
    scope = jax.named_scope
    line, rows, depth, qr, kr, cr = (
        dims["line"], dims["rows"], dims["depth"], dims["qr"], dims["kr"], dims["cr"]
    )
    sp = lax.axis_index("sp")
    tp = lax.axis_index("tp")
    z, y = sp // 2, sp % 2
    x, c = tp // 2, tp % 2
    y_peer = (2 * z + 1 - y, tp)
    x_peer = (sp, 2 * (1 - x) + c)
    c_peer = (sp, 2 * x + 1 - c)
    low_side = z < 2
    toward = jnp.where(low_side, 1, -1)
    is_end = (z == 0) | (z == line - 1)
    inner = (z > 0) & (z < line - 1)
    m_plane = z + toward
    e_plane = jnp.where(inner, z - toward, m_plane)
    m_peer = (2 * m_plane + y, tp)
    e_peer = (2 * e_plane + y, tp)
    near = jnp.where(inner, z - toward, z + toward)
    mid = jnp.where(inner, z + toward, z + 2 * toward)
    far = jnp.where(inner, z + 2 * toward, z + 3 * toward)
    sources = (z, near, mid, far)
    s_own = sp
    s_mate = 2 * z + 1 - y
    plane = 8 * rows
    core = qr + kr

    barrier = pltpu.get_barrier_semaphore()
    for peer in (y_peer, x_peer, c_peer, m_peer):
        pl.semaphore_signal(barrier, inc=1, device_id=peer, device_id_type=MESH)

    @pl.when(inner)
    def _():
        pl.semaphore_signal(barrier, inc=1, device_id=e_peer, device_id_type=MESH)

    def local(src, dst, place):
        copy = pltpu.make_async_copy(src, dst, local_sem.at[place])
        copy.start()
        return copy

    def in_pieces(which, dst, place):
        q0, c0 = pl.multiple_of(which * qr, qr), pl.multiple_of(which * cr, cr)
        local(q_hbm.at[pl.ds(q0, qr)], dst.at[0:qr], place)

        @pl.when(which == 0)
        def _():
            local(k_hbm, dst.at[qr:core], place)

        @pl.when(which == 1)
        def _():
            local(v_hbm, dst.at[qr:core], place)

        for turn, ref in enumerate((g_hbm, l_hbm, i_hbm)):
            lo = core + turn * cr
            local(ref.at[pl.ds(c0, cr)], dst.at[lo : lo + cr], place)
        return pltpu.make_async_copy(dst, dst, local_sem.at[place])

    def out_pieces(which, dst, place):
        q0, c0 = pl.multiple_of(which * qr, qr), pl.multiple_of(which * cr, cr)
        local(oa_hbm.at[pl.ds(q0, qr)], dst.at[0:qr], place)
        local(oc_hbm.at[pl.ds(c0, cr)], dst.at[qr : qr + cr], place)
        return pltpu.make_async_copy(dst, dst, local_sem.at[place])

    loads = [in_pieces(y, win.at[s_own], 0), in_pieces(1 - y, stage, 1)]
    tok_loads = [local(tok_hbm, tok, 2), local(gain_hbm, gain_ref, 3)]
    loads += [out_pieces(y, wout.at[s_own], 4), out_pieces(1 - y, ostage, 5)]
    side_copies = [
        local(trig_hbm.at[pl.ds(pl.multiple_of(z * plane, plane), plane)], trig, 6),
        local(qgain_hbm, qgain_ref, 7),
        local(kgain_hbm, kgain_ref, 8),
        local(sink_hbm, sink_ref, 9),
        local(conv_hbm, conv_ref, 10),
    ]

    with scope("barrier"):
        pl.semaphore_wait(barrier, 4 + inner.astype(jnp.int32))

    def remote(src, dst, send, recv, peer):
        return pltpu.make_async_remote_copy(
            src_ref=src, dst_ref=dst, send_sem=send, recv_sem=recv,
            device_id=peer, device_id_type=MESH,
        )

    def chunk(kind, s):
        if kind > 1:
            return wout.at[s, 0:qr] if kind == 2 else wout.at[s, qr : qr + cr]
        return win.at[s, 0:core] if kind == 0 else win.at[s, core : core + 3 * cr]

    def hop(kind, s, sends, peer):
        return remote(chunk(kind, s), chunk(kind, s), sends.at[kind], w_recv.at[kind, s], peer)

    def send_m(kind, s):
        hop(kind, s, m_send, m_peer).start()

    def send_e(kind, s):
        hop(kind, s, e_send, e_peer).start()

    def take(kind, s):
        hop(kind, s, m_send, m_peer).wait_recv()

    def y_hop(kind):
        if kind > 1:
            src = ostage.at[0:qr] if kind == 2 else ostage.at[qr : qr + cr]
        else:
            src = stage.at[0:core] if kind == 0 else stage.at[core : core + 3 * cr]
        return remote(src, chunk(kind, s_own), y_send.at[kind], w_recv.at[kind, s_own], y_peer)

    def out_hop(s, *sends):
        for kind in (2, 3):
            take(kind, s)
            for send in sends:
                send(kind, s)

    def out_send(s, send):
        send(2, s)
        send(3, s)

    def first_of(source):
        return 2 * source + y

    def second_of(source):
        return 2 * source + 1 - y

    for copy in loads:
        copy.wait()
    send_m(0, s_own)

    @pl.when(inner)
    def _():
        send_e(0, s_own)

    y_hop(0).start()

    @pl.when(inner)
    def _():
        send_m(1, s_own)
        out_send(s_own, send_e)

    with scope("norm"):
        for copy in tok_loads:
            copy.wait()
        t = tok[...].astype(jnp.float32)
        t = t * lax.rsqrt(jnp.mean(t * t, axis=-1, keepdims=True) + EPS) * gain_ref[...]

        def block_of(yy, xx, cc):
            return 4 * yy + 2 * xx + cc

        own_block = block_of(y, x, c)
        xb = block_of(y, 1 - x, c)
        yb = block_of(1 - y, x, c)
        db = block_of(1 - y, 1 - x, c)
        normed[own_block] = t.astype(jnp.bfloat16)

    def part(ref, block, half):
        if half == 2:
            return ref.at[block]
        return ref.at[block, half * rows // 2 : (half + 1) * rows // 2]

    def tok_hop(block, half, place, peer):
        here = part(normed, block, half)
        return remote(here, here, tok_send.at[0], tok_recv.at[place], peer)

    def end_tok(block, half, place):
        return remote(
            part(normed, block, half), part(normed2, block, half), tok2_send.at[0],
            tok2_recv.at[place], m_peer,
        )

    def tok2_hop(block, place, peer):
        return remote(
            normed2.at[block], normed2.at[block], tok2_send.at[0], tok2_recv.at[place], peer
        )

    def quad(yy, xx):
        return 2 * yy + xx

    def tok_go(block, half, place, peer):
        tok_hop(block, half, place, peer).start()

    def tok_wait(block, half, place):
        tok_hop(block, half, place, x_peer).wait_recv()

    def tok2_wait(block, place):
        tok2_hop(block, place, x_peer).wait_recv()

    def tok_share(block, yy, xx):
        tok_go(block, 2, 6 + quad(yy, xx), c_peer)

    def tok2_share(block, yy, xx):
        tok2_hop(block, 4 + quad(yy, xx), c_peer).start()

    @pl.when(is_end)
    def _():
        end_tok(own_block, 0, 0).start()

    tok_go(own_block, 1, 1, x_peer)
    tok_go(own_block, 0, 2, y_peer)
    tok_go(own_block, 0, 0, x_peer)
    tok_go(own_block, 1, 3, y_peer)
    y_hop(1).start()
    tok_share(own_block, y, x)

    with scope("c_mate"):
        take(0, s_mate)
        send_m(0, s_mate)

        @pl.when(inner)
        def _():
            send_e(0, s_mate)
            take(0, first_of(near))
            send_m(0, first_of(near))
            take(0, first_of(mid))
            send_e(0, first_of(mid))

        @pl.when(is_end)
        def _():
            end_tok(own_block, 1, 0).start()
            send_m(1, s_own)

    with scope("tok_xy"):
        tok_wait(xb, 1, 1)
        tok_go(xb, 1, 5, y_peer)
        tok_wait(yb, 0, 2)
        tok_go(yb, 0, 4, x_peer)
        tok_wait(xb, 0, 0)
        tok_share(xb, y, 1 - x)
        tok_wait(yb, 1, 3)
        tok_share(yb, 1 - y, x)

    with scope("c_fwd"):
        @pl.when(inner)
        def _():
            take(0, second_of(mid))
            send_e(0, second_of(mid))
            take(0, second_of(near))
            send_m(0, second_of(near))

        @pl.when(inner)
        def _():
            out_send(s_own, send_m)

    with scope("tok2_own"):
        @pl.when(inner)
        def _():
            tok2_wait(own_block, 0)
            tok2_hop(own_block, 2, x_peer).start()
            tok2_hop(own_block, 3, y_peer).start()
            tok2_share(own_block, y, x)

    y_hop(2).start()
    y_hop(3).start()

    with scope("far1"):
        @pl.when(inner)
        def _():
            take(0, first_of(far))
            send_e(0, first_of(far))

    with scope("v_mate"):
        take(1, s_mate)
        send_m(1, s_mate)

    with scope("far2"):
        @pl.when(inner)
        def _():
            take(0, second_of(far))
            send_e(0, second_of(far))

    with scope("tok_db"):
        tok_wait(db, 0, 4)
        tok_wait(db, 1, 5)
        tok_share(db, 1 - y, 1 - x)

        @pl.when(is_end)
        def _():
            end_tok(db, 2, 1).start()

    with scope("v_near1"):
        @pl.when(inner)
        def _():
            take(1, first_of(near))
            send_m(1, first_of(near))

        @pl.when(inner)
        def _():
            out_hop(first_of(mid), send_e)

    with scope("tok_rest"):
        for yy in range(2):
            for xx in range(2):
                tok_wait(block_of(yy, xx, 1 - c), 2, 6 + quad(yy, xx))

    def columns(s):
        return pl.ds(pl.multiple_of(s * depth, depth), depth)

    def dot_t(a, w):
        return lax.dot_general(a, w, (((1,), (1,)), ((), ())), preferred_element_type=jnp.float32)

    def plane_dots(tokens, into, cols, weight_rows, source, add):
        total = into[:, cols] if add else None
        for half in range(2):
            s = 2 * source + half
            a = tokens[:, :, columns(s)].reshape(plane, depth)
            product = dot_t(a, win[s, weight_rows])
            total = product if total is None else total + product
        into[:, cols] = total

    conv_rows = slice(core, core + 3 * cr)
    conv_cols = slice(2 * qr, 2 * qr + 3 * cr)

    def early_dots(tokens, into, cols, weight_rows, count):
        plane_dots(tokens, into, cols, weight_rows, z, False)

        def step(k, carry):
            source = jnp.where(k == 1, near, jnp.where(k == 2, mid, far))
            plane_dots(tokens, into, cols, weight_rows, source, True)
            return carry

        lax.fori_loop(1, count, step, 0)

    with scope("c_dots"):
        @pl.when(is_end)
        def _():
            for source in (near, mid, far):
                for s in (first_of(source), second_of(source)):
                    take(0, s)

        early_dots(normed, acc, slice(0, core), slice(0, core), line)

    with scope("rot"):
        for copy in side_copies:
            copy.wait()
        lane = lax.broadcasted_iota(jnp.int32, (plane, qr), 1)
        half_dim = HEAD_DIM // 2
        table = trig[...]
        cos2 = jnp.where(lane < HEAD_DIM, table, pltpu.roll(table, HEAD_DIM, 1))
        sin2 = jnp.where(lane < HEAD_DIM, pltpu.roll(table, HEAD_DIM, 1), table)
        low = lane < HEAD_DIM
        first_half = lane % HEAD_DIM < half_dim

        def rot(v):
            partner = jnp.where(
                first_half, pltpu.roll(v, qr - half_dim, 1), pltpu.roll(v, half_dim, 1)
            )
            return v * cos2 + partner * sin2

        def bf(v):
            return v.astype(jnp.bfloat16).astype(jnp.float32)

        kv = jnp.where(low, bf(acc[:, qr : 2 * qr]), 0.0)
        ksq = jnp.sum(kv * kv, axis=-1, keepdims=True) / HEAD_DIM
        kgain = jnp.concatenate([kgain_ref[...], kgain_ref[...]], axis=1)
        kn = kv * lax.rsqrt(ksq + EPS) * kgain
        krot = rot(kn)
        keyed = jnp.where(y == 0, jnp.where(low, krot, 0.0), kv)
        keys[y, WINDOW : WINDOW + plane, :] = keyed.astype(jnp.bfloat16)

    bottom = pl.ds(WINDOW, WINDOW)
    top = pl.ds(plane, WINDOW)
    up = (jnp.minimum(2 * (z + 1) + y, 2 * line - 1), tp)
    down = (jnp.maximum(2 * (z - 1) + y, 0), tp)
    has_up = z < line - 1
    has_down = z > 0
    rim_up = remote(
        keys.at[y, top], keys.at[y, pl.ds(0, WINDOW)], rim_send.at[0], rim_recv.at[0], up
    )
    rim_down = remote(
        keys.at[y, bottom], keys.at[y, pl.ds(WINDOW + plane, WINDOW)], rim_send.at[1],
        rim_recv.at[1], down,
    )

    @pl.when(has_up)
    def _():
        rim_up.start()

    @pl.when(has_down)
    def _():
        rim_down.start()

    def kv_hop(place):
        begin, size = ((WINDOW, plane), (0, WINDOW), (WINDOW + plane, WINDOW))[place]
        here = keys.at[y, pl.ds(begin, size)]
        return remote(here, here, kv_send.at[place], kv_recv.at[place], y_peer)

    kv_hop(0).start()
    zero_rim = jnp.zeros((2, WINDOW, qr), jnp.bfloat16)

    @pl.when(z == 0)
    def _():
        keys[:, 0:WINDOW] = zero_rim

    @pl.when(z == line - 1)
    def _():
        keys[:, WINDOW + plane :] = zero_rim

    with scope("rotq"):
        qv = bf(acc[:, 0:qr])
        qq = qv * qv
        q_lo = jnp.sum(jnp.where(low, qq, 0.0), axis=-1, keepdims=True) / HEAD_DIM
        q_hi = jnp.sum(jnp.where(low, 0.0, qq), axis=-1, keepdims=True) / HEAD_DIM
        qgain = jnp.concatenate([qgain_ref[...], qgain_ref[...]], axis=1)
        qn = qv * lax.rsqrt(jnp.where(low, q_lo, q_hi) + EPS) * qgain
        qro = rot(qn)
        qrot[0] = jnp.where(low, qro, 0.0).astype(jnp.bfloat16)
        qrot[1] = jnp.where(low, pltpu.roll(qro, HEAD_DIM, 1), 0.0).astype(jnp.bfloat16)

    with scope("tok2_xb"):
        @pl.when(inner)
        def _():
            tok2_wait(xb, 2)
            tok2_share(xb, y, 1 - x)

    span = BLOCK + 2 * WINDOW
    total = plane * line

    def att_block(block):
        begin = pl.multiple_of(block * BLOCK, BLOCK)
        keyed = keys[0, pl.ds(begin, span), :]
        valued = keys[1, pl.ds(begin, span), :]
        qb = qrot[:, pl.ds(begin, BLOCK), :].reshape(2 * BLOCK, qr)
        scores = lax.dot_general(
            qb, keyed, (((1,), (1,)), ((), ())), preferred_element_type=jnp.float32
        ) * HEAD_DIM ** (-0.5)
        row = lax.broadcasted_iota(jnp.int32, (2 * BLOCK, span), 0)
        col = lax.broadcasted_iota(jnp.int32, (2 * BLOCK, span), 1)
        gap = row % BLOCK + WINDOW - col
        pos = z * plane + begin - WINDOW + col
        allowed = (gap <= WINDOW) & (gap >= -WINDOW) & (pos >= 0) & (pos < total)
        scores = jnp.where(allowed, scores, NEG_FILL)
        head = lax.broadcasted_iota(jnp.int32, (2 * BLOCK, 1), 0)
        sink = jnp.where(head < BLOCK, sink_ref[0, 2 * y], sink_ref[0, 2 * y + 1])
        peak = jnp.maximum(jnp.max(scores, axis=-1, keepdims=True), sink)
        expo = jnp.exp(scores - peak)
        denom = jnp.sum(expo, axis=-1, keepdims=True) + jnp.exp(sink - peak)
        weights = (expo / denom).astype(jnp.bfloat16)
        o = jnp.dot(weights, valued, preferred_element_type=jnp.float32)
        low_b = lax.broadcasted_iota(jnp.int32, (BLOCK, qr), 1) < HEAD_DIM
        both = jnp.where(low_b, o[:BLOCK], pltpu.roll(o[BLOCK:], HEAD_DIM, 1))
        mix_a[pl.ds(begin, BLOCK), :] = both.astype(jnp.bfloat16)

    nblocks = plane // BLOCK

    def att_inner(block, carry):
        att_block(block)
        return carry

    with scope("v_near2"):
        @pl.when(inner)
        def _():
            take(1, second_of(near))
            send_m(1, second_of(near))

    with scope("tok2_yb"):
        @pl.when(inner)
        def _():
            tok2_wait(yb, 3)
            tok2_share(yb, 1 - y, x)

    with scope("v_mid"):
        @pl.when(inner)
        def _():
            for s in (first_of(mid), second_of(mid)):
                take(1, s)

    with scope("v_dots"):
        @pl.when(inner)
        def _():
            early_dots(normed, acc, conv_cols, conv_rows, 3)

    def share_rims():
        with scope("rim_wait"):
            @pl.when(has_down)
            def _():
                rim_up.wait_recv()
                kv_hop(1).start()

            @pl.when(has_up)
            def _():
                rim_down.wait_recv()
                kv_hop(2).start()

    with scope("tok2_db"):
        @pl.when(inner)
        def _():
            tok2_wait(db, 1)
            tok2_share(db, 1 - y, 1 - x)

    with scope("o_mate"):
        @pl.when(is_end)
        def _():
            out_send(s_own, send_m)
            out_hop(s_mate, send_m)

    share_rims()

    with scope("o_mate"):
        @pl.when(inner)
        def _():
            out_hop(s_mate, send_m, send_e)

    def attend():
        with scope("kv_wait"):
            kv_hop(0).wait_recv()

        with scope("att_in"):
            lax.fori_loop(1, nblocks - 1, att_inner, 0)

        with scope("o_fwd"):
            @pl.when(inner)
            def _():
                out_hop(second_of(mid), send_e)

        with scope("kv_rims"):
            @pl.when(has_down)
            def _():
                kv_hop(1).wait_recv()

            @pl.when(has_up)
            def _():
                kv_hop(2).wait_recv()

        with scope("att_out"):
            def att_outer(k, carry):
                att_block(k * (nblocks - 1))
                return carry

            lax.fori_loop(0, 2, att_outer, 0)

    pad = 16
    zero_pad = jnp.zeros((pad, cr), jnp.bfloat16)
    taps = conv_ref[y]
    base = 2 * qr

    def convolve(ref, gate):
        p = ref[...].astype(jnp.float32)
        before = pltpu.roll(p, 1, 0)[pad : pad + plane]
        after = pltpu.roll(p, plane + 2 * pad - 1, 0)[pad : pad + plane]
        mixed = taps[0:1] * before + taps[1:2] * p[pad : pad + plane] + taps[2:3] * after
        return (gate * mixed).astype(jnp.bfloat16)

    prod_up = remote(
        prod.at[pl.ds(plane, pad)], prod.at[pl.ds(0, pad)], prod_send.at[0], prod_recv.at[0], up
    )
    prod_down = remote(
        prod.at[pl.ds(pad, pad)], prod.at[pl.ds(pad + plane, pad)],
        prod_send.at[1], prod_recv.at[1], down,
    )
    low_inner = inner & low_side
    high_inner = inner & (z >= 2)
    g_copy = remote(gated2, mix_c, g_send.at[0], g_recv.at[0], e_peer)

    @pl.when(inner)
    def _():
        with scope("tok2_rest"):
            for yy in range(2):
                for xx in range(2):
                    tok2_wait(block_of(yy, xx, 1 - c), 4 + quad(yy, xx))

        with scope("help_dots"):
            early_dots(normed2, acc2, slice(0, 3 * cr), conv_rows, 3)

        with scope("far_dots"):
            for s in (first_of(far), second_of(far)):
                take(1, s)
            plane_dots(normed2, acc2, slice(0, 3 * cr), conv_rows, far, True)
            plane_dots(normed, acc, conv_cols, conv_rows, far, True)

        with scope("prod"):
            left = bf(acc[:, base + cr : base + 2 * cr])
            inputs = bf(acc[:, base + 2 * cr : base + 3 * cr])
            prod[pad : pad + plane] = (left * inputs).astype(jnp.bfloat16)

            @pl.when(low_inner)
            def _():
                prod_up.start()

            @pl.when(high_inner)
            def _():
                prod_down.start()

            out_hop(2 * near, send_m)

            prod2[pad : pad + plane] = (
                bf(acc2[:, cr : 2 * cr]) * bf(acc2[:, 2 * cr : 3 * cr])
            ).astype(jnp.bfloat16)

            @pl.when(z == 1)
            def _():
                prod2[0:pad] = zero_pad
                prod2[pad + plane :] = prod[pad : 2 * pad]
                prod[0:pad] = prod2[plane : plane + pad]

            @pl.when(z != 1)
            def _():
                prod2[0:pad] = prod[plane : plane + pad]
                prod2[pad + plane :] = zero_pad
                prod[pad + plane :] = prod2[pad : 2 * pad]

            gated2[...] = convolve(prod2, bf(acc2[:, 0:cr]))
            g_copy.start()

            out_hop(2 * near + 1, send_m)

        attend()

        with scope("prod_wait"):
            @pl.when(low_inner)
            def _():
                prod_down.wait_recv()

            @pl.when(high_inner)
            def _():
                prod_up.wait_recv()

            mix_c[...] = convolve(prod, bf(acc[:, base : base + cr]))

    @pl.when(is_end)
    def _():
        attend()
        with scope("g_wait"):
            g_copy.wait_recv()

    def group(cc):
        spans = [pl.ds(pl.multiple_of((2 * q + cc) * rows, rows), rows) for q in range(4)]
        return [jnp.concatenate([mix_a[w, :], mix_c[w, :]], axis=1) for w in spans]

    mine_rows = jnp.concatenate(group(c), axis=0)
    other_rows = jnp.concatenate(group(1 - c), axis=0)

    def rs_hop(src, dst, stage_id, s, peer):
        return remote(src, dst, rs_send.at[min(stage_id, 1)], rs_recv.at[stage_id, s], peer)

    def out_take(i):
        s = 2 * sources[i // 2] + i % 2
        out_hop(s)

    def out_forward(i):
        out_hop(2 * sources[i // 2] + i % 2, send_e)

    def stage_a(i):
        s = 2 * sources[i // 2] + i % 2
        weight = wout[s]
        s1[s] = jnp.dot(
            other_rows, weight, preferred_element_type=jnp.float32
        ).astype(jnp.bfloat16).reshape(2, 2, rows, depth)
        rs_hop(s1.at[s], r1.at[s], 0, s, c_peer).start()
        keep[s] = jnp.dot(
            mine_rows, weight, preferred_element_type=jnp.float32
        ).reshape(2, 2, rows, depth)

    d_peer = (2 * z + 1 - y, 2 * (1 - x) + c)
    corners = ((1 - y, 1 - x, d_peer), (1 - y, x, y_peer), (y, 1 - x, x_peer))

    staged = 6

    def stage_b(i):
        half = i % 2
        s = 2 * sources[i // 2] + half
        rs_hop(s1.at[s], r1.at[s], 0, s, c_peer).wait_recv()

        def put(j, yy, xx):
            s2[s, j] = (keep[s, yy, xx] + r1[s, yy, xx].astype(jnp.float32)).astype(jnp.bfloat16)

        if i < staged:
            for j in range(2):
                put(j, *((1 - y, j) if half == 0 else (j, 1 - x)))
            pair_hop(s, half).start()
        else:
            for j, (yy, xx, peer) in enumerate(corners):
                put(j, yy, xx)
                rs_hop(s2.at[s, j], r2.at[s, j], 1, s, peer).start()

    def pair_hop(s, half):
        peer = y_peer if half == 0 else x_peer
        return rs_hop(s2.at[s, 0:2], r2.at[s, 0:2], 1, s, peer)

    def last_hop(s, half):
        peer = x_peer if half == 0 else y_peer
        return rs_hop(s2.at[s, 2], r2.at[s, 2], 2, s, peer)

    def stage_c(i):
        half = i % 2
        s = 2 * sources[i // 2] + half
        pair_hop(s, half).wait_recv()
        yy, xx, j = (y, 1 - x, 1 - x) if half == 0 else (1 - y, x, 1 - y)
        piece = keep[s, yy, xx] + r1[s, yy, xx].astype(jnp.float32)
        s2[s, 2] = (piece + r2[s, j].astype(jnp.float32)).astype(jnp.bfloat16)
        last_hop(s, half).start()

    def stage_d(i):
        half = i % 2
        s = 2 * sources[i // 2] + half
        piece = keep[s, y, x] + r1[s, y, x].astype(jnp.float32)
        if i < staged:
            last_hop(s, half).wait_recv()
            piece = piece + r2[s, x if half == 0 else y].astype(jnp.float32)
            piece = piece + r2[s, 2].astype(jnp.float32)
        else:
            rs_hop(s2.at[s], r2.at[s], 1, s, d_peer).wait_recv()
            for j in range(3):
                piece = piece + r2[s, j].astype(jnp.float32)
        out_ref[:, columns(s)] = piece.astype(jnp.bfloat16)

    order = (
        ("a", (0, 1,)), ("f", (6,)), ("b", (0,)), ("a", (2,)), ("b", (1,)), ("a", (3,)),
        ("b", (2,)), ("w", (4,)), ("a", (4,)), ("b", (3,)), ("f", (7,)), ("w", (5,)), ("a", (5,)),
        ("b", (4,)), ("c", (0, 1,)), ("w", (6,)), ("a", (6,)), ("b", (5,)), ("c", (2, 3,)),
        ("w", (7,)), ("a", (7,)), ("b", (6, 7,)), ("c", (4, 5,)),
        ("d", (0, 1, 2, 3, 4, 6, 5, 7,)),
    )

    for step, places in order:
        for i in places:
            with scope(f"{step}{i}"):
                if step == "w":
                    pl.when(is_end)(functools.partial(out_take, i))
                elif step == "f":
                    pl.when(inner)(functools.partial(out_forward, i))
                elif step == "a":
                    if i in (2, 3):
                        pl.when(is_end)(functools.partial(out_take, i))
                    stage_a(i)
                elif step == "b":
                    stage_b(i)
                elif step == "c":
                    stage_c(i)
                else:
                    stage_d(i)

    def sent(ref, send):
        remote(ref, ref, send, w_recv.at[0, 0], m_peer).wait_send()

    def chunks_sent(kind, count, sends):
        if kind > 1:
            ref = wout.at[0:count, 0:qr] if kind == 2 else wout.at[0:count, qr : qr + cr]
        else:
            ref = win.at[0:count, 0:core] if kind == 0 else win.at[0:count, core : core + 3 * cr]
        sent(ref, sends.at[kind])

    with scope("sends"):
        for kind in range(4):
            y_hop(kind).wait_send()
        sent(normed.at[0:7], tok_send.at[0])
        sent(s1, rs_send.at[0])
        sent(s2, rs_send.at[1])

        kv_hop(0).wait_send()

        @pl.when(has_up)
        def _():
            rim_up.wait_send()
            kv_hop(2).wait_send()

        @pl.when(has_down)
        def _():
            rim_down.wait_send()
            kv_hop(1).wait_send()

        @pl.when(is_end)
        def _():
            sent(normed.at[0:2], tok2_send.at[0])
            for kind in range(4):
                chunks_sent(kind, 2, m_send)

        @pl.when(inner)
        def _():
            sent(normed2.at[0:6], tok2_send.at[0])
            g_copy.wait_send()
            for kind in range(4):
                chunks_sent(kind, 4, m_send)
            for kind in (0, 2, 3):
                chunks_sent(kind, 6, e_send)

        @pl.when(low_inner)
        def _():
            prod_up.wait_send()

        @pl.when(high_inner)
        def _():
            prod_down.wait_send()


def trig_table(total):
    half = HEAD_DIM // 2
    freq = np.float64(ROPE_BASE) ** (-np.arange(half) / half)
    angle = np.arange(total)[:, None] * freq
    cosine, sine = np.cos(angle), np.sin(angle)
    return np.concatenate([cosine, cosine, -sine, sine], axis=1).astype(np.float32)


def fused_device(
    tokens, norm_gain, query_weight, key_weight, value_weight, gate_weight, left_weight,
    input_weight, query_gain, key_gain, sink_logit, conv_weight, out_attention, out_conv,
):
    sp_count = lax.axis_size("sp")
    line = sp_count // 2
    rows, width = tokens.shape
    depth = query_weight.shape[1]
    qr = query_weight.shape[0] // 2
    kr = key_weight.shape[0]
    cr = gate_weight.shape[0] // 2
    fan = qr + kr + 3 * cr
    plane = 8 * rows
    dims = dict(line=line, rows=rows, depth=depth, qr=qr, kr=kr, cr=cr)
    hb = pl.BlockSpec(memory_space=pltpu.HBM)
    bf16, f32 = jnp.bfloat16, jnp.float32
    dma = pltpu.SemaphoreType.DMA
    n = sp_count
    scratch = [
        pltpu.VMEM((1, width), f32),
        pltpu.VMEM((1, HEAD_DIM), f32),
        pltpu.VMEM((1, HEAD_DIM), f32),
        pltpu.SMEM((1, 4), f32),
        pltpu.VMEM((2, 3, cr), f32),
        pltpu.VMEM((rows, width), bf16),
        pltpu.VMEM((plane, 2 * HEAD_DIM), f32),
        pltpu.VMEM((fan, depth), bf16),
        pltpu.VMEM((qr + cr, depth), bf16),
        pltpu.VMEM((n, fan, depth), bf16),
        pltpu.VMEM((n, qr + cr, depth), bf16),
        pltpu.VMEM((8, rows, width), bf16),
        pltpu.VMEM((8, rows, width), bf16),
        pltpu.VMEM((plane, 2 * qr + 3 * cr), f32),
        pltpu.VMEM((plane, 3 * cr), f32),
        pltpu.VMEM((2, plane + 2 * WINDOW, qr), bf16),
        pltpu.VMEM((plane + 32, cr), bf16),
        pltpu.VMEM((plane + 32, cr), bf16),
        pltpu.VMEM((plane, qr), bf16),
        pltpu.VMEM((plane, cr), bf16),
        pltpu.VMEM((plane, cr), bf16),
        pltpu.VMEM((2, plane, qr), bf16),
        pltpu.VMEM((n, 2, 2, rows, depth), f32),
        pltpu.VMEM((n, 2, 2, rows, depth), bf16),
        pltpu.VMEM((n, 2, 2, rows, depth), bf16),
        pltpu.VMEM((n, 3, rows, depth), bf16),
        pltpu.VMEM((n, 3, rows, depth), bf16),
        dma((11,)), dma((4,)), dma((4, n)), dma((4,)), dma((4,)),
        dma((1,)), dma((10,)), dma((1,)), dma((8,)), dma((2,)), dma((2,)), dma((3,)), dma((3,)),
        dma((2,)), dma((2,)),
        dma((1,)), dma((1,)), dma((2,)), dma((3, n)),
    ]
    taps = conv_weight.reshape(3, 2, cr).transpose(1, 0, 2)
    return pl.pallas_call(
        functools.partial(fused_kernel, dims),
        out_shape=jax.ShapeDtypeStruct((rows, width), bf16),
        in_specs=[hb] * 15,
        out_specs=pl.BlockSpec(memory_space=pltpu.VMEM),
        scratch_shapes=scratch,
        compiler_params=pltpu.CompilerParams(
            collective_id=0, has_side_effects=True, vmem_limit_bytes=32 * 1024 * 1024
        ),
    )(*(pltpu.with_memory_space_constraint(array, pltpu.HBM) for array in (
        tokens, norm_gain[None, :], query_weight, key_weight, value_weight, gate_weight,
        left_weight, input_weight, query_gain[None, :],
        key_gain[None, :], sink_logit[None, :], taps, out_attention, out_conv,
        jnp.asarray(trig_table(plane * line)),
    )))


def local_device(*args):
    tokens, query_weight, key_weight, gate_weight = args[0], args[2], args[3], args[5]
    fits = (
        lax.axis_size("sp") == 8
        and lax.axis_size("tp") == 4
        and query_weight.shape[1] % 128 == 0
        and query_weight.shape[0] == 4 * HEAD_DIM
        and key_weight.shape[0] == HEAD_DIM
        and gate_weight.shape[0] == 256
        and tokens.shape[0] % 32 == 0
        and 8 * tokens.shape[0] % BLOCK == 0
        and 8 * tokens.shape[0] >= 2 * BLOCK
    )
    return fused_device(*args) if fits else per_device(*args)


def solution(mesh):
    in_specs = (
        P(("sp", "tp"), None),
        P(),
        P("tp", "sp"),
        P("tp", "sp"),
        P("tp", "sp"),
        P("tp", "sp"),
        P("tp", "sp"),
        P("tp", "sp"),
        P(),
        P(),
        P("tp"),
        P(None, "tp"),
        P("tp", "sp"),
        P("tp", "sp"),
    )
    out_specs = P(("sp", "tp"), None)
    return jax.shard_map(
        local_device, mesh=mesh, in_specs=in_specs, out_specs=out_specs, check_vma=False
    )
```

```python
import functools

import jax
import jax.numpy as jnp
import numpy as np
from jax import lax
from jax.experimental import pallas as pl
from jax.experimental.pallas import tpu as pltpu
from jax.sharding import PartitionSpec as P

HEAD_DIM = 64
WINDOW = 128
BLOCK = 128


EPS = 1e-06
ROPE_BASE = 10000.0
NEG_FILL = -1e30


def with_halo(cells, sides, width):
    for axis, dim in sides:
        count = lax.axis_size(axis)
        ends = count - 1
        head = lax.slice_in_dim(cells, 0, width, axis=dim)
        tail = lax.slice_in_dim(cells, cells.shape[dim] - width, cells.shape[dim], axis=dim)
        cells = jnp.concatenate(
            [
                lax.ppermute(tail, axis, [(i, (i + 1) % count) for i in range(ends)]),
                cells,
                lax.ppermute(head, axis, [((i + 1) % count, i) for i in range(ends)]),
            ],
            axis=dim,
        )
    return cells


def normalize(values, gain):
    return values * lax.rsqrt(jnp.mean(values * values, axis=-1, keepdims=True) + EPS) * gain


def rotate(values, positions):
    half = values.shape[-1] // 2
    freq = ROPE_BASE ** (-jnp.arange(half, dtype=jnp.float32) / half)
    angle = positions[:, None] * freq
    cosine = jnp.cos(angle)[:, None, :]
    sine = jnp.sin(angle)[:, None, :]
    first = values[..., :half]
    second = values[..., half:]
    return jnp.concatenate(
        [first * cosine - second * sine, second * cosine + first * sine], axis=-1
    )


def project(rows, weight):
    return lax.dot_general(
        rows, weight, (((1,), (1,)), ((), ())), preferred_element_type=jnp.float32
    ).astype(jnp.bfloat16)


def attend(query_rot, key_rim, value_rim, sinks, offset, total):
    count = query_rot.shape[0]
    local_heads = query_rot.shape[1]
    kv_local = key_rim.shape[1]
    group = local_heads // kv_local
    span = BLOCK + 2 * WINDOW
    nblocks = count // BLOCK
    shaped = query_rot.reshape(nblocks, BLOCK, kv_local, group, HEAD_DIM)
    sink_group = sinks.reshape(kv_local, group)[:, :, None]

    def one_block(packed):
        block_index, query_block = packed
        begin = block_index * BLOCK
        key_block = lax.dynamic_slice_in_dim(key_rim, begin, span, 0)
        value_block = lax.dynamic_slice_in_dim(value_rim, begin, span, 0)
        scores = jnp.einsum(
            "qkgd,nkd->kgqn", query_block, key_block, preferred_element_type=jnp.float32
        ) * HEAD_DIM ** (-0.5)
        query_pos = offset + begin + jnp.arange(BLOCK, dtype=jnp.int32)
        key_pos = offset + begin - WINDOW + jnp.arange(span, dtype=jnp.int32)
        allowed = (
            (jnp.abs(query_pos[:, None] - key_pos[None, :]) <= WINDOW)
            & (key_pos >= 0)[None, :]
            & (key_pos < total)[None, :]
        )
        scores = jnp.where(allowed, scores, NEG_FILL)
        top = jnp.maximum(jnp.max(scores, axis=-1), sink_group)
        expo = jnp.exp(scores - top[..., None])
        denom = jnp.sum(expo, axis=-1) + jnp.exp(sink_group - top)
        weights = (expo / denom[..., None]).astype(jnp.bfloat16)
        return jnp.einsum(
            "kgqn,nkd->qkgd", weights, value_block, preferred_element_type=jnp.float32
        ).astype(jnp.bfloat16)

    result = lax.map(one_block, (jnp.arange(nblocks, dtype=jnp.int32), shaped))
    return result.reshape(count, local_heads * HEAD_DIM)


def per_device(
    tokens,
    norm_gain,
    query_weight,
    key_weight,
    value_weight,
    gate_weight,
    left_weight,
    input_weight,
    query_gain,
    key_gain,
    sink_logit,
    conv_weight,
    out_attention,
    out_conv,
):
    sp_count = lax.axis_size("sp")
    sp_place = lax.axis_index("sp")
    gathered = (
        lax.all_gather(query_weight, "sp", axis=1, tiled=True),
        lax.all_gather(key_weight, "sp", axis=1, tiled=True),
        lax.all_gather(value_weight, "sp", axis=1, tiled=True),
        lax.all_gather(gate_weight, "sp", axis=1, tiled=True),
        lax.all_gather(left_weight, "sp", axis=1, tiled=True),
        lax.all_gather(input_weight, "sp", axis=1, tiled=True),
        lax.all_gather(out_attention, "sp", axis=1, tiled=True),
        lax.all_gather(out_conv, "sp", axis=1, tiled=True),
    )
    (
        query_full,
        key_full,
        value_full,
        gate_full,
        left_full,
        input_full,
        attn_out_full,
        conv_out_full,
    ) = gathered
    normed = normalize(tokens.astype(jnp.float32), norm_gain).astype(jnp.bfloat16)
    widths = [
        query_full.shape[0],
        key_full.shape[0],
        value_full.shape[0],
        gate_full.shape[0],
        left_full.shape[0],
        input_full.shape[0],
    ]
    piece = lax.all_gather(normed, "tp", axis=0, tiled=True)
    joined = jnp.concatenate(
        [
            project(piece, weight)
            for weight in (query_full, key_full, value_full, gate_full, left_full, input_full)
        ],
        axis=1,
    )
    count = joined.shape[0]
    bounds = [0]
    for width in widths:
        bounds.append(bounds[-1] + width)
    query, keys, values, gate, left, inputs = [
        joined[:, bounds[place] : bounds[place + 1]] for place in range(6)
    ]
    offset = sp_place * count
    total = count * sp_count
    positions = (offset + jnp.arange(count, dtype=jnp.int32)).astype(jnp.float32)
    local_heads = widths[0] // HEAD_DIM
    kv_local = widths[1] // HEAD_DIM
    query_rot = rotate(
        normalize(query.reshape(count, local_heads, HEAD_DIM).astype(jnp.float32), query_gain),
        positions,
    ).astype(jnp.bfloat16)
    key_rot = rotate(
        normalize(keys.reshape(count, kv_local, HEAD_DIM).astype(jnp.float32), key_gain), positions
    ).astype(jnp.bfloat16)
    key_flat = key_rot.reshape(count, kv_local * HEAD_DIM)
    product = (left.astype(jnp.float32) * inputs.astype(jnp.float32)).astype(jnp.bfloat16)
    kv_width = widths[1]
    pair_rim = with_halo(jnp.concatenate([key_flat, values], axis=1), (("sp", 0),), WINDOW)
    product_rim = with_halo(product, (("sp", 0),), 1)
    rim_rows = pair_rim.shape[0]
    key_rim = pair_rim[:, :kv_width].reshape(rim_rows, kv_local, HEAD_DIM)
    value_rim = pair_rim[:, kv_width:].reshape(rim_rows, kv_local, HEAD_DIM)
    attended = attend(query_rot, key_rim, value_rim, sink_logit, offset, total)
    padded = product_rim.astype(jnp.float32)
    convolved = (
        conv_weight[0] * padded[:-2] + conv_weight[1] * padded[1:-1] + conv_weight[2] * padded[2:]
    )
    gated = (gate.astype(jnp.float32) * convolved).astype(jnp.bfloat16)
    return lax.psum_scatter(
        (
            jnp.dot(attended, attn_out_full, preferred_element_type=jnp.float32)
            + jnp.dot(gated, conv_out_full, preferred_element_type=jnp.float32)
        ).astype(jnp.bfloat16),
        "tp",
        scatter_dimension=0,
        tiled=True,
    )


MESH = pl.DeviceIdType.MESH


def fused_kernel(
    dims,
    tok_hbm, gain_hbm, q_hbm, k_hbm, v_hbm, g_hbm, l_hbm, i_hbm,
    qgain_hbm, kgain_hbm, sink_hbm, conv_hbm, oa_hbm, oc_hbm, trig_hbm,
    out_ref,
    gain_ref, qgain_ref, kgain_ref, sink_ref, conv_ref, tok, trig, stage, ostage, win, wout, normed, normed2, acc, acc2, keys, prod, prod2, mix_a, mix_c, gated2,
    qrot,
    keep, s1, r1, s2, r2,
    local_sem, y_send, w_recv, m_send, e_send,
    tok_send, tok_recv, tok2_send, tok2_recv, rim_send, rim_recv, kv_send, kv_recv, prod_send, prod_recv, g_send, g_recv,
    rs_send, rs_recv,
):
    scope = jax.named_scope
    line, rows, depth, qr, kr, cr = (
        dims["line"], dims["rows"], dims["depth"], dims["qr"], dims["kr"], dims["cr"]
    )
    sp = lax.axis_index("sp")
    tp = lax.axis_index("tp")
    z, y = sp // 2, sp % 2
    x, c = tp // 2, tp % 2
    y_peer = (2 * z + 1 - y, tp)
    x_peer = (sp, 2 * (1 - x) + c)
    c_peer = (sp, 2 * x + 1 - c)
    low_side = z < 2
    toward = jnp.where(low_side, 1, -1)
    is_end = (z == 0) | (z == line - 1)
    inner = (z > 0) & (z < line - 1)
    m_plane = z + toward
    e_plane = jnp.where(inner, z - toward, m_plane)
    m_peer = (2 * m_plane + y, tp)
    e_peer = (2 * e_plane + y, tp)
    near = jnp.where(inner, z - toward, z + toward)
    mid = jnp.where(inner, z + toward, z + 2 * toward)
    far = jnp.where(inner, z + 2 * toward, z + 3 * toward)
    sources = (z, near, mid, far)
    s_own = sp
    s_mate = 2 * z + 1 - y
    plane = 8 * rows
    core = qr + kr

    barrier = pltpu.get_barrier_semaphore()
    for peer in (y_peer, x_peer, c_peer, m_peer):
        pl.semaphore_signal(barrier, inc=1, device_id=peer, device_id_type=MESH)

    @pl.when(inner)
    def _():
        pl.semaphore_signal(barrier, inc=1, device_id=e_peer, device_id_type=MESH)

    def local(src, dst, place):
        copy = pltpu.make_async_copy(src, dst, local_sem.at[place])
        copy.start()
        return copy

    def in_pieces(which, dst, place):
        q0, c0 = pl.multiple_of(which * qr, qr), pl.multiple_of(which * cr, cr)
        local(q_hbm.at[pl.ds(q0, qr)], dst.at[0:qr], place)

        @pl.when(which == 0)
        def _():
            local(k_hbm, dst.at[qr:core], place)

        @pl.when(which == 1)
        def _():
            local(v_hbm, dst.at[qr:core], place)

        for turn, ref in enumerate((g_hbm, l_hbm, i_hbm)):
            lo = core + turn * cr
            local(ref.at[pl.ds(c0, cr)], dst.at[lo : lo + cr], place)
        return pltpu.make_async_copy(dst, dst, local_sem.at[place])

    def out_pieces(which, dst, place):
        q0, c0 = pl.multiple_of(which * qr, qr), pl.multiple_of(which * cr, cr)
        local(oa_hbm.at[pl.ds(q0, qr)], dst.at[0:qr], place)
        local(oc_hbm.at[pl.ds(c0, cr)], dst.at[qr : qr + cr], place)
        return pltpu.make_async_copy(dst, dst, local_sem.at[place])

    loads = [in_pieces(y, win.at[s_own], 0), in_pieces(1 - y, stage, 1)]
    tok_loads = [local(tok_hbm, tok, 2), local(gain_hbm, gain_ref, 3)]
    loads += [out_pieces(y, wout.at[s_own], 4), out_pieces(1 - y, ostage, 5)]
    side_copies = [
        local(trig_hbm.at[pl.ds(pl.multiple_of(z * plane, plane), plane)], trig, 6),
        local(qgain_hbm, qgain_ref, 7),
        local(kgain_hbm, kgain_ref, 8),
        local(sink_hbm, sink_ref, 9),
        local(conv_hbm, conv_ref, 10),
    ]

    with scope("barrier"):
        pl.semaphore_wait(barrier, 4 + inner.astype(jnp.int32))

    def remote(src, dst, send, recv, peer):
        return pltpu.make_async_remote_copy(
            src_ref=src, dst_ref=dst, send_sem=send, recv_sem=recv,
            device_id=peer, device_id_type=MESH,
        )

    def chunk(kind, s):
        if kind > 1:
            return wout.at[s, 0:qr] if kind == 2 else wout.at[s, qr : qr + cr]
        return win.at[s, 0:core] if kind == 0 else win.at[s, core : core + 3 * cr]

    def hop(kind, s, sends, peer):
        return remote(chunk(kind, s), chunk(kind, s), sends.at[kind], w_recv.at[kind, s], peer)

    def send_m(kind, s):
        hop(kind, s, m_send, m_peer).start()

    def send_e(kind, s):
        hop(kind, s, e_send, e_peer).start()

    def take(kind, s):
        hop(kind, s, m_send, m_peer).wait_recv()

    def y_hop(kind):
        if kind > 1:
            src = ostage.at[0:qr] if kind == 2 else ostage.at[qr : qr + cr]
        else:
            src = stage.at[0:core] if kind == 0 else stage.at[core : core + 3 * cr]
        return remote(src, chunk(kind, s_own), y_send.at[kind], w_recv.at[kind, s_own], y_peer)

    def out_hop(s, *sends):
        for kind in (2, 3):
            take(kind, s)
            for send in sends:
                send(kind, s)

    def out_send(s, send):
        send(2, s)
        send(3, s)

    def first_of(source):
        return 2 * source + y

    def second_of(source):
        return 2 * source + 1 - y

    for copy in loads:
        copy.wait()
    send_m(0, s_own)

    @pl.when(inner)
    def _():
        send_e(0, s_own)

    y_hop(0).start()

    @pl.when(inner)
    def _():
        send_m(1, s_own)
        out_send(s_own, send_e)

    with scope("norm"):
        for copy in tok_loads:
            copy.wait()
        t = tok[...].astype(jnp.float32)
        t = t * lax.rsqrt(jnp.mean(t * t, axis=-1, keepdims=True) + EPS) * gain_ref[...]

        def block_of(yy, xx, cc):
            return 4 * yy + 2 * xx + cc

        own_block = block_of(y, x, c)
        xb = block_of(y, 1 - x, c)
        yb = block_of(1 - y, x, c)
        db = block_of(1 - y, 1 - x, c)
        normed[own_block] = t.astype(jnp.bfloat16)

    def part(ref, block, half):
        if half == 2:
            return ref.at[block]
        return ref.at[block, half * rows // 2 : (half + 1) * rows // 2]

    def tok_hop(block, half, place, peer):
        here = part(normed, block, half)
        return remote(here, here, tok_send.at[0], tok_recv.at[place], peer)

    def end_tok(block, half, place):
        return remote(
            part(normed, block, half), part(normed2, block, half), tok2_send.at[0],
            tok2_recv.at[place], m_peer,
        )

    def tok2_hop(block, place, peer):
        return remote(
            normed2.at[block], normed2.at[block], tok2_send.at[0], tok2_recv.at[place], peer
        )

    def quad(yy, xx):
        return 2 * yy + xx

    def tok_go(block, half, place, peer):
        tok_hop(block, half, place, peer).start()

    def tok_wait(block, half, place):
        tok_hop(block, half, place, x_peer).wait_recv()

    def tok2_wait(block, place):
        tok2_hop(block, place, x_peer).wait_recv()

    def tok_share(block, yy, xx):
        tok_go(block, 2, 6 + quad(yy, xx), c_peer)

    def tok2_share(block, yy, xx):
        tok2_hop(block, 4 + quad(yy, xx), c_peer).start()

    @pl.when(is_end)
    def _():
        end_tok(own_block, 0, 0).start()

    tok_go(own_block, 1, 1, x_peer)
    tok_go(own_block, 0, 2, y_peer)
    tok_go(own_block, 0, 0, x_peer)
    tok_go(own_block, 1, 3, y_peer)
    y_hop(1).start()
    tok_share(own_block, y, x)

    with scope("c_mate"):
        take(0, s_mate)
        send_m(0, s_mate)

        @pl.when(inner)
        def _():
            send_e(0, s_mate)
            take(0, first_of(near))
            send_m(0, first_of(near))
            take(0, first_of(mid))
            send_e(0, first_of(mid))

        @pl.when(is_end)
        def _():
            end_tok(own_block, 1, 0).start()
            send_m(1, s_own)

    with scope("tok_xy"):
        tok_wait(xb, 1, 1)
        tok_go(xb, 1, 5, y_peer)
        tok_wait(yb, 0, 2)
        tok_go(yb, 0, 4, x_peer)
        tok_wait(xb, 0, 0)
        tok_share(xb, y, 1 - x)
        tok_wait(yb, 1, 3)
        tok_share(yb, 1 - y, x)

    with scope("c_fwd"):
        @pl.when(inner)
        def _():
            take(0, second_of(mid))
            send_e(0, second_of(mid))
            take(0, second_of(near))
            send_m(0, second_of(near))
            send_m(2, s_own)

        @pl.when(inner & (c == 1))
        def _():
            send_m(3, s_own)

    with scope("tok2_own"):
        @pl.when(inner)
        def _():
            tok2_wait(own_block, 0)
            tok2_hop(own_block, 2, x_peer).start()
            tok2_hop(own_block, 3, y_peer).start()
            tok2_share(own_block, y, x)

    y_hop(2).start()
    y_hop(3).start()

    with scope("far1"):
        @pl.when(inner)
        def _():
            take(0, first_of(far))
            send_e(0, first_of(far))

    with scope("v_mate"):
        take(1, s_mate)
        send_m(1, s_mate)

    with scope("far2"):
        @pl.when(inner)
        def _():
            take(0, second_of(far))
            send_e(0, second_of(far))

    with scope("tok_db"):
        tok_wait(db, 0, 4)
        tok_wait(db, 1, 5)
        tok_share(db, 1 - y, 1 - x)

        @pl.when(is_end)
        def _():
            end_tok(db, 2, 1).start()

    with scope("v_near1"):
        @pl.when(inner)
        def _():
            take(1, first_of(near))
            send_m(1, first_of(near))

        @pl.when(inner)
        def _():
            take(2, first_of(mid))
            send_e(2, first_of(mid))

        @pl.when(inner & (c == 1))
        def _():
            take(3, first_of(mid))
            send_e(3, first_of(mid))

    with scope("tok_rest"):
        for yy in range(2):
            for xx in range(2):
                tok_wait(block_of(yy, xx, 1 - c), 2, 6 + quad(yy, xx))

    def columns(s):
        return pl.ds(pl.multiple_of(s * depth, depth), depth)

    def dot_t(a, w):
        return lax.dot_general(a, w, (((1,), (1,)), ((), ())), preferred_element_type=jnp.float32)

    def plane_dots(tokens, into, cols, weight_rows, source, add):
        total = into[:, cols] if add else None
        for half in range(2):
            s = 2 * source + half
            a = tokens[:, :, columns(s)].reshape(plane, depth)
            product = dot_t(a, win[s, weight_rows])
            total = product if total is None else total + product
        into[:, cols] = total

    conv_rows = slice(core, core + 3 * cr)
    conv_cols = slice(2 * qr, 2 * qr + 3 * cr)

    def early_dots(tokens, into, cols, weight_rows, count):
        plane_dots(tokens, into, cols, weight_rows, z, False)

        def step(k, carry):
            source = jnp.where(k == 1, near, jnp.where(k == 2, mid, far))
            plane_dots(tokens, into, cols, weight_rows, source, True)
            return carry

        lax.fori_loop(1, count, step, 0)

    with scope("c_dots"):
        @pl.when(is_end)
        def _():
            for source in (near, mid, far):
                for s in (first_of(source), second_of(source)):
                    take(0, s)

        early_dots(normed, acc, slice(0, core), slice(0, core), line)

    with scope("rot"):
        for copy in side_copies:
            copy.wait()
        lane = lax.broadcasted_iota(jnp.int32, (plane, qr), 1)
        half_dim = HEAD_DIM // 2
        table = trig[...]
        cos2 = jnp.where(lane < HEAD_DIM, table, pltpu.roll(table, HEAD_DIM, 1))
        sin2 = jnp.where(lane < HEAD_DIM, pltpu.roll(table, HEAD_DIM, 1), table)
        low = lane < HEAD_DIM
        first_half = lane % HEAD_DIM < half_dim

        def rot(v):
            partner = jnp.where(
                first_half, pltpu.roll(v, qr - half_dim, 1), pltpu.roll(v, half_dim, 1)
            )
            return v * cos2 + partner * sin2

        def bf(v):
            return v.astype(jnp.bfloat16).astype(jnp.float32)

        kv = jnp.where(low, bf(acc[:, qr : 2 * qr]), 0.0)
        ksq = jnp.sum(kv * kv, axis=-1, keepdims=True) / HEAD_DIM
        kgain = jnp.concatenate([kgain_ref[...], kgain_ref[...]], axis=1)
        kn = kv * lax.rsqrt(ksq + EPS) * kgain
        krot = rot(kn)
        keyed = jnp.where(y == 0, jnp.where(low, krot, 0.0), kv)
        keys[y, WINDOW : WINDOW + plane, :] = keyed.astype(jnp.bfloat16)

    bottom = pl.ds(WINDOW, WINDOW)
    top = pl.ds(plane, WINDOW)
    up = (jnp.minimum(2 * (z + 1) + y, 2 * line - 1), tp)
    down = (jnp.maximum(2 * (z - 1) + y, 0), tp)
    has_up = z < line - 1
    has_down = z > 0
    rim_up = remote(
        keys.at[y, top], keys.at[y, pl.ds(0, WINDOW)], rim_send.at[0], rim_recv.at[0], up
    )
    rim_down = remote(
        keys.at[y, bottom], keys.at[y, pl.ds(WINDOW + plane, WINDOW)], rim_send.at[1],
        rim_recv.at[1], down,
    )

    @pl.when(has_up)
    def _():
        rim_up.start()

    @pl.when(has_down)
    def _():
        rim_down.start()

    def kv_hop(place):
        begin, size = ((WINDOW, plane), (0, WINDOW), (WINDOW + plane, WINDOW))[place]
        here = keys.at[y, pl.ds(begin, size)]
        return remote(here, here, kv_send.at[place], kv_recv.at[place], y_peer)

    kv_hop(0).start()
    zero_rim = jnp.zeros((2, WINDOW, qr), jnp.bfloat16)

    @pl.when(z == 0)
    def _():
        keys[:, 0:WINDOW] = zero_rim

    @pl.when(z == line - 1)
    def _():
        keys[:, WINDOW + plane :] = zero_rim

    with scope("rotq"):
        qv = bf(acc[:, 0:qr])
        qq = qv * qv
        q_lo = jnp.sum(jnp.where(low, qq, 0.0), axis=-1, keepdims=True) / HEAD_DIM
        q_hi = jnp.sum(jnp.where(low, 0.0, qq), axis=-1, keepdims=True) / HEAD_DIM
        qgain = jnp.concatenate([qgain_ref[...], qgain_ref[...]], axis=1)
        qn = qv * lax.rsqrt(jnp.where(low, q_lo, q_hi) + EPS) * qgain
        qro = rot(qn)
        qrot[0] = jnp.where(low, qro, 0.0).astype(jnp.bfloat16)
        qrot[1] = jnp.where(low, pltpu.roll(qro, HEAD_DIM, 1), 0.0).astype(jnp.bfloat16)

    with scope("tok2_xb"):
        @pl.when(inner)
        def _():
            tok2_wait(xb, 2)
            tok2_share(xb, y, 1 - x)

    span = BLOCK + 2 * WINDOW
    total = plane * line

    def att_block(block):
        begin = pl.multiple_of(block * BLOCK, BLOCK)
        keyed = keys[0, pl.ds(begin, span), :]
        valued = keys[1, pl.ds(begin, span), :]
        qb = qrot[:, pl.ds(begin, BLOCK), :].reshape(2 * BLOCK, qr)
        scores = lax.dot_general(
            qb, keyed, (((1,), (1,)), ((), ())), preferred_element_type=jnp.float32
        ) * HEAD_DIM ** (-0.5)
        row = lax.broadcasted_iota(jnp.int32, (2 * BLOCK, span), 0)
        col = lax.broadcasted_iota(jnp.int32, (2 * BLOCK, span), 1)
        gap = row % BLOCK + WINDOW - col
        pos = z * plane + begin - WINDOW + col
        allowed = (gap <= WINDOW) & (gap >= -WINDOW) & (pos >= 0) & (pos < total)
        scores = jnp.where(allowed, scores, NEG_FILL)
        head = lax.broadcasted_iota(jnp.int32, (2 * BLOCK, 1), 0)
        sink = jnp.where(head < BLOCK, sink_ref[0, 2 * y], sink_ref[0, 2 * y + 1])
        peak = jnp.maximum(jnp.max(scores, axis=-1, keepdims=True), sink)
        expo = jnp.exp(scores - peak)
        denom = jnp.sum(expo, axis=-1, keepdims=True) + jnp.exp(sink - peak)
        weights = (expo / denom).astype(jnp.bfloat16)
        o = jnp.dot(weights, valued, preferred_element_type=jnp.float32)
        low_b = lax.broadcasted_iota(jnp.int32, (BLOCK, qr), 1) < HEAD_DIM
        both = jnp.where(low_b, o[:BLOCK], pltpu.roll(o[BLOCK:], HEAD_DIM, 1))
        mix_a[pl.ds(begin, BLOCK), :] = both.astype(jnp.bfloat16)

    nblocks = plane // BLOCK

    def att_inner(block, carry):
        att_block(block)
        return carry

    with scope("v_near2"):
        @pl.when(inner)
        def _():
            take(1, second_of(near))
            send_m(1, second_of(near))

        @pl.when(inner & (c == 0))
        def _():
            send_m(3, s_own)


    with scope("tok2_yb"):
        @pl.when(inner)
        def _():
            tok2_wait(yb, 3)
            tok2_share(yb, 1 - y, x)

    with scope("v_mid"):
        @pl.when(inner)
        def _():
            for s in (first_of(mid), second_of(mid)):
                take(1, s)

    with scope("v_dots"):
        @pl.when(inner)
        def _():
            early_dots(normed, acc, conv_cols, conv_rows, 3)

    def share_rims():
        with scope("rim_wait"):
            @pl.when(has_down)
            def _():
                rim_up.wait_recv()
                kv_hop(1).start()

            @pl.when(has_up)
            def _():
                rim_down.wait_recv()
                kv_hop(2).start()

    with scope("tok2_db"):
        @pl.when(inner)
        def _():
            tok2_wait(db, 1)
            tok2_share(db, 1 - y, 1 - x)

    with scope("o_mate"):
        @pl.when(is_end)
        def _():
            out_send(s_own, send_m)
            out_hop(s_mate, send_m)

    share_rims()

    with scope("o_mate"):
        @pl.when(inner)
        def _():
            out_hop(s_mate, send_m, send_e)

    def attend():
        with scope("kv_wait"):
            kv_hop(0).wait_recv()

        with scope("att_in"):
            lax.fori_loop(1, nblocks - 1, att_inner, 0)

        with scope("o_fwd"):
            @pl.when(inner)
            def _():
                out_hop(second_of(mid), send_e)

            @pl.when(inner & (c == 0))
            def _():
                take(3, first_of(mid))
                send_e(3, first_of(mid))

        with scope("kv_rims"):
            @pl.when(has_down)
            def _():
                kv_hop(1).wait_recv()

            @pl.when(has_up)
            def _():
                kv_hop(2).wait_recv()

        with scope("att_out"):
            def att_outer(k, carry):
                att_block(k * (nblocks - 1))
                return carry

            lax.fori_loop(0, 2, att_outer, 0)

    pad = 16
    zero_pad = jnp.zeros((pad, cr), jnp.bfloat16)
    taps = conv_ref[y]
    base = 2 * qr

    def convolve(ref, gate):
        p = ref[...].astype(jnp.float32)
        before = pltpu.roll(p, 1, 0)[pad : pad + plane]
        after = pltpu.roll(p, plane + 2 * pad - 1, 0)[pad : pad + plane]
        mixed = taps[0:1] * before + taps[1:2] * p[pad : pad + plane] + taps[2:3] * after
        return (gate * mixed).astype(jnp.bfloat16)

    prod_up = remote(
        prod.at[pl.ds(plane, pad)], prod.at[pl.ds(0, pad)], prod_send.at[0], prod_recv.at[0], up
    )
    prod_down = remote(
        prod.at[pl.ds(pad, pad)], prod.at[pl.ds(pad + plane, pad)],
        prod_send.at[1], prod_recv.at[1], down,
    )
    low_inner = inner & low_side
    high_inner = inner & (z >= 2)
    g_copy = remote(gated2, mix_c, g_send.at[0], g_recv.at[0], e_peer)

    @pl.when(inner)
    def _():
        with scope("tok2_rest"):
            for yy in range(2):
                for xx in range(2):
                    tok2_wait(block_of(yy, xx, 1 - c), 4 + quad(yy, xx))

        with scope("help_dots"):
            early_dots(normed2, acc2, slice(0, 3 * cr), conv_rows, 3)

        with scope("far_dots"):
            for s in (first_of(far), second_of(far)):
                take(1, s)
            plane_dots(normed2, acc2, slice(0, 3 * cr), conv_rows, far, True)
            plane_dots(normed, acc, conv_cols, conv_rows, far, True)

        with scope("prod"):
            left = bf(acc[:, base + cr : base + 2 * cr])
            inputs = bf(acc[:, base + 2 * cr : base + 3 * cr])
            prod[pad : pad + plane] = (left * inputs).astype(jnp.bfloat16)

            @pl.when(low_inner)
            def _():
                prod_up.start()

            @pl.when(high_inner)
            def _():
                prod_down.start()

            out_hop(2 * near, send_m)

            prod2[pad : pad + plane] = (
                bf(acc2[:, cr : 2 * cr]) * bf(acc2[:, 2 * cr : 3 * cr])
            ).astype(jnp.bfloat16)

            @pl.when(z == 1)
            def _():
                prod2[0:pad] = zero_pad
                prod2[pad + plane :] = prod[pad : 2 * pad]
                prod[0:pad] = prod2[plane : plane + pad]

            @pl.when(z != 1)
            def _():
                prod2[0:pad] = prod[plane : plane + pad]
                prod2[pad + plane :] = zero_pad
                prod[pad + plane :] = prod2[pad : 2 * pad]

            gated2[...] = convolve(prod2, bf(acc2[:, 0:cr]))
            g_copy.start()

            out_hop(2 * near + 1, send_m)

        attend()

        with scope("prod_wait"):
            @pl.when(low_inner)
            def _():
                prod_down.wait_recv()

            @pl.when(high_inner)
            def _():
                prod_up.wait_recv()

            mix_c[...] = convolve(prod, bf(acc[:, base : base + cr]))

    @pl.when(is_end)
    def _():
        attend()
        with scope("g_wait"):
            g_copy.wait_recv()

    def group(cc):
        spans = [pl.ds(pl.multiple_of((2 * q + cc) * rows, rows), rows) for q in range(4)]
        return [jnp.concatenate([mix_a[w, :], mix_c[w, :]], axis=1) for w in spans]

    mine_rows = jnp.concatenate(group(c), axis=0)
    other_rows = jnp.concatenate(group(1 - c), axis=0)

    def rs_hop(src, dst, stage_id, s, peer):
        return remote(src, dst, rs_send.at[min(stage_id, 1)], rs_recv.at[stage_id, s], peer)

    def out_take(i):
        s = 2 * sources[i // 2] + i % 2
        out_hop(s)

    def out_forward(i):
        out_hop(2 * sources[i // 2] + i % 2, send_e)

    def stage_a(i):
        s = 2 * sources[i // 2] + i % 2
        weight = wout[s]
        s1[s] = jnp.dot(
            other_rows, weight, preferred_element_type=jnp.float32
        ).astype(jnp.bfloat16).reshape(2, 2, rows, depth)
        rs_hop(s1.at[s], r1.at[s], 0, s, c_peer).start()
        keep[s] = jnp.dot(
            mine_rows, weight, preferred_element_type=jnp.float32
        ).reshape(2, 2, rows, depth)

    d_peer = (2 * z + 1 - y, 2 * (1 - x) + c)
    corners = ((1 - y, 1 - x, d_peer), (1 - y, x, y_peer), (y, 1 - x, x_peer))

    staged = 6

    def stage_b(i):
        half = i % 2
        s = 2 * sources[i // 2] + half
        rs_hop(s1.at[s], r1.at[s], 0, s, c_peer).wait_recv()

        def put(j, yy, xx):
            s2[s, j] = (keep[s, yy, xx] + r1[s, yy, xx].astype(jnp.float32)).astype(jnp.bfloat16)

        if i < staged:
            for j in range(2):
                put(j, *((1 - y, j) if half == 0 else (j, 1 - x)))
            pair_hop(s, half).start()
        else:
            for j, (yy, xx, peer) in enumerate(corners):
                put(j, yy, xx)
                rs_hop(s2.at[s, j], r2.at[s, j], 1, s, peer).start()

    def pair_hop(s, half):
        peer = y_peer if half == 0 else x_peer
        return rs_hop(s2.at[s, 0:2], r2.at[s, 0:2], 1, s, peer)

    def last_hop(s, half):
        peer = x_peer if half == 0 else y_peer
        return rs_hop(s2.at[s, 2], r2.at[s, 2], 2, s, peer)

    def stage_c(i):
        half = i % 2
        s = 2 * sources[i // 2] + half
        pair_hop(s, half).wait_recv()
        yy, xx, j = (y, 1 - x, 1 - x) if half == 0 else (1 - y, x, 1 - y)
        piece = keep[s, yy, xx] + r1[s, yy, xx].astype(jnp.float32)
        s2[s, 2] = (piece + r2[s, j].astype(jnp.float32)).astype(jnp.bfloat16)
        last_hop(s, half).start()

    def stage_d(i):
        half = i % 2
        s = 2 * sources[i // 2] + half
        piece = keep[s, y, x] + r1[s, y, x].astype(jnp.float32)
        if i < staged:
            last_hop(s, half).wait_recv()
            piece = piece + r2[s, x if half == 0 else y].astype(jnp.float32)
            piece = piece + r2[s, 2].astype(jnp.float32)
        else:
            rs_hop(s2.at[s], r2.at[s], 1, s, d_peer).wait_recv()
            for j in range(3):
                piece = piece + r2[s, j].astype(jnp.float32)
        out_ref[:, columns(s)] = piece.astype(jnp.bfloat16)

    order = (
        ("a", (0, 1,)), ("f", (6,)), ("b", (0,)), ("a", (2,)), ("b", (1,)), ("a", (3,)),
        ("b", (2,)), ("w", (4,)), ("a", (4,)), ("b", (3,)), ("f", (7,)), ("w", (5,)), ("a", (5,)),
        ("b", (4,)), ("c", (0, 1,)), ("w", (6,)), ("a", (6,)), ("b", (5,)), ("c", (2, 3,)),
        ("w", (7,)), ("a", (7,)), ("b", (6, 7,)), ("c", (4, 5,)),
        ("d", (0, 1, 2, 3, 4, 6, 5, 7,)),
    )

    for step, places in order:
        for i in places:
            with scope(f"{step}{i}"):
                if step == "w":
                    pl.when(is_end)(functools.partial(out_take, i))
                elif step == "f":
                    pl.when(inner)(functools.partial(out_forward, i))
                elif step == "a":
                    if i in (2, 3):
                        pl.when(is_end)(functools.partial(out_take, i))
                    stage_a(i)
                elif step == "b":
                    stage_b(i)
                elif step == "c":
                    stage_c(i)
                else:
                    stage_d(i)

    def sent(ref, send):
        remote(ref, ref, send, w_recv.at[0, 0], m_peer).wait_send()

    def chunks_sent(kind, count, sends):
        if kind > 1:
            ref = wout.at[0:count, 0:qr] if kind == 2 else wout.at[0:count, qr : qr + cr]
        else:
            ref = win.at[0:count, 0:core] if kind == 0 else win.at[0:count, core : core + 3 * cr]
        sent(ref, sends.at[kind])

    with scope("sends"):
        for kind in range(4):
            y_hop(kind).wait_send()
        sent(normed.at[0:7], tok_send.at[0])
        sent(s1, rs_send.at[0])
        sent(s2, rs_send.at[1])

        kv_hop(0).wait_send()

        @pl.when(has_up)
        def _():
            rim_up.wait_send()
            kv_hop(2).wait_send()

        @pl.when(has_down)
        def _():
            rim_down.wait_send()
            kv_hop(1).wait_send()

        @pl.when(is_end)
        def _():
            sent(normed.at[0:2], tok2_send.at[0])
            for kind in range(4):
                chunks_sent(kind, 2, m_send)

        @pl.when(inner)
        def _():
            sent(normed2.at[0:6], tok2_send.at[0])
            g_copy.wait_send()
            for kind in range(4):
                chunks_sent(kind, 4, m_send)
            for kind in (0, 2, 3):
                chunks_sent(kind, 6, e_send)

        @pl.when(low_inner)
        def _():
            prod_up.wait_send()

        @pl.when(high_inner)
        def _():
            prod_down.wait_send()


def trig_table(total):
    half = HEAD_DIM // 2
    freq = np.float64(ROPE_BASE) ** (-np.arange(half) / half)
    angle = np.arange(total)[:, None] * freq
    cosine, sine = np.cos(angle), np.sin(angle)
    return np.concatenate([cosine, cosine, -sine, sine], axis=1).astype(np.float32)


def fused_device(
    tokens, norm_gain, query_weight, key_weight, value_weight, gate_weight, left_weight,
    input_weight, query_gain, key_gain, sink_logit, conv_weight, out_attention, out_conv,
):
    sp_count = lax.axis_size("sp")
    line = sp_count // 2
    rows, width = tokens.shape
    depth = query_weight.shape[1]
    qr = query_weight.shape[0] // 2
    kr = key_weight.shape[0]
    cr = gate_weight.shape[0] // 2
    fan = qr + kr + 3 * cr
    plane = 8 * rows
    dims = dict(line=line, rows=rows, depth=depth, qr=qr, kr=kr, cr=cr)
    hb = pl.BlockSpec(memory_space=pltpu.HBM)
    bf16, f32 = jnp.bfloat16, jnp.float32
    dma = pltpu.SemaphoreType.DMA
    n = sp_count
    scratch = [
        pltpu.VMEM((1, width), f32),
        pltpu.VMEM((1, HEAD_DIM), f32),
        pltpu.VMEM((1, HEAD_DIM), f32),
        pltpu.SMEM((1, 4), f32),
        pltpu.VMEM((2, 3, cr), f32),
        pltpu.VMEM((rows, width), bf16),
        pltpu.VMEM((plane, 2 * HEAD_DIM), f32),
        pltpu.VMEM((fan, depth), bf16),
        pltpu.VMEM((qr + cr, depth), bf16),
        pltpu.VMEM((n, fan, depth), bf16),
        pltpu.VMEM((n, qr + cr, depth), bf16),
        pltpu.VMEM((8, rows, width), bf16),
        pltpu.VMEM((8, rows, width), bf16),
        pltpu.VMEM((plane, 2 * qr + 3 * cr), f32),
        pltpu.VMEM((plane, 3 * cr), f32),
        pltpu.VMEM((2, plane + 2 * WINDOW, qr), bf16),
        pltpu.VMEM((plane + 32, cr), bf16),
        pltpu.VMEM((plane + 32, cr), bf16),
        pltpu.VMEM((plane, qr), bf16),
        pltpu.VMEM((plane, cr), bf16),
        pltpu.VMEM((plane, cr), bf16),
        pltpu.VMEM((2, plane, qr), bf16),
        pltpu.VMEM((n, 2, 2, rows, depth), f32),
        pltpu.VMEM((n, 2, 2, rows, depth), bf16),
        pltpu.VMEM((n, 2, 2, rows, depth), bf16),
        pltpu.VMEM((n, 3, rows, depth), bf16),
        pltpu.VMEM((n, 3, rows, depth), bf16),
        dma((11,)), dma((4,)), dma((4, n)), dma((4,)), dma((4,)),
        dma((1,)), dma((10,)), dma((1,)), dma((8,)), dma((2,)), dma((2,)), dma((3,)), dma((3,)),
        dma((2,)), dma((2,)),
        dma((1,)), dma((1,)), dma((2,)), dma((3, n)),
    ]
    taps = conv_weight.reshape(3, 2, cr).transpose(1, 0, 2)
    return pl.pallas_call(
        functools.partial(fused_kernel, dims),
        out_shape=jax.ShapeDtypeStruct((rows, width), bf16),
        in_specs=[hb] * 15,
        out_specs=pl.BlockSpec(memory_space=pltpu.VMEM),
        scratch_shapes=scratch,
        compiler_params=pltpu.CompilerParams(
            collective_id=0, has_side_effects=True, vmem_limit_bytes=32 * 1024 * 1024
        ),
    )(*(pltpu.with_memory_space_constraint(array, pltpu.HBM) for array in (
        tokens, norm_gain[None, :], query_weight, key_weight, value_weight, gate_weight,
        left_weight, input_weight, query_gain[None, :],
        key_gain[None, :], sink_logit[None, :], taps, out_attention, out_conv,
        jnp.asarray(trig_table(plane * line)),
    )))


def local_device(*args):
    tokens, query_weight, key_weight, gate_weight = args[0], args[2], args[3], args[5]
    fits = (
        lax.axis_size("sp") == 8
        and lax.axis_size("tp") == 4
        and query_weight.shape[1] % 128 == 0
        and query_weight.shape[0] == 4 * HEAD_DIM
        and key_weight.shape[0] == HEAD_DIM
        and gate_weight.shape[0] == 256
        and tokens.shape[0] % 32 == 0
        and 8 * tokens.shape[0] % BLOCK == 0
        and 8 * tokens.shape[0] >= 2 * BLOCK
    )
    return fused_device(*args) if fits else per_device(*args)


def solution(mesh):
    in_specs = (
        P(("sp", "tp"), None),
        P(),
        P("tp", "sp"),
        P("tp", "sp"),
        P("tp", "sp"),
        P("tp", "sp"),
        P("tp", "sp"),
        P("tp", "sp"),
        P(),
        P(),
        P("tp"),
        P(None, "tp"),
        P("tp", "sp"),
        P("tp", "sp"),
    )
    out_specs = P(("sp", "tp"), None)
    return jax.shard_map(
        local_device, mesh=mesh, in_specs=in_specs, out_specs=out_specs, check_vma=False
    )
```
